32 devices in a mesh: sp: 4 (over z), tp: 8 (over y, x, core).
Axes of the slice: x: 2, y: 2, z: 4, core: 2. Of those that a mesh axis runs over, the one named last changes fastest.
Arguments:
- target_rows: bfloat16 [768, 2048], P(('sp', 'tp')), may hold values from -6 to 6
- source_rows: bfloat16 [4096, 2048], P(('sp', 'tp')), may hold values from -6 to 6
- target_gain: float32 [2048], replicated, may hold values from 0.55 to 9
- source_gain: float32 [2048], replicated, may hold values from 0.55 to 9
- query_weight: bfloat16 [2048, 2048], P(None, 'tp'), may hold values from -0.125 to 0.125
- key_weight: bfloat16 [2048, 512], P('tp'), may hold values from -0.125 to 0.125
- value_weight: bfloat16 [2048, 512], P('tp'), may hold values from -0.125 to 0.125
- out_weight: bfloat16 [2048, 2048], P('tp'), may hold values from -0.125 to 0.125
- out_cotangent: bfloat16 [768, 2048], P(('sp', 'tp')), may hold values from -6 to 6
Outputs:
- target_grad: float32 [768, 2048], P(('sp', 'tp'))
- source_grad: float32 [4096, 2048], P(('sp', 'tp'))
- out_weight_grad: float32 [2048, 2048], P('tp')
The draws below stay inside these ranges and needn't reach their ends.
All inputs are finite; a program needn't handle non-finite values.
Results may differ from the reference program's by a relative error of at most 0.03.
Values may be sent and summed in bfloat16 or wider, within the bound.
A program may use at most 64 MiB of HBM per device.

```python
import jax
import jax.numpy as jnp
from jax import lax

D = 2048
HEADS = 32
HEAD_DIM = 64
KV_HEADS = 8
TGT_ALL = 768
SRC_ALL = 4096


def gain_draw(seed_key):
    return 1.0 + 0.18 * jax.random.truncated_normal(seed_key, -2.5, 2.5, (D,), jnp.float32)


def draw_target_gain(key, part):
    return gain_draw(jax.random.fold_in(key, 11))


def draw_source_gain(key, part):
    return gain_draw(jax.random.fold_in(key, 23))


def steps_of(key, extent, cuts, least, largest):
    level = 1.0
    for axis_at, blocks in cuts:
        heights = jax.random.uniform(jax.random.fold_in(jax.random.fold_in(key, 6), axis_at), (blocks,), jnp.float32, least / len(cuts), largest / len(cuts))
        level = level * jnp.repeat(jnp.exp(heights), extent[axis_at] // blocks).reshape((-1,) + (1,) * (len(extent) - 1 - axis_at))
    return level


def scatter_about(key, extent, spread, bound, shards=(), kind=jnp.bfloat16):
    drawn = jax.random.normal(key, extent, jnp.float32) * spread
    if len(shards) > 0:
        drawn = steps_of(key, extent, shards, -0.22, 0.18) * drawn
    return jnp.clip(drawn, min=-bound, max=bound).astype(kind)


def setup_inputs(seed: int = 0) -> dict:
    streams_of = jax.random.split(jax.random.key(seed), 10)
    return {
        "target_rows": scatter_about(streams_of[0], (TGT_ALL, D), 1.0, 6.0, ((0, 32),)),
        "source_rows": scatter_about(streams_of[1], (SRC_ALL, D), 1.0, 6.0, ((0, 32),)),
        "target_gain": draw_target_gain(jax.random.fold_in(streams_of[9], 71), 0),
        "source_gain": draw_source_gain(jax.random.fold_in(streams_of[9], 71), 0),
        "query_weight": scatter_about(streams_of[4], (D, HEADS * HEAD_DIM), D ** -0.5, 0.125, ((1, 8),)),
        "key_weight": scatter_about(streams_of[5], (D, KV_HEADS * HEAD_DIM), D ** -0.5, 0.125, ((0, 8),)),
        "value_weight": scatter_about(streams_of[6], (D, KV_HEADS * HEAD_DIM), D ** -0.5, 0.125, ((0, 8),)),
        "out_weight": scatter_about(streams_of[7], (HEADS * HEAD_DIM, D), (HEADS * HEAD_DIM) ** -0.5, 0.125, ((0, 8),)),
        "out_cotangent": scatter_about(streams_of[8], (TGT_ALL, D), 1.0, 6.0, ((0, 32),)),
    }


EPSILON = 1e-06

def normalize(matrix, gain_vector):
    widened = matrix.astype(jnp.float32)
    factor = lax.rsqrt(lax.optimization_barrier(jnp.mean(widened * widened, axis=-1, keepdims=True)) + EPSILON)
    return (widened * factor * gain_vector).astype(jnp.bfloat16)

def norm_back(matrix, gain_vector, upstream):
    widened = matrix.astype(jnp.float32)
    factor = lax.rsqrt(lax.optimization_barrier(jnp.mean(widened * widened, axis=-1, keepdims=True)) + EPSILON)
    weighted = upstream * gain_vector
    inner_sum = lax.optimization_barrier(jnp.mean(weighted * widened, axis=-1, keepdims=True))
    return factor * weighted - widened * factor ** 3 * inner_sum

def reference(target_rows, source_rows, target_gain, source_gain, query_weight, key_weight, value_weight, out_weight, out_cotangent):
    score_scale = HEAD_DIM ** (-0.5)
    group_size = HEADS // KV_HEADS
    normed_t = normalize(target_rows, target_gain)
    normed_s = normalize(source_rows, source_gain)
    queries = jnp.dot(normed_t, query_weight, preferred_element_type=jnp.float32).astype(jnp.bfloat16)
    keys_all = jnp.dot(normed_s, key_weight, preferred_element_type=jnp.float32).astype(jnp.bfloat16)
    values_all = jnp.dot(normed_s, value_weight, preferred_element_type=jnp.float32).astype(jnp.bfloat16)
    query_heads = queries.reshape(TGT_ALL, HEADS, HEAD_DIM).transpose(1, 0, 2)
    key_heads = keys_all.reshape(SRC_ALL, KV_HEADS, HEAD_DIM).transpose(1, 0, 2)
    value_heads = values_all.reshape(SRC_ALL, KV_HEADS, HEAD_DIM).transpose(1, 0, 2)
    out_heads = out_weight.reshape(HEADS, HEAD_DIM, D)

    def one_head(head_index):
        query = query_heads[head_index]
        key_head = key_heads[head_index // group_size]
        value_head = value_heads[head_index // group_size]
        scores = jnp.dot(query, key_head.T, preferred_element_type=jnp.float32) * score_scale
        row_max = lax.optimization_barrier(jnp.max(scores, axis=1, keepdims=True))
        weights = jnp.exp(scores - row_max)
        total = lax.optimization_barrier(jnp.sum(weights, axis=1, keepdims=True))
        attended = (jnp.dot(weights.astype(jnp.bfloat16), value_head, preferred_element_type=jnp.float32) / total).astype(jnp.bfloat16)
        log_total = row_max + jnp.log(total)
        d_attended = jnp.dot(out_cotangent, out_heads[head_index].T, preferred_element_type=jnp.float32).astype(jnp.bfloat16)
        delta = lax.optimization_barrier(jnp.sum(d_attended.astype(jnp.float32) * attended.astype(jnp.float32), axis=1, keepdims=True))
        probs = jnp.exp(scores - log_total)
        d_value = jnp.dot(probs.astype(jnp.bfloat16).T, d_attended, preferred_element_type=jnp.float32)
        d_probs = jnp.dot(d_attended, value_head.T, preferred_element_type=jnp.float32)
        d_scores = (probs * (d_probs - delta)).astype(jnp.bfloat16)
        d_query = jnp.dot(d_scores, key_head, preferred_element_type=jnp.float32) * score_scale
        d_key = jnp.dot(d_scores.T, query, preferred_element_type=jnp.float32) * score_scale
        return (attended, d_query, d_key, d_value)
    attended, d_query, d_key, d_value = lax.map(one_head, jnp.arange(HEADS))
    key_sum = lax.optimization_barrier(jnp.sum(d_key.reshape(KV_HEADS, group_size, SRC_ALL, HEAD_DIM), axis=1))
    value_sum = lax.optimization_barrier(jnp.sum(d_value.reshape(KV_HEADS, group_size, SRC_ALL, HEAD_DIM), axis=1))
    key_grad = key_sum.transpose(1, 0, 2).reshape(SRC_ALL, KV_HEADS * HEAD_DIM).astype(jnp.bfloat16)
    value_grad = value_sum.transpose(1, 0, 2).reshape(SRC_ALL, KV_HEADS * HEAD_DIM).astype(jnp.bfloat16)
    attended_rows = attended.transpose(1, 0, 2).reshape(TGT_ALL, HEADS * HEAD_DIM)
    query_grad = d_query.transpose(1, 0, 2).reshape(TGT_ALL, HEADS * HEAD_DIM).astype(jnp.bfloat16)
    out_weight_grad = jnp.dot(attended_rows.T, out_cotangent, preferred_element_type=jnp.float32)
    d_normed_t = jnp.dot(query_grad, query_weight.T, preferred_element_type=jnp.float32)
    target_grad = out_cotangent.astype(jnp.float32) + norm_back(target_rows, target_gain, d_normed_t)
    d_normed_s = jnp.dot(key_grad, key_weight.T, preferred_element_type=jnp.float32) + jnp.dot(value_grad, value_weight.T, preferred_element_type=jnp.float32)
    source_grad = norm_back(source_rows, source_gain, d_normed_s)
    return (target_grad, source_grad, out_weight_grad)
```

```python
import functools

import jax
import jax.numpy as jnp
from jax import lax
from jax.experimental import pallas as pl
from jax.experimental.pallas import tpu as pltpu
from jax.sharding import PartitionSpec as P

HEAD_DIM = 64
KV_HEADS = 8
EPSILON = 1e-06
MESH = pl.DeviceIdType.MESH


def normalize(matrix, gain_vector):
    widened = matrix.astype(jnp.float32)
    factor = lax.rsqrt(jnp.mean(widened * widened, axis=-1, keepdims=True) + EPSILON)
    return (widened * factor * gain_vector).astype(jnp.bfloat16)


def norm_back(matrix, gain_vector, upstream):
    widened = matrix.astype(jnp.float32)
    factor = lax.rsqrt(jnp.mean(widened * widened, axis=-1, keepdims=True) + EPSILON)
    weighted = upstream * gain_vector
    inner_sum = jnp.mean(weighted * widened, axis=-1, keepdims=True)
    return factor * weighted - widened * factor**3 * inner_sum


def exchange_kernel(kinds, sp_n, tp_n, *refs):
    count = len(kinds)
    ins, outs = refs[:count], refs[count : 2 * count]
    send_sems, recv_sems = refs[2 * count : 3 * count], refs[3 * count :]
    sp_me, tp_me = lax.axis_index("sp"), lax.axis_index("tp")
    sizes, places = {"sp": sp_n, "tp": tp_n}, {"sp": sp_me, "tp": tp_me}

    def address(axis, peer):
        return (peer, tp_me) if axis == "sp" else (sp_me, peer)

    axes = sorted({kind.split("_")[1] for kind in kinds})
    barrier = pltpu.get_barrier_semaphore()
    for axis in axes:
        for k in range(1, sizes[axis]):
            peer = lax.rem(places[axis] + k, sizes[axis])
            pl.semaphore_signal(barrier, inc=1, device_id=address(axis, peer), device_id_type=MESH)
    pl.semaphore_wait(barrier, sum(sizes[axis] - 1 for axis in axes))

    def copy(i, axis, source, slot, k, peer):
        return pltpu.make_async_remote_copy(
            src_ref=source,
            dst_ref=outs[i].at[slot],
            send_sem=send_sems[i].at[k],
            recv_sem=recv_sems[i].at[slot],
            device_id=address(axis, peer),
            device_id_type=MESH,
        )

    sent = []
    used = [0] * count

    def send(i, axis, source, target, recv, peer, keep=True):
        one = pltpu.make_async_remote_copy(
            src_ref=source,
            dst_ref=target,
            send_sem=send_sems[i].at[used[i]],
            recv_sem=recv_sems[i].at[recv],
            device_id=address(axis, peer),
            device_id_type=MESH,
        )
        used[i] += 1
        one.start()
        if keep:
            sent.append(one)
        return one

    def arrived(i, axis, target, recv):
        pltpu.make_async_remote_copy(
            src_ref=target,
            dst_ref=target,
            send_sem=send_sems[i].at[0],
            recv_sem=recv_sems[i].at[recv],
            device_id=address(axis, lax.rem(places[axis] + 1, sizes[axis])),
            device_id_type=MESH,
        ).wait_recv()

    square = tp_n == 8
    partner = tp_me + 1 - 2 * lax.rem(tp_me, 2)

    def across(index):
        return index + 2 - 4 * lax.rem(index // 2, 2)

    def along(index):
        return index + 4 - 8 * lax.rem(index // 4, 2)

    def relatives(index):
        if square:
            return [across(index), along(index)]
        return [lax.rem(index + 2 * k, tp_n) for k in range(1, tp_n // 2)]

    def forward(i, c, origin):
        chunks = ins[i].shape[0]
        piece, recv = outs[i].at[origin, c], origin * chunks + c
        arrived(i, "tp", piece, recv)
        send(i, "tp", piece, piece, recv, partner)
        return piece, recv

    line_sent = []
    depth = max([ins[i].shape[0] for i in range(count) if kinds[i] == "pair_tp"], default=0)
    for c in range(depth):
        for i, kind in enumerate(kinds):
            if kind == "pair_tp" and c < ins[i].shape[0]:
                chunks = ins[i].shape[0]
                for peer in relatives(tp_me) + [partner]:
                    piece = outs[i].at[tp_me, c]
                    send(i, "tp", ins[i].at[c], piece, tp_me * chunks + c, peer)
    for i, kind in enumerate(kinds):
        mode, axis = kind.split("_")
        n, me = sizes[axis], places[axis]
        if mode == "line":
            for step in (1, -1):
                inside = (me < n - 1) if step == 1 else (me > 0)
                for c in range(ins[i].shape[0]):
                    line_sent.append((i, inside, used[i], me, c))
                    recv = me * ins[i].shape[0] + c

                    @pl.when(inside)
                    def _():
                        piece = outs[i].at[me, c]
                        send(i, axis, ins[i].at[c], piece, recv, me + step, keep=False)
        elif mode != "pair":
            for k in range(1, n):
                peer = lax.rem(me + k, n)
                source = ins[i] if mode == "gather" else ins[i].at[peer]
                send(i, axis, source, outs[i].at[me], me, peer)
    for i, kind in enumerate(kinds):
        mode, axis = kind.split("_")
        me = places[axis]
        outs[i][me] = ins[i][me] if mode == "swap" else ins[i][...]

    def line_step(i, far, c):
        n, me = sp_n, sp_me
        chunks = ins[i].shape[0]
        for step in (1, -1):
            origin = me - step * far
            valid = (origin >= 0) if step == 1 else (origin <= n - 1)
            onward = (valid & (me < n - 1)) if step == 1 else (valid & (me > 0))

            @pl.when(valid)
            def _():
                arrived(i, "sp", outs[i].at[origin, c], origin * chunks + c)

            if far < n - 1:
                line_sent.append((i, onward, used[i], origin, c))

                @pl.when(onward)
                def _():
                    piece = outs[i].at[origin, c]
                    recv = origin * chunks + c
                    send(i, "sp", piece, piece, recv, me + step, keep=False)

    def pair_step(i, c):
        me = tp_me
        chunks = ins[i].shape[0]
        for order, origin in enumerate(relatives(me)):
            piece, recv = forward(i, c, origin)
            if square and order == (i + c) % 2:
                send(i, "tp", piece, piece, recv, along(me) if order == 0 else across(me))

    lines = [i for i in range(count) if kinds[i] == "line_sp"]
    pairs = [i for i in range(count) if kinds[i] == "pair_tp"]
    for turn in range(max(depth, sp_n - 1 if lines else 0)):
        for i in pairs:
            if turn < ins[i].shape[0]:
                pair_step(i, turn)
        for i in lines:
            if turn + 1 < sp_n:
                for c in range(ins[i].shape[0]):
                    line_step(i, turn + 1, c)
    if square:
        for c in range(depth):
            for i in pairs:
                if c < ins[i].shape[0]:
                    forward(i, c, across(along(tp_me)))
    for i, kind in enumerate(kinds):
        mode, axis = kind.split("_")
        n, me = sizes[axis], places[axis]
        if mode == "pair":
            chunks = ins[i].shape[0]
            others = relatives(partner) + ([across(along(partner))] if square else [])
            for origin in [partner] + others:
                for c in range(chunks):
                    arrived(i, axis, outs[i].at[origin, c], origin * chunks + c)
        elif mode != "line":
            for k in range(1, n):
                origin = lax.rem(me + n - k, n)
                arrived(i, axis, outs[i].at[origin], origin)
    for one in sent:
        one.wait_send()
    for i, happened, slot, origin, c in line_sent:

        @pl.when(happened)
        def _():
            pltpu.make_async_remote_copy(
                src_ref=outs[i].at[origin, c],
                dst_ref=outs[i].at[origin, c],
                send_sem=send_sems[i].at[slot],
                recv_sem=recv_sems[i].at[0],
                device_id=address("sp", lax.rem(sp_me + 1, sp_n)),
                device_id_type=MESH,
            ).wait_send()


def exchange(collective_id, *parts):
    sp_n, tp_n = lax.axis_size("sp"), lax.axis_size("tp")
    kinds = tuple(kind for kind, array in parts)
    arrays = [array for kind, array in parts]
    shapes, sends, recvs = [], [], []
    for kind, array in parts:
        mode, axis = kind.split("_")
        n = sp_n if axis == "sp" else tp_n
        shape = array.shape if mode == "swap" else (n,) + array.shape
        shapes.append(jax.ShapeDtypeStruct(shape, array.dtype))
        chunks = array.shape[0] if mode in ("pair", "line") else 1
        sends.append(pltpu.SemaphoreType.DMA(((2 * n + 8) * chunks,)))
        recvs.append(pltpu.SemaphoreType.DMA((n * chunks,)))
    return pl.pallas_call(
        functools.partial(exchange_kernel, kinds, sp_n, tp_n),
        out_shape=shapes,
        in_specs=[pl.BlockSpec(memory_space=pltpu.VMEM)] * len(parts),
        out_specs=[pl.BlockSpec(memory_space=pltpu.VMEM)] * len(parts),
        scratch_shapes=sends + recvs,
        compiler_params=pltpu.CompilerParams(
            collective_id=collective_id,
            has_side_effects=True,
            vmem_limit_bytes=56 * 1024 * 1024,
        ),
    )(*arrays)


def matmul(left, right):
    return jnp.dot(left, right, preferred_element_type=jnp.float32)


def einsum(text, left, right):
    return jnp.einsum(text, left, right, preferred_element_type=jnp.float32)


def body(
    target_rows,
    source_rows,
    target_gain,
    source_gain,
    query_weight,
    key_weight,
    value_weight,
    out_weight,
    out_cotangent,
):
    sp_n, tp_n = lax.axis_size("sp"), lax.axis_size("tp")
    width = target_rows.shape[1]
    local_width = query_weight.shape[1]
    local_heads = local_width // HEAD_DIM
    slot_heads = max(1, KV_HEADS // tp_n)
    copies = max(1, tp_n // KV_HEADS)
    per_slot = local_heads // slot_heads
    slot_width = slot_heads * HEAD_DIM
    score_scale = HEAD_DIM ** (-0.5)
    bf16 = jnp.bfloat16

    normed_t = normalize(target_rows, target_gain)
    normed_s = normalize(source_rows, source_gain)
    source_local = normed_s.shape[0]
    target_local = normed_t.shape[0]
    target_block = tp_n * target_local
    source_block = tp_n * source_local

    rows_in, cot_in = exchange(
        0,
        ("pair_tp", normed_t[None]),
        ("pair_tp", out_cotangent[None]),
    )
    queries = matmul(rows_in.reshape(target_block, width), query_weight).astype(bf16)
    d_attended = matmul(cot_in.reshape(target_block, width), out_weight.T).astype(bf16)
    halves = (2, key_weight.shape[0] // 2, key_weight.shape[1])
    split = (2, target_block // 2, local_width)
    key_full, value_full, all_queries, all_grads, cot_column = exchange(
        1,
        ("pair_tp", key_weight.reshape(halves)),
        ("pair_tp", value_weight.reshape(halves)),
        ("line_sp", queries.reshape(split)),
        ("line_sp", d_attended.reshape(split)),
        ("line_sp", out_cotangent[None]),
    )
    key_full = key_full.reshape(width, -1)
    value_full = value_full.reshape(width, -1)
    key_own = matmul(normed_s, key_full).astype(bf16)
    value_own = matmul(normed_s, value_full).astype(bf16)

    def to_slots(matrix):
        split = matrix.reshape(source_local, tp_n // copies, 1, slot_width)
        spread = jnp.broadcast_to(split, (source_local, tp_n // copies, copies, slot_width))
        return spread.reshape(source_local, tp_n, slot_width).transpose(1, 0, 2)

    slots = jnp.concatenate([to_slots(key_own), to_slots(value_own)], axis=2)
    (kv_block,) = exchange(2, ("swap_tp", slots))
    whole_rows = sp_n * target_block
    kv_block = kv_block.reshape(source_block, 2, slot_heads, HEAD_DIM)
    keys, values = kv_block[:, 0], kv_block[:, 1]
    head_shape = (whole_rows, slot_heads, per_slot, HEAD_DIM)
    query_view = all_queries.reshape(head_shape)
    grad_view = all_grads.reshape(head_shape)

    scores = einsum("tgqd,sgd->gqts", query_view, keys) * score_scale
    part_max = jnp.max(scores, axis=-1)
    weights = jnp.exp(scores - part_max[..., None])
    part_total = jnp.sum(weights, axis=-1)
    d_probs = einsum("tgqd,sgd->gqts", grad_view, values)
    part_delta = jnp.sum(weights * d_probs, axis=-1)
    part_sum = einsum("gqts,sgd->tgqd", weights.astype(bf16), values)
    stats = jnp.stack([part_max, part_total, part_delta]).reshape(3 * local_heads, whole_rows)
    (all_stats,) = exchange(3, ("gather_sp", stats))
    all_stats = all_stats.reshape(sp_n, 3, slot_heads, per_slot, whole_rows)
    row_max = jnp.max(all_stats[:, 0], axis=0)
    rescale = jnp.exp(all_stats[:, 0] - row_max)
    total = jnp.sum(all_stats[:, 1] * rescale, axis=0)
    delta = jnp.sum(all_stats[:, 2] * rescale, axis=0) / total
    local_scale = jnp.exp(part_max - row_max) / total

    attended_part = part_sum * local_scale.transpose(2, 0, 1)[..., None]
    attended_part = attended_part.reshape(sp_n, target_block, local_width).astype(bf16)
    probs = weights * local_scale[..., None]
    d_scores = (probs * (d_probs - delta[..., None])).astype(bf16)
    value_sum = einsum("gqts,tgqd->sgd", probs.astype(bf16), grad_view)
    key_sum = einsum("gqts,tgqd->sgd", d_scores, query_view) * score_scale
    d_query = einsum("gqts,sgd->tgqd", d_scores, keys) * score_scale
    d_query = d_query.reshape(sp_n, target_block, local_width).astype(bf16)
    grads = jnp.concatenate(
        [key_sum.reshape(source_block, slot_width), value_sum.reshape(source_block, slot_width)],
        axis=1,
    )
    grads = grads.reshape(tp_n, source_local, 2 * slot_width).astype(bf16)
    query_terms, attended_terms, grads_back, cot_all = exchange(
        4,
        ("swap_sp", d_query),
        ("swap_sp", attended_part),
        ("swap_tp", grads),
        ("pair_tp", cot_column.reshape(sp_n, target_local, width)),
    )
    query_grad = jnp.sum(query_terms.astype(jnp.float32), axis=0).astype(bf16)
    attended = jnp.sum(attended_terms.astype(jnp.float32), axis=0).astype(bf16)

    target_terms = matmul(query_grad, query_weight.T).astype(bf16)
    target_back, attended_all = exchange(
        5,
        ("swap_tp", target_terms.reshape(tp_n, target_local, width)),
        ("line_sp", attended.reshape(split)),
    )

    def from_slots(matrix):
        folded = matrix.reshape(tp_n // copies, copies, source_local, slot_width)
        folded = jnp.sum(folded.astype(jnp.float32), axis=1)
        return folded.transpose(1, 0, 2).reshape(source_local, -1).astype(bf16)

    key_grad = from_slots(grads_back[:, :, :slot_width])
    value_grad = from_slots(grads_back[:, :, slot_width:])
    d_normed_s = matmul(key_grad, key_full.T) + matmul(value_grad, value_full.T)
    source_grad = norm_back(source_rows, source_gain, d_normed_s)
    d_normed_t = jnp.sum(target_back.astype(jnp.float32), axis=0)
    target_grad = out_cotangent.astype(jnp.float32) + norm_back(
        target_rows, target_gain, d_normed_t
    )
    attended_rows = attended_all.reshape(sp_n, tp_n, target_local, local_width)
    out_weight_grad = jnp.einsum(
        "stlw,tsld->wd", attended_rows, cot_all, preferred_element_type=jnp.float32
    )
    return (target_grad, source_grad, out_weight_grad)


def fused_kernel(sp_n, tp_n, *refs):
    target, source, tgain, sgain, qw, kw, vw, ow, cot = refs[:9]
    tgrad, sgrad, owg = refs[9:12]
    (t_rx, c_rx, rows, cotf, w_rx, ns, q_all, d_all, kv_tx, kv_rx, k2, v2, kvt) = refs[12:25]
    (qc, dc, p_buf, dp_buf, st, o_tx, o_rx, att, attb, dq_tx, dq_rx, qg) = refs[25:37]
    (dk, dv, g_tx, g_rx, gcat, tt, tp_rx, ts_tx, ts_rx, un, share) = refs[37:48]
    send_s, t_s, c_s, w_s, cz_s, q_s, d_s, kv_s = refs[48:56]
    st_s, o_s, att_s, dq_s, g_s, tp_s, ts_s = refs[56:63]
    f32, bf16 = jnp.float32, jnp.bfloat16
    z, me = lax.axis_index("sp"), lax.axis_index("tp")
    core = lax.rem(me, 2)
    t_loc, width = target.shape
    s_loc = source.shape[0]
    slab, local_width = w_rx.shape[2], qw.shape[1]
    heads = local_width // HEAD_DIM
    t_block = tp_n * t_loc
    lanes = heads * t_block
    s_block = tp_n * s_loc
    pairs = w_rx.shape[0]
    scale = HEAD_DIM ** (-0.5)

    def across(i):
        return i + 2 - 4 * lax.rem(i // 2, 2)

    def along(i):
        return i + 4 - 8 * lax.rem(i // 4, 2)

    mate = me + 1 - 2 * core
    zs = [lax.rem(z + k, sp_n) for k in range(1, sp_n)]
    ts = [lax.rem(me + k, tp_n) for k in range(1, tp_n)]

    barrier = pltpu.get_barrier_semaphore()
    for peer in zs:
        pl.semaphore_signal(barrier, inc=1, device_id=(peer, me), device_id_type=MESH)
    for peer in ts:
        pl.semaphore_signal(barrier, inc=1, device_id=(z, peer), device_id_type=MESH)

    sent = []

    def push(src, dst, sem, zz, i, when=None):
        one = pltpu.make_async_remote_copy(
            src_ref=src,
            dst_ref=dst,
            send_sem=send_s.at[len(sent)],
            recv_sem=sem,
            device_id=(zz, i),
            device_id_type=MESH,
        )
        sent.append((one, when))
        if when is None:
            one.start()
        else:
            pl.when(when)(lambda: one.start())

    def pull(ref, sem):
        pltpu.make_async_remote_copy(
            src_ref=ref,
            dst_ref=ref,
            send_sem=send_s.at[0],
            recv_sem=sem,
            device_id=(z, mate),
            device_id_type=MESH,
        ).wait_recv()

    def nt(a, b):
        return lax.dot_general(a, b, (((1,), (1,)), ((), ())), preferred_element_type=f32)

    def nn(a, b):
        return jnp.dot(a, b, preferred_element_type=f32)

    class Gather:
        def __init__(self, slot, sem, turn):
            self.slot, self.sem, self.turn = slot, sem, turn

        def start(self):
            for peer in (across(me), along(me), mate):
                push(self.slot(me), self.slot(me), self.sem(me), z, peer)

        def mid(self):
            for order, origin in enumerate((across(me), along(me))):
                piece, sem = self.slot(origin), self.sem(origin)
                pull(piece, sem)
                if order == self.turn:
                    push(piece, piece, sem, z, along(me) if order == 0 else across(me))
                push(piece, piece, sem, z, mate)

        def fin(self):
            origin = across(along(me))
            piece, sem = self.slot(origin), self.sem(origin)
            pull(piece, sem)
            push(piece, piece, sem, z, mate)

        def rest(self):
            for origin in (mate, across(mate), along(mate), across(along(mate))):
                pull(self.slot(origin), self.sem(origin))

    t_rx[me] = normalize(target[...], tgain[...])
    c_rx[z, me] = cot[...]
    pl.semaphore_wait(barrier, sp_n - 1 + tp_n - 1)

    t_all = Gather(lambda o: t_rx.at[o], lambda o: t_s.at[o], 0)
    c_own = Gather(lambda o: c_rx.at[z, o], lambda o: c_s.at[z * tp_n + o], 1)
    w_all = [
        Gather(lambda o, c=c: w_rx.at[c, o], lambda o, c=c: w_s.at[c * tp_n + o], c % 2)
        for c in range(pairs)
    ]
    c_far = [
        Gather(lambda o, p=p: c_rx.at[p, o], lambda o, p=p: c_s.at[p * tp_n + o], k % 2)
        for k, p in enumerate(zs)
    ]

    t_all.start()
    c_own.start()
    for peer in zs:
        push(c_rx.at[z, me], c_rx.at[z, me], cz_s.at[z], peer, me)
    for c in range(pairs):
        for j in range(2):
            head = 2 * c + j
            cols = slice(head * HEAD_DIM, (head + 1) * HEAD_DIM)
            both = jnp.concatenate([kw[:, cols], vw[:, cols]], axis=1)
            w_rx[c, me, :, j * 2 * HEAD_DIM : (j + 1) * 2 * HEAD_DIM] = both
    t_all.mid()
    c_own.mid()
    for c in range(pairs):
        w_all[c].start()
    step = min(s_loc, 32)
    for i in range(0, s_loc, step):
        ns[i : i + step] = normalize(source[i : i + step], sgain[...])
    t_all.fin()
    c_own.fin()
    t_all.rest()
    for o in range(tp_n):
        rows[o * t_loc : (o + 1) * t_loc] = t_rx[o]
    q_all[z] = (nn(rows[...], qw[...]).astype(bf16) * scale).astype(bf16)
    for peer in zs:
        push(q_all.at[z], q_all.at[z], q_s.at[z], peer, me)
    c_own.rest()
    for o in range(tp_n):
        cotf[z, o * t_loc : (o + 1) * t_loc] = c_rx[z, o]
    d_all[z] = nt(cotf[z], ow[...]).astype(bf16)
    for peer in zs:
        push(d_all.at[z], d_all.at[z], d_s.at[z], peer, me)

    def split_kv(c):
        w_all[c].rest()
        total = nn(ns[:, :slab], w_rx[c, 0])
        for o in range(1, tp_n):
            total += nn(ns[:, o * slab : (o + 1) * slab], w_rx[c, o])
        total = total.astype(bf16)
        for j in range(2):
            head = 2 * c + j
            part = total[:, j * 2 * HEAD_DIM : (j + 1) * 2 * HEAD_DIM]
            kv_tx[head] = part

            @pl.when(me == head)
            def _():
                kv_rx[head] = part

            push(kv_tx.at[head], kv_rx.at[me], kv_s.at[me], z, head, me != head)

    for c in range(pairs):
        w_all[c].mid()
        if c >= 1:
            w_all[c - 1].fin()
        if c >= 2:
            split_kv(c - 2)
    split_kv(pairs - 2)
    w_all[pairs - 1].fin()
    split_kv(pairs - 1)
    for k, p in enumerate(zs):
        pull(c_rx.at[p, me], cz_s.at[p])
        c_far[k].start()
    for p in zs:
        pull(q_all.at[p], q_s.at[p])
        pull(d_all.at[p], d_s.at[p])
    for b in range(sp_n):
        for h in range(heads):
            cols = slice(h * HEAD_DIM, (h + 1) * HEAD_DIM)
            qc[b, h * t_block : (h + 1) * t_block] = q_all[b, :, cols]
            dc[b, h * t_block : (h + 1) * t_block] = d_all[b, :, cols]
    for o in ts:
        pull(kv_rx.at[o], kv_s.at[o])
    for o in range(tp_n):
        part = kv_rx[o]
        k2[o * s_loc : (o + 1) * s_loc] = part[:, :HEAD_DIM]
        v2[o * s_loc : (o + 1) * s_loc] = part[:, HEAD_DIM:]
        kvt[:, o * s_loc : (o + 1) * s_loc] = part.astype(f32).T.astype(bf16)

    tile = 256
    steps = lanes // tile

    def first(b):
        def body(j, carry):
            cols = pl.ds(pl.multiple_of(j * tile, tile), tile)
            score = nt(k2[...], qc[b, cols])
            top = jnp.max(score, axis=0, keepdims=True)
            weight = jnp.exp(score - top)
            d_prob = nt(v2[...], dc[b, cols])
            total = jnp.sum(weight, axis=0, keepdims=True)
            inner = jnp.sum(weight * d_prob, axis=0, keepdims=True)
            p_buf[b, :, cols] = weight
            dp_buf[b, :, cols] = d_prob
            o_tx[b, :, cols] = nn(kvt[HEAD_DIM:], weight.astype(bf16)).astype(bf16)
            filler = jnp.zeros((5, tile), f32)
            st[b, z, :, cols] = jnp.concatenate([top, total, inner, filler], axis=0)
            return carry

        lax.fori_loop(0, steps, body, 0)
        for peer in zs:
            push(st.at[b, z], st.at[b, z], st_s.at[b * sp_n + z], peer, me)
        push(o_tx.at[b], o_rx.at[z], o_s.at[z], b, me, z != b)

    for b in range(sp_n):
        first(b)
        if b < len(c_far):
            c_far[b].mid()
        if b >= 1 and b - 1 < len(c_far):
            c_far[b - 1].fin()
    for k in range(sp_n - 1, len(c_far)):
        c_far[k].fin()

    def stats(b):
        tops = [st[b, s, 0:1] for s in range(sp_n)]
        row_max = functools.reduce(jnp.maximum, tops)
        lifts = [jnp.exp(top - row_max) for top in tops]
        total = sum(st[b, s, 1:2] * lifts[s] for s in range(sp_n))
        inner = sum(st[b, s, 2:3] * lifts[s] for s in range(sp_n))
        return row_max, lifts, total, inner / total

    def stats_in(b):
        for p in zs:
            pull(st.at[b, p], st_s.at[b * sp_n + p])

    def attend():
        for p in zs:
            pull(o_rx.at[p], o_s.at[p])
        row_max, lifts, total, inner = stats(z)
        o_rx[z] = o_tx[z]
        mixed = sum(o_rx[s].astype(f32) * lifts[s] for s in range(sp_n))
        att[z] = (mixed / total).astype(bf16)
        for peer in zs:
            push(att.at[z], att.at[z], att_s.at[z], peer, me)

    def second(i):
        b = z if i == sp_n - 1 else i + (i >= z).astype(jnp.int32)
        if i < sp_n - 1:
            stats_in(b)
        row_max, lifts, total, inner = stats(b)
        share[0:1] = jnp.exp(st[b, z, 0:1] - row_max) / total
        share[1:2] = inner

        def body(j, carry):
            cols = pl.ds(pl.multiple_of(j * tile, tile), tile)
            prob = p_buf[b, :, cols] * share[0:1, cols]
            d_score = (prob * (dp_buf[b, :, cols] - share[1:2, cols])).astype(bf16)
            prob = prob.astype(bf16)
            dv[...] += nn(prob, dc[b, cols])
            dk[...] += nn(d_score, qc[b, cols])
            dq_tx[b, :, cols] = nn(kvt[:HEAD_DIM], d_score).astype(bf16)
            return carry

        lax.fori_loop(0, steps, body, 0)
        if i < sp_n - 1:
            push(dq_tx.at[b], dq_rx.at[z], dq_s.at[z], b, me)

    dk[...] = jnp.zeros_like(dk)
    dv[...] = jnp.zeros_like(dv)
    for i in range(sp_n):
        second(i)
        if i == 0:
            stats_in(z)
            attend()

    for o in range(tp_n):
        part = slice(o * s_loc, (o + 1) * s_loc)
        g_tx[o] = jnp.concatenate([dk[part], dv[part]], axis=1).astype(bf16)
    for o in ts:
        push(g_tx.at[o], g_rx.at[me], g_s.at[me], z, o)
    g_rx[me] = g_tx[me]

    for p in zs:
        pull(dq_rx.at[p], dq_s.at[p])
    dq_rx[z] = dq_tx[z]
    summed = sum(dq_rx[s].astype(f32) for s in range(sp_n)) * scale
    summed = summed.T
    for h in range(heads):
        piece = summed[h * t_block : (h + 1) * t_block].astype(bf16)
        qg[:, h * HEAD_DIM : (h + 1) * HEAD_DIM] = piece

    wide = 512

    def terms(j, carry):
        cols = pl.ds(pl.multiple_of(j * wide, wide), wide)
        value = nt(qg[...], qw[cols])
        for o in range(tp_n):
            tt[o, :, cols] = value[o * t_loc : (o + 1) * t_loc].astype(bf16)
        return carry

    lax.fori_loop(0, width // wide, terms, 0)
    chips = tp_n // 2
    for c in range(chips):
        push(tt.at[2 * c + 1 - core], tp_rx.at[c], tp_s.at[c], z, mate)
    for c in range(chips):
        pull(tp_rx.at[c], tp_s.at[c])
        ts_tx[c] = (tt[2 * c + core].astype(f32) + tp_rx[c].astype(f32)).astype(bf16)
    for r, peer in enumerate((across(along(me)), across(me), along(me))):
        push(ts_tx.at[peer // 2], ts_rx.at[r], ts_s.at[r], z, peer)

    for k, p in enumerate(zs):
        c_far[k].rest()
        for o in range(tp_n):
            cotf[p, o * t_loc : (o + 1) * t_loc] = c_rx[p, o]
    for p in zs:
        pull(att.at[p], att_s.at[p])
    for b in range(sp_n):
        for h in range(heads):
            piece = att[b, :, h * t_block : (h + 1) * t_block]
            attb[b, h * HEAD_DIM : (h + 1) * HEAD_DIM] = piece

    def weight_grad(j, carry):
        cols = pl.ds(pl.multiple_of(j * tile, tile), tile)
        total = nn(attb[0], cotf[0, :, cols])
        for b in range(1, sp_n):
            total += nn(attb[b], cotf[b, :, cols])
        owg[:, cols] = total
        return carry

    lax.fori_loop(0, width // tile, weight_grad, 0)

    for o in ts:
        pull(g_rx.at[o], g_s.at[o])
    for o in range(tp_n):
        gcat[:, o * 2 * HEAD_DIM : (o + 1) * 2 * HEAD_DIM] = g_rx[o]

    def upstream(o, carry):
        cols = pl.ds(pl.multiple_of(o * slab, slab), slab)
        total = nt(gcat[:, : 4 * HEAD_DIM], w_rx[0, o])
        for c in range(1, pairs):
            total += nt(gcat[:, c * 4 * HEAD_DIM : (c + 1) * 4 * HEAD_DIM], w_rx[c, o])
        un[:, cols] = total
        return carry

    lax.fori_loop(0, tp_n, upstream, 0)
    for i in range(0, s_loc, step):
        part = slice(i, i + step)
        sgrad[part] = norm_back(source[part], sgain[...], un[part])

    mine = ts_tx[me // 2].astype(f32)
    for r in range(3):
        pull(ts_rx.at[r], ts_s.at[r])
    mine = mine + sum(ts_rx[r].astype(f32) for r in range(3))
    tgrad[...] = cot[...].astype(f32) + norm_back(target[...], tgain[...], mine)

    for one, when in sent:
        if when is None:
            one.wait_send()
        else:
            pl.when(when)(lambda one=one: one.wait_send())


def fused_body(
    target_rows,
    source_rows,
    target_gain,
    source_gain,
    query_weight,
    key_weight,
    value_weight,
    out_weight,
    out_cotangent,
):
    sp_n, tp_n = lax.axis_size("sp"), lax.axis_size("tp")
    t_loc, width = target_rows.shape
    s_loc = source_rows.shape[0]
    local_width = query_weight.shape[1]
    heads = local_width // HEAD_DIM
    t_block, s_block = tp_n * t_loc, tp_n * s_loc
    lanes = heads * t_block
    slab = key_weight.shape[0]
    pairs = KV_HEADS // 2
    two = 2 * HEAD_DIM
    f32, bf16 = jnp.float32, jnp.bfloat16
    vmem, sem = pltpu.VMEM, pltpu.SemaphoreType.DMA
    scratch = [
        vmem((tp_n, t_loc, width), bf16),
        vmem((sp_n, tp_n, t_loc, width), bf16),
        vmem((t_block, width), bf16),
        vmem((sp_n, t_block, width), bf16),
        vmem((pairs, tp_n, slab, 2 * two), bf16),
        vmem((s_loc, width), bf16),
        vmem((sp_n, t_block, local_width), bf16),
        vmem((sp_n, t_block, local_width), bf16),
        vmem((tp_n, s_loc, two), bf16),
        vmem((tp_n, s_loc, two), bf16),
        vmem((s_block, HEAD_DIM), bf16),
        vmem((s_block, HEAD_DIM), bf16),
        vmem((two, s_block), bf16),
        vmem((sp_n, lanes, HEAD_DIM), bf16),
        vmem((sp_n, lanes, HEAD_DIM), bf16),
        vmem((sp_n, s_block, lanes), f32),
        vmem((sp_n, s_block, lanes), f32),
        vmem((sp_n, sp_n, 8, lanes), f32),
        vmem((sp_n, HEAD_DIM, lanes), bf16),
        vmem((sp_n, HEAD_DIM, lanes), bf16),
        vmem((sp_n, HEAD_DIM, lanes), bf16),
        vmem((sp_n, local_width, t_block), bf16),
        vmem((sp_n, HEAD_DIM, lanes), bf16),
        vmem((sp_n, HEAD_DIM, lanes), bf16),
        vmem((t_block, local_width), bf16),
        vmem((s_block, HEAD_DIM), f32),
        vmem((s_block, HEAD_DIM), f32),
        vmem((tp_n, s_loc, two), bf16),
        vmem((tp_n, s_loc, two), bf16),
        vmem((s_loc, tp_n * two), bf16),
        vmem((tp_n, t_loc, width), bf16),
        vmem((tp_n // 2, t_loc, width), bf16),
        vmem((tp_n // 2, t_loc, width), bf16),
        vmem((3, t_loc, width), bf16),
        vmem((s_loc, width), f32),
        vmem((8, lanes), f32),
        sem((256,)),
        sem((tp_n,)),
        sem((sp_n * tp_n,)),
        sem((pairs * tp_n,)),
        sem((sp_n,)),
        sem((sp_n,)),
        sem((sp_n,)),
        sem((tp_n,)),
        sem((sp_n * sp_n,)),
        sem((sp_n,)),
        sem((sp_n,)),
        sem((sp_n,)),
        sem((tp_n,)),
        sem((tp_n // 2,)),
        sem((3,)),
    ]
    return pl.pallas_call(
        functools.partial(fused_kernel, sp_n, tp_n),
        out_shape=[
            jax.ShapeDtypeStruct((t_loc, width), f32),
            jax.ShapeDtypeStruct((s_loc, width), f32),
            jax.ShapeDtypeStruct((local_width, width), f32),
        ],
        in_specs=[pl.BlockSpec(memory_space=pltpu.VMEM)] * 9,
        out_specs=[pl.BlockSpec(memory_space=pltpu.VMEM)] * 3,
        scratch_shapes=scratch,
        compiler_params=pltpu.CompilerParams(
            collective_id=0,
            has_side_effects=True,
            vmem_limit_bytes=67043328,
        ),
    )(
        target_rows,
        source_rows,
        target_gain[None],
        source_gain[None],
        query_weight,
        key_weight,
        value_weight,
        out_weight,
        out_cotangent,
    )


def choose(*args):
    square = lax.axis_size("tp") == 8 and KV_HEADS == 8
    lanes = lax.axis_size("tp") * args[0].shape[0] * args[4].shape[1] // HEAD_DIM
    if square and lanes % 256 == 0:
        return fused_body(*args)
    return body(*args)


def solution(mesh):
    return jax.shard_map(
        choose,
        mesh=mesh,
        in_specs=(
            P(("sp", "tp"), None),
            P(("sp", "tp"), None),
            P(),
            P(),
            P(None, "tp"),
            P("tp", None),
            P("tp", None),
            P("tp", None),
            P(("sp", "tp"), None),
        ),
        out_specs=(P(("sp", "tp"), None), P(("sp", "tp"), None), P("tp", None)),
        check_vma=False,
    )
```

```python
import functools

import jax
import jax.numpy as jnp
from jax import lax
from jax.experimental import pallas as pl
from jax.experimental.pallas import tpu as pltpu
from jax.sharding import PartitionSpec as P

HEAD_DIM = 64
KV_HEADS = 8
EPSILON = 1e-06
MESH = pl.DeviceIdType.MESH


def normalize(matrix, gain_vector):
    widened = matrix.astype(jnp.float32)
    factor = lax.rsqrt(jnp.mean(widened * widened, axis=-1, keepdims=True) + EPSILON)
    return (widened * factor * gain_vector).astype(jnp.bfloat16)


def norm_back(matrix, gain_vector, upstream):
    widened = matrix.astype(jnp.float32)
    factor = lax.rsqrt(jnp.mean(widened * widened, axis=-1, keepdims=True) + EPSILON)
    weighted = upstream * gain_vector
    inner_sum = jnp.mean(weighted * widened, axis=-1, keepdims=True)
    return factor * weighted - widened * factor**3 * inner_sum


def exchange_kernel(kinds, sp_n, tp_n, *refs):
    count = len(kinds)
    ins, outs = refs[:count], refs[count : 2 * count]
    send_sems, recv_sems = refs[2 * count : 3 * count], refs[3 * count :]
    sp_me, tp_me = lax.axis_index("sp"), lax.axis_index("tp")
    sizes, places = {"sp": sp_n, "tp": tp_n}, {"sp": sp_me, "tp": tp_me}

    def address(axis, peer):
        return (peer, tp_me) if axis == "sp" else (sp_me, peer)

    axes = sorted({kind.split("_")[1] for kind in kinds})
    barrier = pltpu.get_barrier_semaphore()
    for axis in axes:
        for k in range(1, sizes[axis]):
            peer = lax.rem(places[axis] + k, sizes[axis])
            pl.semaphore_signal(barrier, inc=1, device_id=address(axis, peer), device_id_type=MESH)
    pl.semaphore_wait(barrier, sum(sizes[axis] - 1 for axis in axes))

    def copy(i, axis, source, slot, k, peer):
        return pltpu.make_async_remote_copy(
            src_ref=source,
            dst_ref=outs[i].at[slot],
            send_sem=send_sems[i].at[k],
            recv_sem=recv_sems[i].at[slot],
            device_id=address(axis, peer),
            device_id_type=MESH,
        )

    sent = []
    used = [0] * count

    def send(i, axis, source, target, recv, peer, keep=True):
        one = pltpu.make_async_remote_copy(
            src_ref=source,
            dst_ref=target,
            send_sem=send_sems[i].at[used[i]],
            recv_sem=recv_sems[i].at[recv],
            device_id=address(axis, peer),
            device_id_type=MESH,
        )
        used[i] += 1
        one.start()
        if keep:
            sent.append(one)
        return one

    def arrived(i, axis, target, recv):
        pltpu.make_async_remote_copy(
            src_ref=target,
            dst_ref=target,
            send_sem=send_sems[i].at[0],
            recv_sem=recv_sems[i].at[recv],
            device_id=address(axis, lax.rem(places[axis] + 1, sizes[axis])),
            device_id_type=MESH,
        ).wait_recv()

    square = tp_n == 8
    partner = tp_me + 1 - 2 * lax.rem(tp_me, 2)

    def across(index):
        return index + 2 - 4 * lax.rem(index // 2, 2)

    def along(index):
        return index + 4 - 8 * lax.rem(index // 4, 2)

    def relatives(index):
        if square:
            return [across(index), along(index)]
        return [lax.rem(index + 2 * k, tp_n) for k in range(1, tp_n // 2)]

    def forward(i, c, origin):
        chunks = ins[i].shape[0]
        piece, recv = outs[i].at[origin, c], origin * chunks + c
        arrived(i, "tp", piece, recv)
        send(i, "tp", piece, piece, recv, partner)
        return piece, recv

    line_sent = []
    depth = max([ins[i].shape[0] for i in range(count) if kinds[i] == "pair_tp"], default=0)
    for c in range(depth):
        for i, kind in enumerate(kinds):
            if kind == "pair_tp" and c < ins[i].shape[0]:
                chunks = ins[i].shape[0]
                for peer in relatives(tp_me) + [partner]:
                    piece = outs[i].at[tp_me, c]
                    send(i, "tp", ins[i].at[c], piece, tp_me * chunks + c, peer)
    for i, kind in enumerate(kinds):
        mode, axis = kind.split("_")
        n, me = sizes[axis], places[axis]
        if mode == "line":
            for step in (1, -1):
                inside = (me < n - 1) if step == 1 else (me > 0)
                for c in range(ins[i].shape[0]):
                    line_sent.append((i, inside, used[i], me, c))
                    recv = me * ins[i].shape[0] + c

                    @pl.when(inside)
                    def _():
                        piece = outs[i].at[me, c]
                        send(i, axis, ins[i].at[c], piece, recv, me + step, keep=False)
        elif mode != "pair":
            for k in range(1, n):
                peer = lax.rem(me + k, n)
                source = ins[i] if mode == "gather" else ins[i].at[peer]
                send(i, axis, source, outs[i].at[me], me, peer)
    for i, kind in enumerate(kinds):
        mode, axis = kind.split("_")
        me = places[axis]
        outs[i][me] = ins[i][me] if mode == "swap" else ins[i][...]

    def line_step(i, far, c):
        n, me = sp_n, sp_me
        chunks = ins[i].shape[0]
        for step in (1, -1):
            origin = me - step * far
            valid = (origin >= 0) if step == 1 else (origin <= n - 1)
            onward = (valid & (me < n - 1)) if step == 1 else (valid & (me > 0))

            @pl.when(valid)
            def _():
                arrived(i, "sp", outs[i].at[origin, c], origin * chunks + c)

            if far < n - 1:
                line_sent.append((i, onward, used[i], origin, c))

                @pl.when(onward)
                def _():
                    piece = outs[i].at[origin, c]
                    recv = origin * chunks + c
                    send(i, "sp", piece, piece, recv, me + step, keep=False)

    def pair_step(i, c):
        me = tp_me
        chunks = ins[i].shape[0]
        for order, origin in enumerate(relatives(me)):
            piece, recv = forward(i, c, origin)
            if square and order == (i + c) % 2:
                send(i, "tp", piece, piece, recv, along(me) if order == 0 else across(me))

    lines = [i for i in range(count) if kinds[i] == "line_sp"]
    pairs = [i for i in range(count) if kinds[i] == "pair_tp"]
    for turn in range(max(depth, sp_n - 1 if lines else 0)):
        for i in pairs:
            if turn < ins[i].shape[0]:
                pair_step(i, turn)
        for i in lines:
            if turn + 1 < sp_n:
                for c in range(ins[i].shape[0]):
                    line_step(i, turn + 1, c)
    if square:
        for c in range(depth):
            for i in pairs:
                if c < ins[i].shape[0]:
                    forward(i, c, across(along(tp_me)))
    for i, kind in enumerate(kinds):
        mode, axis = kind.split("_")
        n, me = sizes[axis], places[axis]
        if mode == "pair":
            chunks = ins[i].shape[0]
            others = relatives(partner) + ([across(along(partner))] if square else [])
            for origin in [partner] + others:
                for c in range(chunks):
                    arrived(i, axis, outs[i].at[origin, c], origin * chunks + c)
        elif mode != "line":
            for k in range(1, n):
                origin = lax.rem(me + n - k, n)
                arrived(i, axis, outs[i].at[origin], origin)
    for one in sent:
        one.wait_send()
    for i, happened, slot, origin, c in line_sent:

        @pl.when(happened)
        def _():
            pltpu.make_async_remote_copy(
                src_ref=outs[i].at[origin, c],
                dst_ref=outs[i].at[origin, c],
                send_sem=send_sems[i].at[slot],
                recv_sem=recv_sems[i].at[0],
                device_id=address("sp", lax.rem(sp_me + 1, sp_n)),
                device_id_type=MESH,
            ).wait_send()


def exchange(collective_id, *parts):
    sp_n, tp_n = lax.axis_size("sp"), lax.axis_size("tp")
    kinds = tuple(kind for kind, array in parts)
    arrays = [array for kind, array in parts]
    shapes, sends, recvs = [], [], []
    for kind, array in parts:
        mode, axis = kind.split("_")
        n = sp_n if axis == "sp" else tp_n
        shape = array.shape if mode == "swap" else (n,) + array.shape
        shapes.append(jax.ShapeDtypeStruct(shape, array.dtype))
        chunks = array.shape[0] if mode in ("pair", "line") else 1
        sends.append(pltpu.SemaphoreType.DMA(((2 * n + 8) * chunks,)))
        recvs.append(pltpu.SemaphoreType.DMA((n * chunks,)))
    return pl.pallas_call(
        functools.partial(exchange_kernel, kinds, sp_n, tp_n),
        out_shape=shapes,
        in_specs=[pl.BlockSpec(memory_space=pltpu.VMEM)] * len(parts),
        out_specs=[pl.BlockSpec(memory_space=pltpu.VMEM)] * len(parts),
        scratch_shapes=sends + recvs,
        compiler_params=pltpu.CompilerParams(
            collective_id=collective_id,
            has_side_effects=True,
            vmem_limit_bytes=56 * 1024 * 1024,
        ),
    )(*arrays)


def matmul(left, right):
    return jnp.dot(left, right, preferred_element_type=jnp.float32)


def einsum(text, left, right):
    return jnp.einsum(text, left, right, preferred_element_type=jnp.float32)


def body(
    target_rows,
    source_rows,
    target_gain,
    source_gain,
    query_weight,
    key_weight,
    value_weight,
    out_weight,
    out_cotangent,
):
    sp_n, tp_n = lax.axis_size("sp"), lax.axis_size("tp")
    width = target_rows.shape[1]
    local_width = query_weight.shape[1]
    local_heads = local_width // HEAD_DIM
    slot_heads = max(1, KV_HEADS // tp_n)
    copies = max(1, tp_n // KV_HEADS)
    per_slot = local_heads // slot_heads
    slot_width = slot_heads * HEAD_DIM
    score_scale = HEAD_DIM ** (-0.5)
    bf16 = jnp.bfloat16

    normed_t = normalize(target_rows, target_gain)
    normed_s = normalize(source_rows, source_gain)
    source_local = normed_s.shape[0]
    target_local = normed_t.shape[0]
    target_block = tp_n * target_local
    source_block = tp_n * source_local

    rows_in, cot_in = exchange(
        0,
        ("pair_tp", normed_t[None]),
        ("pair_tp", out_cotangent[None]),
    )
    queries = matmul(rows_in.reshape(target_block, width), query_weight).astype(bf16)
    d_attended = matmul(cot_in.reshape(target_block, width), out_weight.T).astype(bf16)
    halves = (2, key_weight.shape[0] // 2, key_weight.shape[1])
    split = (2, target_block // 2, local_width)
    key_full, value_full, all_queries, all_grads, cot_column = exchange(
        1,
        ("pair_tp", key_weight.reshape(halves)),
        ("pair_tp", value_weight.reshape(halves)),
        ("line_sp", queries.reshape(split)),
        ("line_sp", d_attended.reshape(split)),
        ("line_sp", out_cotangent[None]),
    )
    key_full = key_full.reshape(width, -1)
    value_full = value_full.reshape(width, -1)
    key_own = matmul(normed_s, key_full).astype(bf16)
    value_own = matmul(normed_s, value_full).astype(bf16)

    def to_slots(matrix):
        split = matrix.reshape(source_local, tp_n // copies, 1, slot_width)
        spread = jnp.broadcast_to(split, (source_local, tp_n // copies, copies, slot_width))
        return spread.reshape(source_local, tp_n, slot_width).transpose(1, 0, 2)

    slots = jnp.concatenate([to_slots(key_own), to_slots(value_own)], axis=2)
    (kv_block,) = exchange(2, ("swap_tp", slots))
    whole_rows = sp_n * target_block
    kv_block = kv_block.reshape(source_block, 2, slot_heads, HEAD_DIM)
    keys, values = kv_block[:, 0], kv_block[:, 1]
    head_shape = (whole_rows, slot_heads, per_slot, HEAD_DIM)
    query_view = all_queries.reshape(head_shape)
    grad_view = all_grads.reshape(head_shape)

    scores = einsum("tgqd,sgd->gqts", query_view, keys) * score_scale
    part_max = jnp.max(scores, axis=-1)
    weights = jnp.exp(scores - part_max[..., None])
    part_total = jnp.sum(weights, axis=-1)
    d_probs = einsum("tgqd,sgd->gqts", grad_view, values)
    part_delta = jnp.sum(weights * d_probs, axis=-1)
    part_sum = einsum("gqts,sgd->tgqd", weights.astype(bf16), values)
    stats = jnp.stack([part_max, part_total, part_delta]).reshape(3 * local_heads, whole_rows)
    (all_stats,) = exchange(3, ("gather_sp", stats))
    all_stats = all_stats.reshape(sp_n, 3, slot_heads, per_slot, whole_rows)
    row_max = jnp.max(all_stats[:, 0], axis=0)
    rescale = jnp.exp(all_stats[:, 0] - row_max)
    total = jnp.sum(all_stats[:, 1] * rescale, axis=0)
    delta = jnp.sum(all_stats[:, 2] * rescale, axis=0) / total
    local_scale = jnp.exp(part_max - row_max) / total

    attended_part = part_sum * local_scale.transpose(2, 0, 1)[..., None]
    attended_part = attended_part.reshape(sp_n, target_block, local_width).astype(bf16)
    probs = weights * local_scale[..., None]
    d_scores = (probs * (d_probs - delta[..., None])).astype(bf16)
    value_sum = einsum("gqts,tgqd->sgd", probs.astype(bf16), grad_view)
    key_sum = einsum("gqts,tgqd->sgd", d_scores, query_view) * score_scale
    d_query = einsum("gqts,sgd->tgqd", d_scores, keys) * score_scale
    d_query = d_query.reshape(sp_n, target_block, local_width).astype(bf16)
    grads = jnp.concatenate(
        [key_sum.reshape(source_block, slot_width), value_sum.reshape(source_block, slot_width)],
        axis=1,
    )
    grads = grads.reshape(tp_n, source_local, 2 * slot_width).astype(bf16)
    query_terms, attended_terms, grads_back, cot_all = exchange(
        4,
        ("swap_sp", d_query),
        ("swap_sp", attended_part),
        ("swap_tp", grads),
        ("pair_tp", cot_column.reshape(sp_n, target_local, width)),
    )
    query_grad = jnp.sum(query_terms.astype(jnp.float32), axis=0).astype(bf16)
    attended = jnp.sum(attended_terms.astype(jnp.float32), axis=0).astype(bf16)

    target_terms = matmul(query_grad, query_weight.T).astype(bf16)
    target_back, attended_all = exchange(
        5,
        ("swap_tp", target_terms.reshape(tp_n, target_local, width)),
        ("line_sp", attended.reshape(split)),
    )

    def from_slots(matrix):
        folded = matrix.reshape(tp_n // copies, copies, source_local, slot_width)
        folded = jnp.sum(folded.astype(jnp.float32), axis=1)
        return folded.transpose(1, 0, 2).reshape(source_local, -1).astype(bf16)

    key_grad = from_slots(grads_back[:, :, :slot_width])
    value_grad = from_slots(grads_back[:, :, slot_width:])
    d_normed_s = matmul(key_grad, key_full.T) + matmul(value_grad, value_full.T)
    source_grad = norm_back(source_rows, source_gain, d_normed_s)
    d_normed_t = jnp.sum(target_back.astype(jnp.float32), axis=0)
    target_grad = out_cotangent.astype(jnp.float32) + norm_back(
        target_rows, target_gain, d_normed_t
    )
    attended_rows = attended_all.reshape(sp_n, tp_n, target_local, local_width)
    out_weight_grad = jnp.einsum(
        "stlw,tsld->wd", attended_rows, cot_all, preferred_element_type=jnp.float32
    )
    return (target_grad, source_grad, out_weight_grad)


def fused_kernel(sp_n, tp_n, *refs):
    loads, stores = refs[:9], refs[9:12]
    target, source, tgain, sgain, qw, kw, vw, ow = refs[12:20]
    tgrad, sgrad, owg = refs[20:23]
    (t_rx, c_rx, rows, cotf, w_rx, ns, q_all, d_all, kv_tx, kv_rx, k2, v2, kvt) = refs[23:36]
    (qc, dc, p_buf, dp_buf, st, o_tx, o_rx, att, attb, dq_tx, dq_rx, qg) = refs[36:48]
    (dk, dv, g_tx, g_rx, gcat, tt, tp_rx, ts_tx, ts_rx, un) = refs[48:58]
    send_s, t_s, c_s, w_s, far_s, cz_s, q_s, d_s, kv_s = refs[58:67]
    st_s, o_s, att_s, dq_s, g_s, tp_s, ts_s, load_s, store_s = refs[67:76]
    f32, bf16 = jnp.float32, jnp.bfloat16
    z, me = lax.axis_index("sp"), lax.axis_index("tp")
    core = lax.rem(me, 2)
    t_loc, width = target.shape
    s_loc = source.shape[0]
    slab, local_width = w_rx.shape[2], qw.shape[1]
    heads = local_width // HEAD_DIM
    t_block = tp_n * t_loc
    lanes = heads * t_block
    s_block = tp_n * s_loc
    pairs = w_rx.shape[0]
    scale = HEAD_DIM ** (-0.5)

    def across(i):
        return i + 2 - 4 * lax.rem(i // 2, 2)

    def along(i):
        return i + 4 - 8 * lax.rem(i // 4, 2)

    mate = me + 1 - 2 * core
    zs = [lax.rem(z + k, sp_n) for k in range(1, sp_n)]
    ts = [lax.rem(me + k, tp_n) for k in range(1, tp_n)]

    barrier = pltpu.get_barrier_semaphore()
    for peer in zs:
        pl.semaphore_signal(barrier, inc=1, device_id=(peer, me), device_id_type=MESH)
    for peer in ts:
        pl.semaphore_signal(barrier, inc=1, device_id=(z, peer), device_id_type=MESH)

    sent = []

    def push(src, dst, sem, zz, i, when=None):
        one = pltpu.make_async_remote_copy(
            src_ref=src,
            dst_ref=dst,
            send_sem=send_s.at[len(sent)],
            recv_sem=sem,
            device_id=(zz, i),
            device_id_type=MESH,
        )
        sent.append((one, when))
        if when is None:
            one.start()
        else:
            pl.when(when)(lambda: one.start())

    def pull(ref, sem):
        pltpu.make_async_remote_copy(
            src_ref=ref,
            dst_ref=ref,
            send_sem=send_s.at[0],
            recv_sem=sem,
            device_id=(z, mate),
            device_id_type=MESH,
        ).wait_recv()

    kept = (target, source, tgain, sgain, qw, kw, vw, ow, c_rx.at[z, me])
    copies = [pltpu.make_async_copy(a, b, load_s.at[i]) for i, (a, b) in enumerate(zip(loads, kept))]
    for i in (0, 2, 8, 5, 6, 1, 3, 4, 7):
        copies[i].start()

    def store(i, a):
        one = pltpu.make_async_copy(a, stores[i], store_s.at[i])
        one.start()
        return one

    def nt(a, b):
        return lax.dot_general(a, b, (((1,), (1,)), ((), ())), preferred_element_type=f32)

    def nn(a, b):
        return jnp.dot(a, b, preferred_element_type=f32)

    class Gather:
        def __init__(self, slot, sem, far, depth):
            self.slot, self.sem, self.far, self.depth = slot, sem, far, depth

        def start(self):
            for peer in (across(me), along(me), mate):
                push(self.slot(me), self.slot(me), self.sem(me), z, peer)

        def half(self, origin, order):
            return self.slot(origin).at[self.depth[order] : self.depth[order + 1]]

        def mid(self):
            for order, origin in enumerate((across(me), along(me))):
                pull(self.slot(origin), self.sem(origin))
                piece = self.half(origin, order)
                push(piece, piece, self.far(order), z, along(me) if order == 0 else across(me))
            for origin in (across(me), along(me)):
                push(self.slot(origin), self.slot(origin), self.sem(origin), z, mate)

        def fin(self):
            origin = across(along(me))
            for order in range(2):
                pull(self.half(origin, order), self.far(order))
            push(self.slot(origin), self.slot(origin), self.sem(origin), z, mate)

        def rest(self):
            for origin in (mate, across(mate), along(mate), across(along(mate))):
                pull(self.slot(origin), self.sem(origin))

    copies[0].wait()
    copies[2].wait()
    t_rx[me] = normalize(target[...], tgain[...])
    copies[8].wait()
    pl.semaphore_wait(barrier, sp_n - 1 + tp_n - 1)

    some, more = (0, t_loc // 2 // 8 * 8, t_loc), (0, slab // 2, slab)
    t_all = Gather(lambda o: t_rx.at[o], lambda o: t_s.at[o], lambda k: far_s.at[k], some)
    c_all = [
        Gather(
            lambda o, p=p: c_rx.at[p, o],
            lambda o, p=p: c_s.at[p * tp_n + o],
            lambda k, n=n: far_s.at[2 * n + 2 + k],
            some,
        )
        for n, p in enumerate([z] + zs)
    ]
    c_own, c_far = c_all[0], c_all[1:]
    w_all = [
        Gather(
            lambda o, c=c: w_rx.at[c, o],
            lambda o, c=c: w_s.at[c * tp_n + o],
            lambda k, c=c: far_s.at[2 * (sp_n + 1 + c) + k],
            more,
        )
        for c in range(pairs)
    ]

    t_all.start()
    c_own.start()
    for peer in zs:
        push(c_rx.at[z, me], c_rx.at[z, me], cz_s.at[z], peer, me)
    copies[5].wait()
    copies[6].wait()

    def weave(c):
        for j in range(2):
            head = 2 * c + j
            cols = slice(head * HEAD_DIM, (head + 1) * HEAD_DIM)
            both = jnp.concatenate([kw[:, cols], vw[:, cols]], axis=1)
            w_rx[c, me, :, j * 2 * HEAD_DIM : (j + 1) * 2 * HEAD_DIM] = both

    for c in range(pairs):
        weave(c)
    w_all[0].start()
    copies[1].wait()
    copies[3].wait()
    step = min(s_loc, 32)
    for i in range(0, s_loc, step):
        ns[i : i + step] = normalize(source[i : i + step], sgain[...])
    t_all.mid()
    c_own.mid()
    w_all[1].start()
    w_all[0].mid()
    w_all[2].start()
    t_all.fin()
    c_own.fin()
    t_all.rest()
    for o in range(tp_n):
        rows[o * t_loc : (o + 1) * t_loc] = t_rx[o]
    copies[4].wait()
    q_all[z] = (nn(rows[...], qw[...]).astype(bf16) * scale).astype(bf16)
    for peer in zs:
        push(q_all.at[z], q_all.at[z], q_s.at[z], peer, me)
    w_all[1].mid()
    w_all[3].start()
    c_own.rest()
    for o in range(tp_n):
        cotf[z, o * t_loc : (o + 1) * t_loc] = c_rx[z, o]
    copies[7].wait()
    d_all[z] = nt(cotf[z], ow[...]).astype(bf16)
    for peer in zs:
        push(d_all.at[z], d_all.at[z], d_s.at[z], peer, me)

    def split_kv(c):
        w_all[c].rest()
        total = nn(ns[:, :slab], w_rx[c, 0])
        for o in range(1, tp_n):
            total += nn(ns[:, o * slab : (o + 1) * slab], w_rx[c, o])
        total = total.astype(bf16)
        for j in range(2):
            head = 2 * c + j
            part = total[:, j * 2 * HEAD_DIM : (j + 1) * 2 * HEAD_DIM]
            kv_tx[head] = part

            @pl.when(me == head)
            def _():
                kv_rx[head] = part

            push(kv_tx.at[head], kv_rx.at[me], kv_s.at[me], z, head, me != head)

    w_all[0].fin()
    split_kv(0)
    for c in range(2, pairs):
        w_all[c].mid()
        w_all[c - 1].fin()
        split_kv(c - 1)
    w_all[pairs - 1].fin()
    split_kv(pairs - 1)
    for k, p in enumerate(zs):
        pull(c_rx.at[p, me], cz_s.at[p])
        c_far[k].start()
    for p in zs:
        pull(q_all.at[p], q_s.at[p])
        pull(d_all.at[p], d_s.at[p])
    for b in range(sp_n):
        for h in range(heads):
            cols = slice(h * HEAD_DIM, (h + 1) * HEAD_DIM)
            qc[b, h * t_block : (h + 1) * t_block] = q_all[b, :, cols]
            dc[b, h * t_block : (h + 1) * t_block] = d_all[b, :, cols]
    for o in ts:
        pull(kv_rx.at[o], kv_s.at[o])
    for o in range(tp_n):
        part = kv_rx[o]
        k2[o * s_loc : (o + 1) * s_loc] = part[:, :HEAD_DIM]
        v2[o * s_loc : (o + 1) * s_loc] = part[:, HEAD_DIM:]
        kvt[:, o * s_loc : (o + 1) * s_loc] = part.astype(f32).T.astype(bf16)

    groups = lanes // 128

    def fold(op, x, n=4):
        size = x.shape[0] // n
        parts = [
            op(x[i * size : (i + 1) * size].reshape(size // 8, 8, x.shape[1]), axis=0)
            for i in range(n)
        ]
        both = jnp.maximum if op is jnp.max else jnp.add
        return op(functools.reduce(both, parts), axis=0, keepdims=True)

    def line(x):
        return jnp.concatenate([x[g : g + 1] for g in range(groups)], axis=1)

    def first(b):
        score = nt(k2[...], qc[b])
        top = fold(jnp.max, score)
        weight = jnp.exp(score - top)
        d_prob = nt(v2[...], dc[b])
        total = fold(jnp.sum, weight)
        inner = fold(jnp.sum, weight * d_prob)
        p_buf[b] = weight
        dp_buf[b] = d_prob
        o_tx[b] = nn(kvt[HEAD_DIM:], weight.astype(bf16)).astype(bf16)
        for k, value in enumerate((top, total, inner)):
            for g in range(groups):
                row = 8 * k + g
                st[b, z, row : row + 1] = value[:, g * 128 : (g + 1) * 128]
        for peer in zs:
            push(st.at[b, z], st.at[b, z], st_s.at[b * sp_n + z], peer, me)
        push(o_tx.at[b], o_rx.at[z], o_s.at[z], b, me, z != b)

    for b in range(sp_n):
        st[b, z] = jnp.zeros((24, 128), f32)
    for b in range(sp_n):
        first(b)
        if b < len(c_far):
            c_far[b].mid()
        if b >= 1 and b - 1 < len(c_far):
            c_far[b - 1].fin()
    for k in range(sp_n - 1, len(c_far)):
        c_far[k].fin()

    def stats(b):
        tops = [st[b, s, 0:8] for s in range(sp_n)]
        row_max = functools.reduce(jnp.maximum, tops)
        lifts = [jnp.exp(top - row_max) for top in tops]
        total = sum(st[b, s, 8:16] * lifts[s] for s in range(sp_n))
        inner = sum(st[b, s, 16:24] * lifts[s] for s in range(sp_n))
        return row_max, lifts, total, inner / total

    def stats_in(b):
        for p in zs:
            pull(st.at[b, p], st_s.at[b * sp_n + p])

    def attend():
        for p in zs:
            pull(o_rx.at[p], o_s.at[p])
        row_max, lifts, total, inner = stats(z)
        o_rx[z] = o_tx[z]
        mixed = sum(o_rx[s].astype(f32) * line(lifts[s]) for s in range(sp_n))
        att[z] = (mixed / line(total)).astype(bf16)

    def second(i):
        b = z if i == sp_n - 1 else i + (i >= z).astype(jnp.int32)
        if i < sp_n - 1:
            stats_in(b)
        row_max, lifts, total, inner = stats(b)
        share = line(jnp.exp(st[b, z, 0:8] - row_max) / total)
        prob = p_buf[b] * share
        d_score = (prob * (dp_buf[b] - line(inner))).astype(bf16)
        prob = prob.astype(bf16)
        dv[...] += nn(prob, dc[b])
        dk[...] += nn(d_score, qc[b])
        dq_tx[b] = nn(kvt[:HEAD_DIM], d_score).astype(bf16)
        if i < sp_n - 1:
            push(dq_tx.at[b], dq_rx.at[z], dq_s.at[z], b, me)

    dk[...] = jnp.zeros_like(dk)
    dv[...] = jnp.zeros_like(dv)
    for i in range(sp_n):
        second(i)
        if i == 0:
            stats_in(z)
            attend()
        if i == max(0, sp_n - 2):
            for peer in zs:
                push(att.at[z], att.at[z], att_s.at[z], peer, me)

    for o in range(tp_n):
        part = slice(o * s_loc, (o + 1) * s_loc)
        g_tx[o] = jnp.concatenate([dk[part], dv[part]], axis=1).astype(bf16)
    for o in ts:
        push(g_tx.at[o], g_rx.at[me], g_s.at[me], z, o)
    g_rx[me] = g_tx[me]

    for p in zs:
        pull(dq_rx.at[p], dq_s.at[p])
    dq_rx[z] = dq_tx[z]
    summed = sum(dq_rx[s].astype(f32) for s in range(sp_n)) * scale
    summed = summed.T
    for h in range(heads):
        piece = summed[h * t_block : (h + 1) * t_block].astype(bf16)
        qg[:, h * HEAD_DIM : (h + 1) * HEAD_DIM] = piece

    wide = 512

    def terms(j, carry):
        cols = pl.ds(pl.multiple_of(j * wide, wide), wide)
        value = nt(qg[...], qw[cols])
        for o in range(tp_n):
            tt[o, :, cols] = value[o * t_loc : (o + 1) * t_loc].astype(bf16)
        return carry

    lax.fori_loop(0, width // wide, terms, 0)
    chips = tp_n // 2
    for c in range(chips):
        push(tt.at[2 * c + 1 - core], tp_rx.at[c], tp_s.at[c], z, mate)
    for c in range(chips):
        pull(tp_rx.at[c], tp_s.at[c])
        ts_tx[c] = (tt[2 * c + core].astype(f32) + tp_rx[c].astype(f32)).astype(bf16)
    for r, peer in enumerate((across(along(me)), across(me), along(me))):
        push(ts_tx.at[peer // 2], ts_rx.at[r], ts_s.at[r], z, peer)

    for k, p in enumerate(zs):
        c_far[k].rest()
        for o in range(tp_n):
            cotf[p, o * t_loc : (o + 1) * t_loc] = c_rx[p, o]
    for p in zs:
        pull(att.at[p], att_s.at[p])
    for b in range(sp_n):
        for h in range(heads):
            piece = att[b, :, h * t_block : (h + 1) * t_block]
            attb[b, h * HEAD_DIM : (h + 1) * HEAD_DIM] = piece

    tile = 256

    def weight_grad(j, carry):
        cols = pl.ds(pl.multiple_of(j * tile, tile), tile)
        total = nn(attb[0], cotf[0, :, cols])
        for b in range(1, sp_n):
            total += nn(attb[b], cotf[b, :, cols])
        owg[:, cols] = total
        return carry

    lax.fori_loop(0, width // tile, weight_grad, 0)
    done = [store(2, owg)]

    for o in ts:
        pull(g_rx.at[o], g_s.at[o])
    for o in range(tp_n):
        gcat[:, o * 2 * HEAD_DIM : (o + 1) * 2 * HEAD_DIM] = g_rx[o]

    def upstream(o, carry):
        cols = pl.ds(pl.multiple_of(o * slab, slab), slab)
        total = nt(gcat[:, : 4 * HEAD_DIM], w_rx[0, o])
        for c in range(1, pairs):
            total += nt(gcat[:, c * 4 * HEAD_DIM : (c + 1) * 4 * HEAD_DIM], w_rx[c, o])
        un[:, cols] = total
        return carry

    lax.fori_loop(0, tp_n, upstream, 0)
    for i in range(0, s_loc, step):
        part = slice(i, i + step)
        sgrad[part] = norm_back(source[part], sgain[...], un[part])
    done.append(store(1, sgrad))

    mine = ts_tx[me // 2].astype(f32)
    for r in range(3):
        pull(ts_rx.at[r], ts_s.at[r])
    mine = mine + sum(ts_rx[r].astype(f32) for r in range(3))
    tgrad[...] = c_rx[z, me].astype(f32) + norm_back(target[...], tgain[...], mine)
    done.append(store(0, tgrad))

    for one, when in sent:
        if when is None:
            one.wait_send()
        else:
            pl.when(when)(lambda one=one: one.wait_send())
    for one in done:
        one.wait()


def fused_body(
    target_rows,
    source_rows,
    target_gain,
    source_gain,
    query_weight,
    key_weight,
    value_weight,
    out_weight,
    out_cotangent,
):
    sp_n, tp_n = lax.axis_size("sp"), lax.axis_size("tp")
    t_loc, width = target_rows.shape
    s_loc = source_rows.shape[0]
    local_width = query_weight.shape[1]
    heads = local_width // HEAD_DIM
    t_block, s_block = tp_n * t_loc, tp_n * s_loc
    lanes = heads * t_block
    slab = key_weight.shape[0]
    pairs = KV_HEADS // 2
    two = 2 * HEAD_DIM
    f32, bf16 = jnp.float32, jnp.bfloat16
    vmem, sem = pltpu.VMEM, pltpu.SemaphoreType.DMA
    scratch = [
        vmem((t_loc, width), bf16),
        vmem((s_loc, width), bf16),
        vmem((1, width), f32),
        vmem((1, width), f32),
        vmem((width, local_width), bf16),
        vmem((slab, key_weight.shape[1]), bf16),
        vmem((slab, key_weight.shape[1]), bf16),
        vmem((local_width, width), bf16),
        vmem((t_loc, width), f32),
        vmem((s_loc, width), f32),
        vmem((local_width, width), f32),
        vmem((tp_n, t_loc, width), bf16),
        vmem((sp_n, tp_n, t_loc, width), bf16),
        vmem((t_block, width), bf16),
        vmem((sp_n, t_block, width), bf16),
        vmem((pairs, tp_n, slab, 2 * two), bf16),
        vmem((s_loc, width), bf16),
        vmem((sp_n, t_block, local_width), bf16),
        vmem((sp_n, t_block, local_width), bf16),
        vmem((tp_n, s_loc, two), bf16),
        vmem((tp_n, s_loc, two), bf16),
        vmem((s_block, HEAD_DIM), bf16),
        vmem((s_block, HEAD_DIM), bf16),
        vmem((two, s_block), bf16),
        vmem((sp_n, lanes, HEAD_DIM), bf16),
        vmem((sp_n, lanes, HEAD_DIM), bf16),
        vmem((sp_n, s_block, lanes), f32),
        vmem((sp_n, s_block, lanes), f32),
        vmem((sp_n, sp_n, 24, 128), f32),
        vmem((sp_n, HEAD_DIM, lanes), bf16),
        vmem((sp_n, HEAD_DIM, lanes), bf16),
        vmem((sp_n, HEAD_DIM, lanes), bf16),
        vmem((sp_n, local_width, t_block), bf16),
        vmem((sp_n, HEAD_DIM, lanes), bf16),
        vmem((sp_n, HEAD_DIM, lanes), bf16),
        vmem((t_block, local_width), bf16),
        vmem((s_block, HEAD_DIM), f32),
        vmem((s_block, HEAD_DIM), f32),
        vmem((tp_n, s_loc, two), bf16),
        vmem((tp_n, s_loc, two), bf16),
        vmem((s_loc, tp_n * two), bf16),
        vmem((tp_n, t_loc, width), bf16),
        vmem((tp_n // 2, t_loc, width), bf16),
        vmem((tp_n // 2, t_loc, width), bf16),
        vmem((3, t_loc, width), bf16),
        vmem((s_loc, width), f32),
        sem((256,)),
        sem((tp_n,)),
        sem((sp_n * tp_n,)),
        sem((pairs * tp_n,)),
        sem((2 * (sp_n + 1 + pairs),)),
        sem((sp_n,)),
        sem((sp_n,)),
        sem((sp_n,)),
        sem((tp_n,)),
        sem((sp_n * sp_n,)),
        sem((sp_n,)),
        sem((sp_n,)),
        sem((sp_n,)),
        sem((tp_n,)),
        sem((tp_n // 2,)),
        sem((3,)),
        sem((9,)),
        sem((3,)),
    ]
    return pl.pallas_call(
        functools.partial(fused_kernel, sp_n, tp_n),
        out_shape=[
            jax.ShapeDtypeStruct((t_loc, width), f32),
            jax.ShapeDtypeStruct((s_loc, width), f32),
            jax.ShapeDtypeStruct((local_width, width), f32),
        ],
        in_specs=[pl.BlockSpec(memory_space=pl.ANY)] * 9,
        out_specs=[pl.BlockSpec(memory_space=pl.ANY)] * 3,
        scratch_shapes=scratch,
        compiler_params=pltpu.CompilerParams(
            collective_id=0,
            has_side_effects=True,
            vmem_limit_bytes=67043328,
        ),
    )(
        target_rows,
        source_rows,
        target_gain[None],
        source_gain[None],
        query_weight,
        key_weight,
        value_weight,
        out_weight,
        out_cotangent,
    )


def choose(*args):
    square = lax.axis_size("tp") == 8 and KV_HEADS == 8
    lanes = lax.axis_size("tp") * args[0].shape[0] * args[4].shape[1] // HEAD_DIM
    if square and lanes % 128 == 0 and lanes <= 1024:
        return fused_body(*args)
    return body(*args)


def solution(mesh):
    return jax.shard_map(
        choose,
        mesh=mesh,
        in_specs=(
            P(("sp", "tp"), None),
            P(("sp", "tp"), None),
            P(),
            P(),
            P(None, "tp"),
            P("tp", None),
            P("tp", None),
            P("tp", None),
            P(("sp", "tp"), None),
        ),
        out_specs=(P(("sp", "tp"), None), P(("sp", "tp"), None), P("tp", None)),
        check_vma=False,
    )
```

```python
import functools

import jax
import jax.numpy as jnp
from jax import lax
from jax.experimental import pallas as pl
from jax.experimental.pallas import tpu as pltpu
from jax.sharding import PartitionSpec as P

HEAD_DIM = 64
KV_HEADS = 8
EPSILON = 1e-06
MESH = pl.DeviceIdType.MESH


def normalize(matrix, gain_vector):
    widened = matrix.astype(jnp.float32)
    factor = lax.rsqrt(jnp.mean(widened * widened, axis=-1, keepdims=True) + EPSILON)
    return (widened * factor * gain_vector).astype(jnp.bfloat16)


def norm_back(matrix, gain_vector, upstream):
    widened = matrix.astype(jnp.float32)
    factor = lax.rsqrt(jnp.mean(widened * widened, axis=-1, keepdims=True) + EPSILON)
    weighted = upstream * gain_vector
    inner_sum = jnp.mean(weighted * widened, axis=-1, keepdims=True)
    return factor * weighted - widened * factor**3 * inner_sum


def exchange_kernel(kinds, sp_n, tp_n, *refs):
    count = len(kinds)
    ins, outs = refs[:count], refs[count : 2 * count]
    send_sems, recv_sems = refs[2 * count : 3 * count], refs[3 * count :]
    sp_me, tp_me = lax.axis_index("sp"), lax.axis_index("tp")
    sizes, places = {"sp": sp_n, "tp": tp_n}, {"sp": sp_me, "tp": tp_me}

    def address(axis, peer):
        return (peer, tp_me) if axis == "sp" else (sp_me, peer)

    axes = sorted({kind.split("_")[1] for kind in kinds})
    barrier = pltpu.get_barrier_semaphore()
    for axis in axes:
        for k in range(1, sizes[axis]):
            peer = lax.rem(places[axis] + k, sizes[axis])
            pl.semaphore_signal(barrier, inc=1, device_id=address(axis, peer), device_id_type=MESH)
    pl.semaphore_wait(barrier, sum(sizes[axis] - 1 for axis in axes))

    def copy(i, axis, source, slot, k, peer):
        return pltpu.make_async_remote_copy(
            src_ref=source,
            dst_ref=outs[i].at[slot],
            send_sem=send_sems[i].at[k],
            recv_sem=recv_sems[i].at[slot],
            device_id=address(axis, peer),
            device_id_type=MESH,
        )

    sent = []
    used = [0] * count

    def send(i, axis, source, target, recv, peer, keep=True):
        one = pltpu.make_async_remote_copy(
            src_ref=source,
            dst_ref=target,
            send_sem=send_sems[i].at[used[i]],
            recv_sem=recv_sems[i].at[recv],
            device_id=address(axis, peer),
            device_id_type=MESH,
        )
        used[i] += 1
        one.start()
        if keep:
            sent.append(one)
        return one

    def arrived(i, axis, target, recv):
        pltpu.make_async_remote_copy(
            src_ref=target,
            dst_ref=target,
            send_sem=send_sems[i].at[0],
            recv_sem=recv_sems[i].at[recv],
            device_id=address(axis, lax.rem(places[axis] + 1, sizes[axis])),
            device_id_type=MESH,
        ).wait_recv()

    square = tp_n == 8
    partner = tp_me + 1 - 2 * lax.rem(tp_me, 2)

    def across(index):
        return index + 2 - 4 * lax.rem(index // 2, 2)

    def along(index):
        return index + 4 - 8 * lax.rem(index // 4, 2)

    def relatives(index):
        if square:
            return [across(index), along(index)]
        return [lax.rem(index + 2 * k, tp_n) for k in range(1, tp_n // 2)]

    def forward(i, c, origin):
        chunks = ins[i].shape[0]
        piece, recv = outs[i].at[origin, c], origin * chunks + c
        arrived(i, "tp", piece, recv)
        send(i, "tp", piece, piece, recv, partner)
        return piece, recv

    line_sent = []
    depth = max([ins[i].shape[0] for i in range(count) if kinds[i] == "pair_tp"], default=0)
    for c in range(depth):
        for i, kind in enumerate(kinds):
            if kind == "pair_tp" and c < ins[i].shape[0]:
                chunks = ins[i].shape[0]
                for peer in relatives(tp_me) + [partner]:
                    piece = outs[i].at[tp_me, c]
                    send(i, "tp", ins[i].at[c], piece, tp_me * chunks + c, peer)
    for i, kind in enumerate(kinds):
        mode, axis = kind.split("_")
        n, me = sizes[axis], places[axis]
        if mode == "line":
            for step in (1, -1):
                inside = (me < n - 1) if step == 1 else (me > 0)
                for c in range(ins[i].shape[0]):
                    line_sent.append((i, inside, used[i], me, c))
                    recv = me * ins[i].shape[0] + c

                    @pl.when(inside)
                    def _():
                        piece = outs[i].at[me, c]
                        send(i, axis, ins[i].at[c], piece, recv, me + step, keep=False)
        elif mode != "pair":
            for k in range(1, n):
                peer = lax.rem(me + k, n)
                source = ins[i] if mode == "gather" else ins[i].at[peer]
                send(i, axis, source, outs[i].at[me], me, peer)
    for i, kind in enumerate(kinds):
        mode, axis = kind.split("_")
        me = places[axis]
        outs[i][me] = ins[i][me] if mode == "swap" else ins[i][...]

    def line_step(i, far, c):
        n, me = sp_n, sp_me
        chunks = ins[i].shape[0]
        for step in (1, -1):
            origin = me - step * far
            valid = (origin >= 0) if step == 1 else (origin <= n - 1)
            onward = (valid & (me < n - 1)) if step == 1 else (valid & (me > 0))

            @pl.when(valid)
            def _():
                arrived(i, "sp", outs[i].at[origin, c], origin * chunks + c)

            if far < n - 1:
                line_sent.append((i, onward, used[i], origin, c))

                @pl.when(onward)
                def _():
                    piece = outs[i].at[origin, c]
                    recv = origin * chunks + c
                    send(i, "sp", piece, piece, recv, me + step, keep=False)

    def pair_step(i, c):
        me = tp_me
        chunks = ins[i].shape[0]
        for order, origin in enumerate(relatives(me)):
            piece, recv = forward(i, c, origin)
            if square and order == (i + c) % 2:
                send(i, "tp", piece, piece, recv, along(me) if order == 0 else across(me))

    lines = [i for i in range(count) if kinds[i] == "line_sp"]
    pairs = [i for i in range(count) if kinds[i] == "pair_tp"]
    for turn in range(max(depth, sp_n - 1 if lines else 0)):
        for i in pairs:
            if turn < ins[i].shape[0]:
                pair_step(i, turn)
        for i in lines:
            if turn + 1 < sp_n:
                for c in range(ins[i].shape[0]):
                    line_step(i, turn + 1, c)
    if square:
        for c in range(depth):
            for i in pairs:
                if c < ins[i].shape[0]:
                    forward(i, c, across(along(tp_me)))
    for i, kind in enumerate(kinds):
        mode, axis = kind.split("_")
        n, me = sizes[axis], places[axis]
        if mode == "pair":
            chunks = ins[i].shape[0]
            others = relatives(partner) + ([across(along(partner))] if square else [])
            for origin in [partner] + others:
                for c in range(chunks):
                    arrived(i, axis, outs[i].at[origin, c], origin * chunks + c)
        elif mode != "line":
            for k in range(1, n):
                origin = lax.rem(me + n - k, n)
                arrived(i, axis, outs[i].at[origin], origin)
    for one in sent:
        one.wait_send()
    for i, happened, slot, origin, c in line_sent:

        @pl.when(happened)
        def _():
            pltpu.make_async_remote_copy(
                src_ref=outs[i].at[origin, c],
                dst_ref=outs[i].at[origin, c],
                send_sem=send_sems[i].at[slot],
                recv_sem=recv_sems[i].at[0],
                device_id=address("sp", lax.rem(sp_me + 1, sp_n)),
                device_id_type=MESH,
            ).wait_send()


def exchange(collective_id, *parts):
    sp_n, tp_n = lax.axis_size("sp"), lax.axis_size("tp")
    kinds = tuple(kind for kind, array in parts)
    arrays = [array for kind, array in parts]
    shapes, sends, recvs = [], [], []
    for kind, array in parts:
        mode, axis = kind.split("_")
        n = sp_n if axis == "sp" else tp_n
        shape = array.shape if mode == "swap" else (n,) + array.shape
        shapes.append(jax.ShapeDtypeStruct(shape, array.dtype))
        chunks = array.shape[0] if mode in ("pair", "line") else 1
        sends.append(pltpu.SemaphoreType.DMA(((2 * n + 8) * chunks,)))
        recvs.append(pltpu.SemaphoreType.DMA((n * chunks,)))
    return pl.pallas_call(
        functools.partial(exchange_kernel, kinds, sp_n, tp_n),
        out_shape=shapes,
        in_specs=[pl.BlockSpec(memory_space=pltpu.VMEM)] * len(parts),
        out_specs=[pl.BlockSpec(memory_space=pltpu.VMEM)] * len(parts),
        scratch_shapes=sends + recvs,
        compiler_params=pltpu.CompilerParams(
            collective_id=collective_id,
            has_side_effects=True,
            vmem_limit_bytes=56 * 1024 * 1024,
        ),
    )(*arrays)


def matmul(left, right):
    return jnp.dot(left, right, preferred_element_type=jnp.float32)


def einsum(text, left, right):
    return jnp.einsum(text, left, right, preferred_element_type=jnp.float32)


def body(
    target_rows,
    source_rows,
    target_gain,
    source_gain,
    query_weight,
    key_weight,
    value_weight,
    out_weight,
    out_cotangent,
):
    sp_n, tp_n = lax.axis_size("sp"), lax.axis_size("tp")
    width = target_rows.shape[1]
    local_width = query_weight.shape[1]
    local_heads = local_width // HEAD_DIM
    slot_heads = max(1, KV_HEADS // tp_n)
    copies = max(1, tp_n // KV_HEADS)
    per_slot = local_heads // slot_heads
    slot_width = slot_heads * HEAD_DIM
    score_scale = HEAD_DIM ** (-0.5)
    bf16 = jnp.bfloat16

    normed_t = normalize(target_rows, target_gain)
    normed_s = normalize(source_rows, source_gain)
    source_local = normed_s.shape[0]
    target_local = normed_t.shape[0]
    target_block = tp_n * target_local
    source_block = tp_n * source_local

    rows_in, cot_in = exchange(
        0,
        ("pair_tp", normed_t[None]),
        ("pair_tp", out_cotangent[None]),
    )
    queries = matmul(rows_in.reshape(target_block, width), query_weight).astype(bf16)
    d_attended = matmul(cot_in.reshape(target_block, width), out_weight.T).astype(bf16)
    halves = (2, key_weight.shape[0] // 2, key_weight.shape[1])
    split = (2, target_block // 2, local_width)
    key_full, value_full, all_queries, all_grads, cot_column = exchange(
        1,
        ("pair_tp", key_weight.reshape(halves)),
        ("pair_tp", value_weight.reshape(halves)),
        ("line_sp", queries.reshape(split)),
        ("line_sp", d_attended.reshape(split)),
        ("line_sp", out_cotangent[None]),
    )
    key_full = key_full.reshape(width, -1)
    value_full = value_full.reshape(width, -1)
    key_own = matmul(normed_s, key_full).astype(bf16)
    value_own = matmul(normed_s, value_full).astype(bf16)

    def to_slots(matrix):
        split = matrix.reshape(source_local, tp_n // copies, 1, slot_width)
        spread = jnp.broadcast_to(split, (source_local, tp_n // copies, copies, slot_width))
        return spread.reshape(source_local, tp_n, slot_width).transpose(1, 0, 2)

    slots = jnp.concatenate([to_slots(key_own), to_slots(value_own)], axis=2)
    (kv_block,) = exchange(2, ("swap_tp", slots))
    whole_rows = sp_n * target_block
    kv_block = kv_block.reshape(source_block, 2, slot_heads, HEAD_DIM)
    keys, values = kv_block[:, 0], kv_block[:, 1]
    head_shape = (whole_rows, slot_heads, per_slot, HEAD_DIM)
    query_view = all_queries.reshape(head_shape)
    grad_view = all_grads.reshape(head_shape)

    scores = einsum("tgqd,sgd->gqts", query_view, keys) * score_scale
    part_max = jnp.max(scores, axis=-1)
    weights = jnp.exp(scores - part_max[..., None])
    part_total = jnp.sum(weights, axis=-1)
    d_probs = einsum("tgqd,sgd->gqts", grad_view, values)
    part_delta = jnp.sum(weights * d_probs, axis=-1)
    part_sum = einsum("gqts,sgd->tgqd", weights.astype(bf16), values)
    stats = jnp.stack([part_max, part_total, part_delta]).reshape(3 * local_heads, whole_rows)
    (all_stats,) = exchange(3, ("gather_sp", stats))
    all_stats = all_stats.reshape(sp_n, 3, slot_heads, per_slot, whole_rows)
    row_max = jnp.max(all_stats[:, 0], axis=0)
    rescale = jnp.exp(all_stats[:, 0] - row_max)
    total = jnp.sum(all_stats[:, 1] * rescale, axis=0)
    delta = jnp.sum(all_stats[:, 2] * rescale, axis=0) / total
    local_scale = jnp.exp(part_max - row_max) / total

    attended_part = part_sum * local_scale.transpose(2, 0, 1)[..., None]
    attended_part = attended_part.reshape(sp_n, target_block, local_width).astype(bf16)
    probs = weights * local_scale[..., None]
    d_scores = (probs * (d_probs - delta[..., None])).astype(bf16)
    value_sum = einsum("gqts,tgqd->sgd", probs.astype(bf16), grad_view)
    key_sum = einsum("gqts,tgqd->sgd", d_scores, query_view) * score_scale
    d_query = einsum("gqts,sgd->tgqd", d_scores, keys) * score_scale
    d_query = d_query.reshape(sp_n, target_block, local_width).astype(bf16)
    grads = jnp.concatenate(
        [key_sum.reshape(source_block, slot_width), value_sum.reshape(source_block, slot_width)],
        axis=1,
    )
    grads = grads.reshape(tp_n, source_local, 2 * slot_width).astype(bf16)
    query_terms, attended_terms, grads_back, cot_all = exchange(
        4,
        ("swap_sp", d_query),
        ("swap_sp", attended_part),
        ("swap_tp", grads),
        ("pair_tp", cot_column.reshape(sp_n, target_local, width)),
    )
    query_grad = jnp.sum(query_terms.astype(jnp.float32), axis=0).astype(bf16)
    attended = jnp.sum(attended_terms.astype(jnp.float32), axis=0).astype(bf16)

    target_terms = matmul(query_grad, query_weight.T).astype(bf16)
    target_back, attended_all = exchange(
        5,
        ("swap_tp", target_terms.reshape(tp_n, target_local, width)),
        ("line_sp", attended.reshape(split)),
    )

    def from_slots(matrix):
        folded = matrix.reshape(tp_n // copies, copies, source_local, slot_width)
        folded = jnp.sum(folded.astype(jnp.float32), axis=1)
        return folded.transpose(1, 0, 2).reshape(source_local, -1).astype(bf16)

    key_grad = from_slots(grads_back[:, :, :slot_width])
    value_grad = from_slots(grads_back[:, :, slot_width:])
    d_normed_s = matmul(key_grad, key_full.T) + matmul(value_grad, value_full.T)
    source_grad = norm_back(source_rows, source_gain, d_normed_s)
    d_normed_t = jnp.sum(target_back.astype(jnp.float32), axis=0)
    target_grad = out_cotangent.astype(jnp.float32) + norm_back(
        target_rows, target_gain, d_normed_t
    )
    attended_rows = attended_all.reshape(sp_n, tp_n, target_local, local_width)
    out_weight_grad = jnp.einsum(
        "stlw,tsld->wd", attended_rows, cot_all, preferred_element_type=jnp.float32
    )
    return (target_grad, source_grad, out_weight_grad)


def fused_kernel(sp_n, tp_n, *refs):
    loads, stores = refs[:9], refs[9:12]
    target, source, tgain, sgain, qw, kw, vw, ow = refs[12:20]
    tgrad, sgrad, owg = refs[20:23]
    t_rx, c_rx, rows, cotf, w_rx, ns, q_all, d_all, kv_tx, kv_rx = refs[23:33]
    k2, v2, kvt, qc, dc, p_buf, dp_buf, own, st, st_rx, o_part = refs[33:44]
    o_tx, o_rx, att, attb, dq_f, dq_tx, dq_rx, qg, dk, dv = refs[44:54]
    g_tx, g_rx, gcat, tt, tp_rx, ts_tx, ts_rx, un = refs[54:62]
    send_s, t_s, c_s, w_s, far_s, cz_s, q_s, d_s, kv_s, near_s = refs[62:72]
    st_s, o_s, att_s, dq_s, g_s, tp_s, ts_s, load_s, store_s = refs[72:81]
    f32, bf16 = jnp.float32, jnp.bfloat16
    z, me = lax.axis_index("sp"), lax.axis_index("tp")
    core = lax.rem(me, 2)
    t_loc, width = target.shape
    s_loc = source.shape[0]
    slab, local_width = w_rx.shape[2], qw.shape[1]
    heads = local_width // HEAD_DIM
    t_block = tp_n * t_loc
    lanes = heads * t_block
    s_block = tp_n * s_loc
    pairs = w_rx.shape[0]
    scale = HEAD_DIM ** (-0.5)

    def across(i):
        return i + 2 - 4 * lax.rem(i // 2, 2)

    def along(i):
        return i + 4 - 8 * lax.rem(i // 4, 2)

    mate = me + 1 - 2 * core
    zt, zn = z + 2 - 4 * (z // 2), z + 1 - 2 * lax.rem(z, 2)
    zs = [lax.rem(z + k, sp_n) for k in range(1, sp_n)]
    ts = [lax.rem(me + k, tp_n) for k in range(1, tp_n)]

    barrier = pltpu.get_barrier_semaphore()
    for peer in zs:
        pl.semaphore_signal(barrier, inc=1, device_id=(peer, me), device_id_type=MESH)
    for peer in ts:
        pl.semaphore_signal(barrier, inc=1, device_id=(z, peer), device_id_type=MESH)

    for peer in ts:
        pl.semaphore_signal(barrier, inc=1, device_id=(zn, peer), device_id_type=MESH)

    sent = []
    ring = send_s.shape[0]

    def drain(one, when):
        if when is None:
            one.wait_send()
        else:
            pl.when(when)(lambda: one.wait_send())

    def push(src, dst, sem, zz, i, when=None):
        turn = len(sent) % ring
        if len(sent) >= ring:
            drain(*sent[len(sent) - ring])
        one = pltpu.make_async_remote_copy(
            src_ref=src,
            dst_ref=dst,
            send_sem=send_s.at[turn],
            recv_sem=sem,
            device_id=(zz, i),
            device_id_type=MESH,
        )
        sent.append((one, when))
        if when is None:
            one.start()
        else:
            pl.when(when)(lambda: one.start())

    def pull(ref, sem):
        pltpu.make_async_remote_copy(
            src_ref=ref,
            dst_ref=ref,
            send_sem=send_s.at[0],
            recv_sem=sem,
            device_id=(z, mate),
            device_id_type=MESH,
        ).wait_recv()

    kept = (target, source, tgain, sgain, qw, kw, vw, ow, c_rx.at[z, me])
    copies = [pltpu.make_async_copy(a, b, load_s.at[i]) for i, (a, b) in enumerate(zip(loads, kept))]
    for i in (0, 2, 8, 5, 6, 1, 3, 4, 7):
        copies[i].start()

    def store(i, a):
        one = pltpu.make_async_copy(a, stores[i], store_s.at[i])
        one.start()
        return one

    def nt(a, b):
        return lax.dot_general(a, b, (((1,), (1,)), ((), ())), preferred_element_type=f32)

    def nn(a, b):
        return jnp.dot(a, b, preferred_element_type=f32)

    class Gather:
        def __init__(self, slot, sem, far, depth):
            self.slot, self.sem, self.far, self.depth = slot, sem, far, depth

        def start(self):
            for peer in (across(me), along(me), mate):
                push(self.slot(me), self.slot(me), self.sem(me), z, peer)

        def half(self, origin, order):
            return self.slot(origin).at[self.depth[order] : self.depth[order + 1]]

        def mid(self):
            for order, origin in enumerate((across(me), along(me))):
                pull(self.slot(origin), self.sem(origin))
                piece = self.half(origin, order)
                push(piece, piece, self.far(order), z, along(me) if order == 0 else across(me))
            for origin in (across(me), along(me)):
                push(self.slot(origin), self.slot(origin), self.sem(origin), z, mate)

        def fin(self):
            origin = across(along(me))
            for order in range(2):
                pull(self.half(origin, order), self.far(order))
            push(self.slot(origin), self.slot(origin), self.sem(origin), z, mate)

        def rest(self):
            for origin in (mate, across(mate), along(mate), across(along(mate))):
                pull(self.slot(origin), self.sem(origin))

    copies[0].wait()
    copies[2].wait()
    t_rx[me] = normalize(target[...], tgain[...])
    copies[8].wait()
    pl.semaphore_wait(barrier, sp_n - 1 + 2 * (tp_n - 1))

    some, more = (0, t_loc // 2 // 8 * 8, t_loc), (0, slab // 2, slab)
    t_all = Gather(lambda o: t_rx.at[o], lambda o: t_s.at[o], lambda k: far_s.at[k], some)
    c_all = [
        Gather(
            lambda o, p=p: c_rx.at[p, o],
            lambda o, p=p: c_s.at[p * tp_n + o],
            lambda k, n=n: far_s.at[2 * n + 2 + k],
            some,
        )
        for n, p in enumerate([z] + zs)
    ]
    c_own, c_far = c_all[0], c_all[1:]
    w_all = [
        Gather(
            lambda o, c=c: w_rx.at[c, o],
            lambda o, c=c: w_s.at[c * tp_n + o],
            lambda k, c=c: far_s.at[2 * (sp_n + 1 + c) + k],
            more,
        )
        for c in range(pairs)
    ]

    t_all.start()
    c_own.start()
    for peer in zs:
        push(c_rx.at[z, me], c_rx.at[z, me], cz_s.at[z], peer, me)
    copies[5].wait()
    copies[6].wait()
    half = w_rx.shape[3]
    for c in range(pairs):
        part = (kw, vw)[c // 2]
        w_rx[c, me] = part[:, (c % 2) * half : (c % 2 + 1) * half]
    w_all[0].start()
    copies[1].wait()
    copies[3].wait()
    step = min(s_loc, 32)
    for i in range(0, s_loc, step):
        ns[i : i + step] = normalize(source[i : i + step], sgain[...])
    t_all.mid()
    c_own.mid()
    w_all[1].start()
    w_all[0].mid()
    w_all[2].start()
    t_all.fin()
    c_own.fin()
    t_all.rest()
    for o in range(tp_n):
        rows[o * t_loc : (o + 1) * t_loc] = t_rx[o]
    copies[4].wait()
    q_all[0] = (nn(rows[...], qw[...]).astype(bf16) * scale).astype(bf16)
    push(q_all.at[0], q_all.at[1], q_s.at[0], zt, me)
    w_all[1].mid()
    w_all[3].start()
    c_own.rest()
    for o in range(tp_n):
        cotf[z, o * t_loc : (o + 1) * t_loc] = c_rx[z, o]
    copies[7].wait()
    d_all[0] = nt(cotf[z], ow[...]).astype(bf16)
    push(d_all.at[0], d_all.at[1], d_s.at[0], zt, me)

    packed = s_loc // 2

    def split_kv(c):
        w_all[c].rest()
        total = nn(ns[:, :slab], w_rx[c, 0])
        for o in range(1, tp_n):
            total += nn(ns[:, o * slab : (o + 1) * slab], w_rx[c, o])
        total = total.astype(bf16)
        for j in range(tp_n // 2):
            head = (c % 2) * (tp_n // 2) + j
            part = total[:, j * HEAD_DIM : (j + 1) * HEAD_DIM]
            part = jnp.concatenate([part[:packed], part[packed:]], axis=1)
            kv_tx[c // 2, head] = part

            @pl.when(me == head)
            def _():
                kv_rx[0, c // 2, head] = part

            sem = kv_s.at[(c // 2) * tp_n + me]
            push(kv_tx.at[c // 2, head], kv_rx.at[0, c // 2, me], sem, z, head, me != head)
            if c // 2 == 1:
                push(kv_tx.at[1, head], kv_rx.at[1, 1, me], near_s.at[1 + me], zn, head)

    def unpack(w, kind):
        if w == 0:
            for o in ts:
                pull(kv_rx.at[0, kind, o], kv_s.at[kind * tp_n + o])
            if kind == 0:
                push(kv_rx.at[0, 0], kv_rx.at[1, 0], near_s.at[0], zn, me)
        elif kind == 0:
            pull(kv_rx.at[1, 0], near_s.at[0])
        else:
            for o in range(tp_n):
                pull(kv_rx.at[1, 1, o], near_s.at[1 + o])
        out = (k2, v2)[kind]
        for o in range(tp_n):
            part = kv_rx[w, kind, o]
            out[w, o * s_loc : o * s_loc + packed] = part[:, :HEAD_DIM]
            out[w, o * s_loc + packed : (o + 1) * s_loc] = part[:, HEAD_DIM:]

    groups = lanes // 128

    def fold(op, x, n=4):
        size = x.shape[0] // n
        parts = [
            op(x[i * size : (i + 1) * size].reshape(size // 8, 8, x.shape[1]), axis=0)
            for i in range(n)
        ]
        both = jnp.maximum if op is jnp.max else jnp.add
        return op(functools.reduce(both, parts), axis=0, keepdims=True)

    def line(x):
        return jnp.concatenate([x[g : g + 1] for g in range(groups)], axis=1)

    def take(u, full, sems, out):
        if u == 1:
            pull(full.at[1], sems.at[0])
        for h in range(heads):
            cols = slice(h * HEAD_DIM, (h + 1) * HEAD_DIM)
            out[u, h * t_block : (h + 1) * t_block] = full[u, :, cols]

    def weigh(u, w):
        if w == 0:
            take(u, q_all, q_s, qc)
        score = nt(k2[w], qc[u])
        top = fold(jnp.max, score)
        weight = jnp.exp(score - top)
        own[u, w, 0:1] = top
        own[u, w, 1:2] = fold(jnp.sum, weight)
        p_buf[u, w] = weight

    def turn_kv(w):
        for o in range(tp_n):
            part = slice(o * s_loc, (o + 1) * s_loc)
            both = jnp.concatenate([k2[w, part], v2[w, part]], axis=1)
            kvt[w, :, part] = both.astype(f32).T.astype(bf16)

    def first(u, w):
        if w == 0:
            take(u, d_all, d_s, dc)
        weight = p_buf[u, w]
        d_prob = nt(v2[w], dc[u])
        own[u, w, 2:3] = fold(jnp.sum, weight * d_prob)
        dp_buf[u, w] = d_prob
        o_part[u, w] = nn(kvt[w, HEAD_DIM:], weight.astype(bf16))

    def join(u):
        top = jnp.maximum(own[u, 0, 0:1], own[u, 1, 0:1])
        lifts = [jnp.exp(own[u, w, 0:1] - top) for w in range(2)]
        total = sum(own[u, w, 1:2] * lifts[w] for w in range(2))
        inner = sum(own[u, w, 2:3] * lifts[w] for w in range(2)) / total
        o_tx[u] = (sum(o_part[u, w] * lifts[w] for w in range(2)) / total).astype(bf16)
        for k, value in enumerate((top + jnp.log(total), inner)):
            for g in range(groups):
                row = groups * k + g
                st[u, row : row + 1] = value[:, g * 128 : (g + 1) * 128]

    cut = lanes // 2 // 128 * 128
    spans = [slice(0, cut), slice(cut, lanes)] if cut else [slice(0, lanes)]

    w_all[0].fin()
    split_kv(0)
    w_all[2].mid()
    w_all[1].fin()
    split_kv(1)
    w_all[3].mid()
    unpack(0, 0)
    weigh(0, 0)
    w_all[2].fin()
    w_all[3].fin()
    split_kv(2)
    split_kv(3)
    for k, p in enumerate(zs):
        pull(c_rx.at[p, me], cz_s.at[p])
        c_far[k].start()
    weigh(1, 0)
    unpack(1, 0)
    weigh(0, 1)
    weigh(1, 1)
    unpack(0, 1)
    turn_kv(0)
    first(0, 0)
    first(1, 0)
    unpack(1, 1)
    turn_kv(1)
    for u in range(2):
        first(u, 1)
        join(u)
        push(st.at[u], st_rx.at[u], st_s.at[u], zt, me)
    for n, span in enumerate(spans):
        push(o_tx.at[1, :, span], o_rx.at[:, span], o_s.at[n], zt, me)

    def stats(u):
        logs = [st[u, :groups], st_rx[1 - u, :groups]]
        inners = [st[u, groups:], st_rx[1 - u, groups:]]
        top = jnp.maximum(*logs)
        log_total = top + jnp.log(sum(jnp.exp(x - top) for x in logs))
        lifts = [jnp.exp(x - log_total) for x in logs]
        return log_total, lifts, inners[0] * lifts[0] + inners[1] * lifts[1]

    def attend():
        lifts = [line(x) for x in stats(0)[1]]
        for n, span in enumerate(spans):
            pull(o_rx.at[:, span], o_s.at[n])
            mine = o_tx[0, :, span].astype(f32) * lifts[0][:, span]
            other = o_rx[:, span].astype(f32) * lifts[1][:, span]
            att[z, :, span] = (mine + other).astype(bf16)
            for peer in zs:
                part = att.at[z, :, span]
                push(part, part, att_s.at[n * sp_n + z], peer, me)

    def second(u, w, start):
        log_total, lifts, inner = stats(u)
        prob = p_buf[u, w] * jnp.exp(own[u, w, 0:1] - line(log_total))
        d_score = (prob * (dp_buf[u, w] - line(inner))).astype(bf16)
        prob = prob.astype(bf16)
        d_value, d_key = nn(prob, dc[u]), nn(d_score, qc[u])
        dv[w] = d_value if u == 1 else dv[w] + d_value
        dk[w] = d_key if u == 1 else dk[w] + d_key
        d_query = nn(kvt[w, :HEAD_DIM], d_score)
        dq_f[u] = d_query if start else dq_f[u] + d_query

    def send_g(w, plane):
        for o in range(tp_n):
            part = slice(o * s_loc, (o + 1) * s_loc)
            g_tx[w, o] = jnp.concatenate([dk[w, part], dv[w, part]], axis=1).astype(bf16)
        for o in ts + ([me] if w == 1 else []):
            push(g_tx.at[w, o], g_rx.at[w, me], g_s.at[w * tp_n + me], plane, o)

    pull(st_rx.at[0], st_s.at[0])
    second(1, 0, True)
    second(1, 1, False)
    dq_tx[...] = dq_f[1].astype(bf16)
    push(dq_tx, dq_rx, dq_s.at[0], zt, me)
    pull(st_rx.at[1], st_s.at[1])
    second(0, 1, True)
    send_g(1, zn)
    c_far[0].mid()
    c_far[1].mid()
    second(0, 0, False)
    send_g(0, z)
    g_rx[0, me] = g_tx[0, me]
    c_far[2].mid()
    pull(dq_rx, dq_s.at[0])
    attend()
    summed = (dq_f[0] + dq_rx[...].astype(f32)) * scale
    summed = summed.T
    for h in range(heads):
        piece = summed[h * t_block : (h + 1) * t_block].astype(bf16)
        qg[:, h * HEAD_DIM : (h + 1) * HEAD_DIM] = piece
    wide = 512

    def terms(j, carry):
        cols = pl.ds(pl.multiple_of(j * wide, wide), wide)
        value = nt(qg[...], qw[cols])
        for o in range(tp_n):
            tt[o, :, cols] = value[o * t_loc : (o + 1) * t_loc].astype(bf16)
        return carry

    lax.fori_loop(0, width // wide, terms, 0)
    chips = tp_n // 2
    for c in range(chips):
        push(tt.at[2 * c + 1 - core], tp_rx.at[c], tp_s.at[c], z, mate)
    tile = 256

    for c in range(chips):
        pull(tp_rx.at[c], tp_s.at[c])
        ts_tx[c] = (tt[2 * c + core].astype(f32) + tp_rx[c].astype(f32)).astype(bf16)
    for r, peer in enumerate((across(along(me)), across(me), along(me))):
        push(ts_tx.at[peer // 2], ts_rx.at[r], ts_s.at[r], z, peer)
    for item in c_far:
        item.fin()
    side = tp_n * HEAD_DIM
    for o in ts:
        pull(g_rx.at[0, o], g_s.at[o])
    for o in range(tp_n):
        pull(g_rx.at[1, o], g_s.at[tp_n + o])
        part = (g_rx[0, o].astype(f32) + g_rx[1, o].astype(f32)).astype(bf16)
        gcat[:, o * HEAD_DIM : (o + 1) * HEAD_DIM] = part[:, :HEAD_DIM]
        gcat[:, side + o * HEAD_DIM : side + (o + 1) * HEAD_DIM] = part[:, HEAD_DIM:]

    def upstream(o, carry):
        cols = pl.ds(pl.multiple_of(o * slab, slab), slab)
        total = nt(gcat[:, : 4 * HEAD_DIM], w_rx[0, o])
        for c in range(1, pairs):
            total += nt(gcat[:, c * 4 * HEAD_DIM : (c + 1) * 4 * HEAD_DIM], w_rx[c, o])
        un[:, cols] = total
        return carry

    lax.fori_loop(0, tp_n, upstream, 0)
    for i in range(0, s_loc, step):
        part = slice(i, i + step)
        sgrad[part] = norm_back(source[part], sgain[...], un[part])
    done = [store(1, sgrad)]
    for k, p in enumerate(zs):
        c_far[k].rest()
        for o in range(tp_n):
            cotf[p, o * t_loc : (o + 1) * t_loc] = c_rx[p, o]
    for p in zs:
        for n, span in enumerate(spans):
            pull(att.at[p, :, span], att_s.at[n * sp_n + p])
    for b in range(sp_n):
        for h in range(heads):
            piece = att[b, :, h * t_block : (h + 1) * t_block]
            attb[b, h * HEAD_DIM : (h + 1) * HEAD_DIM] = piece

    def weight_grad(j, carry):
        cols = pl.ds(pl.multiple_of(j * tile, tile), tile)
        owg[:, cols] = sum(nn(attb[b], cotf[b, :, cols]) for b in range(sp_n))
        return carry

    rest = width // tile // 2
    for n in range(2):
        lax.fori_loop(n * rest, (n + 1) * rest, weight_grad, 0)
        part = slice(n * rest * tile, (n + 1) * rest * tile)
        one = pltpu.make_async_copy(owg.at[:, part], stores[2].at[:, part], store_s.at[2 + n])
        one.start()
        done.append(one)
    mine = ts_tx[me // 2].astype(f32)
    for r in range(3):
        pull(ts_rx.at[r], ts_s.at[r])
    mine = mine + sum(ts_rx[r].astype(f32) for r in range(3))
    tgrad[...] = c_rx[z, me].astype(f32) + norm_back(target[...], tgain[...], mine)
    done.append(store(0, tgrad))

    for one, when in sent[-ring:]:
        drain(one, when)
    for one in done:
        one.wait()


def finish_kernel(*refs):
    ins, outs, held = refs[:3], refs[3:6], refs[6:9]
    in_sems, out_sems = refs[9:11]
    pieces = []
    for i in (2, 1, 0):
        size = ins[i].shape[0]
        step = max(size // 4 // 8 * 8, 8)
        for at in range(0, size, step):
            part = pl.ds(at, min(step, size - at))
            pieces.append((ins[i].at[part], held[i].at[part], outs[i].at[part]))
    for k, (a, b, c) in enumerate(pieces):
        pltpu.make_async_copy(a, b, in_sems.at[k]).start()
    for k, (a, b, c) in enumerate(pieces):
        pltpu.make_async_copy(a, b, in_sems.at[k]).wait()
        pltpu.make_async_copy(b, c, out_sems.at[k]).start()
    for k, (a, b, c) in enumerate(pieces):
        pltpu.make_async_copy(b, c, out_sems.at[k]).wait()


def finish(*arrays):
    return pl.pallas_call(
        finish_kernel,
        out_shape=[jax.ShapeDtypeStruct(a.shape, a.dtype) for a in arrays],
        in_specs=[pl.BlockSpec(memory_space=pltpu.HBM)] * 3,
        out_specs=[pl.BlockSpec(memory_space=pl.ANY)] * 3,
        scratch_shapes=[pltpu.VMEM(a.shape, a.dtype) for a in arrays]
        + [pltpu.SemaphoreType.DMA((12,)), pltpu.SemaphoreType.DMA((12,))],
        compiler_params=pltpu.CompilerParams(vmem_limit_bytes=67043328),
    )(*arrays)


def fused_body(
    target_rows,
    source_rows,
    target_gain,
    source_gain,
    query_weight,
    key_weight,
    value_weight,
    out_weight,
    out_cotangent,
):
    sp_n, tp_n = lax.axis_size("sp"), lax.axis_size("tp")
    t_loc, width = target_rows.shape
    s_loc = source_rows.shape[0]
    local_width = query_weight.shape[1]
    heads = local_width // HEAD_DIM
    t_block, s_block = tp_n * t_loc, tp_n * s_loc
    lanes = heads * t_block
    slab = key_weight.shape[0]
    pairs = KV_HEADS // 2
    two = 2 * HEAD_DIM
    f32, bf16 = jnp.float32, jnp.bfloat16
    vmem, sem = pltpu.VMEM, pltpu.SemaphoreType.DMA
    sends = 48
    scratch = [
        vmem((t_loc, width), bf16),
        vmem((s_loc, width), bf16),
        vmem((1, width), f32),
        vmem((1, width), f32),
        vmem((width, local_width), bf16),
        vmem((slab, key_weight.shape[1]), bf16),
        vmem((slab, key_weight.shape[1]), bf16),
        vmem((local_width, width), bf16),
        vmem((t_loc, width), f32),
        vmem((s_loc, width), f32),
        vmem((local_width, width), f32),
        vmem((tp_n, t_loc, width), bf16),
        vmem((sp_n, tp_n, t_loc, width), bf16),
        vmem((t_block, width), bf16),
        vmem((sp_n, t_block, width), bf16),
        vmem((pairs, tp_n, slab, 2 * two), bf16),
        vmem((s_loc, width), bf16),
        vmem((2, t_block, local_width), bf16),
        vmem((2, t_block, local_width), bf16),
        vmem((2, tp_n, s_loc // 2, two), bf16),
        vmem((2, 2, tp_n, s_loc // 2, two), bf16),
        vmem((2, s_block, HEAD_DIM), bf16),
        vmem((2, s_block, HEAD_DIM), bf16),
        vmem((2, two, s_block), bf16),
        vmem((2, lanes, HEAD_DIM), bf16),
        vmem((2, lanes, HEAD_DIM), bf16),
        vmem((2, 2, s_block, lanes), f32),
        vmem((2, 2, s_block, lanes), f32),
        vmem((2, 2, 3, lanes), f32),
        vmem((2, lanes // 64, 128), f32),
        vmem((2, lanes // 64, 128), f32),
        vmem((2, 2, HEAD_DIM, lanes), f32),
        vmem((2, HEAD_DIM, lanes), bf16),
        vmem((HEAD_DIM, lanes), bf16),
        vmem((sp_n, HEAD_DIM, lanes), bf16),
        vmem((sp_n, local_width, t_block), bf16),
        vmem((2, HEAD_DIM, lanes), f32),
        vmem((HEAD_DIM, lanes), bf16),
        vmem((HEAD_DIM, lanes), bf16),
        vmem((t_block, local_width), bf16),
        vmem((2, s_block, HEAD_DIM), f32),
        vmem((2, s_block, HEAD_DIM), f32),
        vmem((2, tp_n, s_loc, two), bf16),
        vmem((2, tp_n, s_loc, two), bf16),
        vmem((s_loc, tp_n * two), bf16),
        vmem((tp_n, t_loc, width), bf16),
        vmem((tp_n // 2, t_loc, width), bf16),
        vmem((tp_n // 2, t_loc, width), bf16),
        vmem((3, t_loc, width), bf16),
        vmem((s_loc, width), f32),
        sem((sends,)),
        sem((tp_n,)),
        sem((sp_n * tp_n,)),
        sem((pairs * tp_n,)),
        sem((2 * (sp_n + 1 + pairs),)),
        sem((sp_n,)),
        sem((1,)),
        sem((1,)),
        sem((2 * tp_n,)),
        sem((1 + tp_n,)),
        sem((2,)),
        sem((2,)),
        sem((2 * sp_n,)),
        sem((1,)),
        sem((2 * tp_n,)),
        sem((tp_n // 2,)),
        sem((3,)),
        sem((9,)),
        sem((4,)),
    ]
    results = pl.pallas_call(
        functools.partial(fused_kernel, sp_n, tp_n),
        out_shape=[
            jax.ShapeDtypeStruct((t_loc, width), f32),
            jax.ShapeDtypeStruct((s_loc, width), f32),
            jax.ShapeDtypeStruct((local_width, width), f32),
        ],
        in_specs=[pl.BlockSpec(memory_space=pl.ANY)] * 9,
        out_specs=[pl.BlockSpec(memory_space=pl.ANY)] * 3,
        scratch_shapes=scratch,
        compiler_params=pltpu.CompilerParams(
            collective_id=0,
            has_side_effects=True,
            vmem_limit_bytes=67043328,
        ),
    )(
        target_rows,
        source_rows,
        target_gain[None],
        source_gain[None],
        query_weight,
        key_weight,
        value_weight,
        out_weight,
        out_cotangent,
    )
    return tuple(finish(*results))


def choose(*args):
    square = lax.axis_size("tp") == 8 and KV_HEADS == 8 and lax.axis_size("sp") == 4
    lanes = lax.axis_size("tp") * args[0].shape[0] * args[4].shape[1] // HEAD_DIM
    if square and lanes % 128 == 0 and lanes <= 1024:
        return fused_body(*args)
    return body(*args)


def solution(mesh):
    return jax.shard_map(
        choose,
        mesh=mesh,
        in_specs=(
            P(("sp", "tp"), None),
            P(("sp", "tp"), None),
            P(),
            P(),
            P(None, "tp"),
            P("tp", None),
            P("tp", None),
            P("tp", None),
            P(("sp", "tp"), None),
        ),
        out_specs=(P(("sp", "tp"), None), P(("sp", "tp"), None), P("tp", None)),
        check_vma=False,
    )
```

```python
import functools

import jax
import jax.numpy as jnp
from jax import lax
from jax.experimental import pallas as pl
from jax.experimental.pallas import tpu as pltpu
from jax.sharding import PartitionSpec as P

HEAD_DIM = 64
KV_HEADS = 8
EPSILON = 1e-06
MESH = pl.DeviceIdType.MESH


def normalize(matrix, gain_vector):
    widened = matrix.astype(jnp.float32)
    factor = lax.rsqrt(jnp.mean(widened * widened, axis=-1, keepdims=True) + EPSILON)
    return (widened * factor * gain_vector).astype(jnp.bfloat16)


def norm_back(matrix, gain_vector, upstream):
    widened = matrix.astype(jnp.float32)
    factor = lax.rsqrt(jnp.mean(widened * widened, axis=-1, keepdims=True) + EPSILON)
    weighted = upstream * gain_vector
    inner_sum = jnp.mean(weighted * widened, axis=-1, keepdims=True)
    return factor * weighted - widened * factor**3 * inner_sum


def exchange_kernel(kinds, sp_n, tp_n, *refs):
    count = len(kinds)
    ins, outs = refs[:count], refs[count : 2 * count]
    send_sems, recv_sems = refs[2 * count : 3 * count], refs[3 * count :]
    sp_me, tp_me = lax.axis_index("sp"), lax.axis_index("tp")
    sizes, places = {"sp": sp_n, "tp": tp_n}, {"sp": sp_me, "tp": tp_me}

    def address(axis, peer):
        return (peer, tp_me) if axis == "sp" else (sp_me, peer)

    axes = sorted({kind.split("_")[1] for kind in kinds})
    barrier = pltpu.get_barrier_semaphore()
    for axis in axes:
        for k in range(1, sizes[axis]):
            peer = lax.rem(places[axis] + k, sizes[axis])
            pl.semaphore_signal(barrier, inc=1, device_id=address(axis, peer), device_id_type=MESH)
    pl.semaphore_wait(barrier, sum(sizes[axis] - 1 for axis in axes))

    def copy(i, axis, source, slot, k, peer):
        return pltpu.make_async_remote_copy(
            src_ref=source,
            dst_ref=outs[i].at[slot],
            send_sem=send_sems[i].at[k],
            recv_sem=recv_sems[i].at[slot],
            device_id=address(axis, peer),
            device_id_type=MESH,
        )

    sent = []
    used = [0] * count

    def send(i, axis, source, target, recv, peer, keep=True):
        one = pltpu.make_async_remote_copy(
            src_ref=source,
            dst_ref=target,
            send_sem=send_sems[i].at[used[i]],
            recv_sem=recv_sems[i].at[recv],
            device_id=address(axis, peer),
            device_id_type=MESH,
        )
        used[i] += 1
        one.start()
        if keep:
            sent.append(one)
        return one

    def arrived(i, axis, target, recv):
        pltpu.make_async_remote_copy(
            src_ref=target,
            dst_ref=target,
            send_sem=send_sems[i].at[0],
            recv_sem=recv_sems[i].at[recv],
            device_id=address(axis, lax.rem(places[axis] + 1, sizes[axis])),
            device_id_type=MESH,
        ).wait_recv()

    square = tp_n == 8
    partner = tp_me + 1 - 2 * lax.rem(tp_me, 2)

    def across(index):
        return index + 2 - 4 * lax.rem(index // 2, 2)

    def along(index):
        return index + 4 - 8 * lax.rem(index // 4, 2)

    def relatives(index):
        if square:
            return [across(index), along(index)]
        return [lax.rem(index + 2 * k, tp_n) for k in range(1, tp_n // 2)]

    def forward(i, c, origin):
        chunks = ins[i].shape[0]
        piece, recv = outs[i].at[origin, c], origin * chunks + c
        arrived(i, "tp", piece, recv)
        send(i, "tp", piece, piece, recv, partner)
        return piece, recv

    line_sent = []
    depth = max([ins[i].shape[0] for i in range(count) if kinds[i] == "pair_tp"], default=0)
    for c in range(depth):
        for i, kind in enumerate(kinds):
            if kind == "pair_tp" and c < ins[i].shape[0]:
                chunks = ins[i].shape[0]
                for peer in relatives(tp_me) + [partner]:
                    piece = outs[i].at[tp_me, c]
                    send(i, "tp", ins[i].at[c], piece, tp_me * chunks + c, peer)
    for i, kind in enumerate(kinds):
        mode, axis = kind.split("_")
        n, me = sizes[axis], places[axis]
        if mode == "line":
            for step in (1, -1):
                inside = (me < n - 1) if step == 1 else (me > 0)
                for c in range(ins[i].shape[0]):
                    line_sent.append((i, inside, used[i], me, c))
                    recv = me * ins[i].shape[0] + c

                    @pl.when(inside)
                    def _():
                        piece = outs[i].at[me, c]
                        send(i, axis, ins[i].at[c], piece, recv, me + step, keep=False)
        elif mode != "pair":
            for k in range(1, n):
                peer = lax.rem(me + k, n)
                source = ins[i] if mode == "gather" else ins[i].at[peer]
                send(i, axis, source, outs[i].at[me], me, peer)
    for i, kind in enumerate(kinds):
        mode, axis = kind.split("_")
        me = places[axis]
        outs[i][me] = ins[i][me] if mode == "swap" else ins[i][...]

    def line_step(i, far, c):
        n, me = sp_n, sp_me
        chunks = ins[i].shape[0]
        for step in (1, -1):
            origin = me - step * far
            valid = (origin >= 0) if step == 1 else (origin <= n - 1)
            onward = (valid & (me < n - 1)) if step == 1 else (valid & (me > 0))

            @pl.when(valid)
            def _():
                arrived(i, "sp", outs[i].at[origin, c], origin * chunks + c)

            if far < n - 1:
                line_sent.append((i, onward, used[i], origin, c))

                @pl.when(onward)
                def _():
                    piece = outs[i].at[origin, c]
                    recv = origin * chunks + c
                    send(i, "sp", piece, piece, recv, me + step, keep=False)

    def pair_step(i, c):
        me = tp_me
        chunks = ins[i].shape[0]
        for order, origin in enumerate(relatives(me)):
            piece, recv = forward(i, c, origin)
            if square and order == (i + c) % 2:
                send(i, "tp", piece, piece, recv, along(me) if order == 0 else across(me))

    lines = [i for i in range(count) if kinds[i] == "line_sp"]
    pairs = [i for i in range(count) if kinds[i] == "pair_tp"]
    for turn in range(max(depth, sp_n - 1 if lines else 0)):
        for i in pairs:
            if turn < ins[i].shape[0]:
                pair_step(i, turn)
        for i in lines:
            if turn + 1 < sp_n:
                for c in range(ins[i].shape[0]):
                    line_step(i, turn + 1, c)
    if square:
        for c in range(depth):
            for i in pairs:
                if c < ins[i].shape[0]:
                    forward(i, c, across(along(tp_me)))
    for i, kind in enumerate(kinds):
        mode, axis = kind.split("_")
        n, me = sizes[axis], places[axis]
        if mode == "pair":
            chunks = ins[i].shape[0]
            others = relatives(partner) + ([across(along(partner))] if square else [])
            for origin in [partner] + others:
                for c in range(chunks):
                    arrived(i, axis, outs[i].at[origin, c], origin * chunks + c)
        elif mode != "line":
            for k in range(1, n):
                origin = lax.rem(me + n - k, n)
                arrived(i, axis, outs[i].at[origin], origin)
    for one in sent:
        one.wait_send()
    for i, happened, slot, origin, c in line_sent:

        @pl.when(happened)
        def _():
            pltpu.make_async_remote_copy(
                src_ref=outs[i].at[origin, c],
                dst_ref=outs[i].at[origin, c],
                send_sem=send_sems[i].at[slot],
                recv_sem=recv_sems[i].at[0],
                device_id=address("sp", lax.rem(sp_me + 1, sp_n)),
                device_id_type=MESH,
            ).wait_send()


def exchange(collective_id, *parts):
    sp_n, tp_n = lax.axis_size("sp"), lax.axis_size("tp")
    kinds = tuple(kind for kind, array in parts)
    arrays = [array for kind, array in parts]
    shapes, sends, recvs = [], [], []
    for kind, array in parts:
        mode, axis = kind.split("_")
        n = sp_n if axis == "sp" else tp_n
        shape = array.shape if mode == "swap" else (n,) + array.shape
        shapes.append(jax.ShapeDtypeStruct(shape, array.dtype))
        chunks = array.shape[0] if mode in ("pair", "line") else 1
        sends.append(pltpu.SemaphoreType.DMA(((2 * n + 8) * chunks,)))
        recvs.append(pltpu.SemaphoreType.DMA((n * chunks,)))
    return pl.pallas_call(
        functools.partial(exchange_kernel, kinds, sp_n, tp_n),
        out_shape=shapes,
        in_specs=[pl.BlockSpec(memory_space=pltpu.VMEM)] * len(parts),
        out_specs=[pl.BlockSpec(memory_space=pltpu.VMEM)] * len(parts),
        scratch_shapes=sends + recvs,
        compiler_params=pltpu.CompilerParams(
            collective_id=collective_id,
            has_side_effects=True,
            vmem_limit_bytes=56 * 1024 * 1024,
        ),
    )(*arrays)


def matmul(left, right):
    return jnp.dot(left, right, preferred_element_type=jnp.float32)


def einsum(text, left, right):
    return jnp.einsum(text, left, right, preferred_element_type=jnp.float32)


def body(
    target_rows,
    source_rows,
    target_gain,
    source_gain,
    query_weight,
    key_weight,
    value_weight,
    out_weight,
    out_cotangent,
):
    sp_n, tp_n = lax.axis_size("sp"), lax.axis_size("tp")
    width = target_rows.shape[1]
    local_width = query_weight.shape[1]
    local_heads = local_width // HEAD_DIM
    slot_heads = max(1, KV_HEADS // tp_n)
    copies = max(1, tp_n // KV_HEADS)
    per_slot = local_heads // slot_heads
    slot_width = slot_heads * HEAD_DIM
    score_scale = HEAD_DIM ** (-0.5)
    bf16 = jnp.bfloat16

    normed_t = normalize(target_rows, target_gain)
    normed_s = normalize(source_rows, source_gain)
    source_local = normed_s.shape[0]
    target_local = normed_t.shape[0]
    target_block = tp_n * target_local
    source_block = tp_n * source_local

    rows_in, cot_in = exchange(
        0,
        ("pair_tp", normed_t[None]),
        ("pair_tp", out_cotangent[None]),
    )
    queries = matmul(rows_in.reshape(target_block, width), query_weight).astype(bf16)
    d_attended = matmul(cot_in.reshape(target_block, width), out_weight.T).astype(bf16)
    halves = (2, key_weight.shape[0] // 2, key_weight.shape[1])
    split = (2, target_block // 2, local_width)
    key_full, value_full, all_queries, all_grads, cot_column = exchange(
        1,
        ("pair_tp", key_weight.reshape(halves)),
        ("pair_tp", value_weight.reshape(halves)),
        ("line_sp", queries.reshape(split)),
        ("line_sp", d_attended.reshape(split)),
        ("line_sp", out_cotangent[None]),
    )
    key_full = key_full.reshape(width, -1)
    value_full = value_full.reshape(width, -1)
    key_own = matmul(normed_s, key_full).astype(bf16)
    value_own = matmul(normed_s, value_full).astype(bf16)

    def to_slots(matrix):
        split = matrix.reshape(source_local, tp_n // copies, 1, slot_width)
        spread = jnp.broadcast_to(split, (source_local, tp_n // copies, copies, slot_width))
        return spread.reshape(source_local, tp_n, slot_width).transpose(1, 0, 2)

    slots = jnp.concatenate([to_slots(key_own), to_slots(value_own)], axis=2)
    (kv_block,) = exchange(2, ("swap_tp", slots))
    whole_rows = sp_n * target_block
    kv_block = kv_block.reshape(source_block, 2, slot_heads, HEAD_DIM)
    keys, values = kv_block[:, 0], kv_block[:, 1]
    head_shape = (whole_rows, slot_heads, per_slot, HEAD_DIM)
    query_view = all_queries.reshape(head_shape)
    grad_view = all_grads.reshape(head_shape)

    scores = einsum("tgqd,sgd->gqts", query_view, keys) * score_scale
    part_max = jnp.max(scores, axis=-1)
    weights = jnp.exp(scores - part_max[..., None])
    part_total = jnp.sum(weights, axis=-1)
    d_probs = einsum("tgqd,sgd->gqts", grad_view, values)
    part_delta = jnp.sum(weights * d_probs, axis=-1)
    part_sum = einsum("gqts,sgd->tgqd", weights.astype(bf16), values)
    stats = jnp.stack([part_max, part_total, part_delta]).reshape(3 * local_heads, whole_rows)
    (all_stats,) = exchange(3, ("gather_sp", stats))
    all_stats = all_stats.reshape(sp_n, 3, slot_heads, per_slot, whole_rows)
    row_max = jnp.max(all_stats[:, 0], axis=0)
    rescale = jnp.exp(all_stats[:, 0] - row_max)
    total = jnp.sum(all_stats[:, 1] * rescale, axis=0)
    delta = jnp.sum(all_stats[:, 2] * rescale, axis=0) / total
    local_scale = jnp.exp(part_max - row_max) / total

    attended_part = part_sum * local_scale.transpose(2, 0, 1)[..., None]
    attended_part = attended_part.reshape(sp_n, target_block, local_width).astype(bf16)
    probs = weights * local_scale[..., None]
    d_scores = (probs * (d_probs - delta[..., None])).astype(bf16)
    value_sum = einsum("gqts,tgqd->sgd", probs.astype(bf16), grad_view)
    key_sum = einsum("gqts,tgqd->sgd", d_scores, query_view) * score_scale
    d_query = einsum("gqts,sgd->tgqd", d_scores, keys) * score_scale
    d_query = d_query.reshape(sp_n, target_block, local_width).astype(bf16)
    grads = jnp.concatenate(
        [key_sum.reshape(source_block, slot_width), value_sum.reshape(source_block, slot_width)],
        axis=1,
    )
    grads = grads.reshape(tp_n, source_local, 2 * slot_width).astype(bf16)
    query_terms, attended_terms, grads_back, cot_all = exchange(
        4,
        ("swap_sp", d_query),
        ("swap_sp", attended_part),
        ("swap_tp", grads),
        ("pair_tp", cot_column.reshape(sp_n, target_local, width)),
    )
    query_grad = jnp.sum(query_terms.astype(jnp.float32), axis=0).astype(bf16)
    attended = jnp.sum(attended_terms.astype(jnp.float32), axis=0).astype(bf16)

    target_terms = matmul(query_grad, query_weight.T).astype(bf16)
    target_back, attended_all = exchange(
        5,
        ("swap_tp", target_terms.reshape(tp_n, target_local, width)),
        ("line_sp", attended.reshape(split)),
    )

    def from_slots(matrix):
        folded = matrix.reshape(tp_n // copies, copies, source_local, slot_width)
        folded = jnp.sum(folded.astype(jnp.float32), axis=1)
        return folded.transpose(1, 0, 2).reshape(source_local, -1).astype(bf16)

    key_grad = from_slots(grads_back[:, :, :slot_width])
    value_grad = from_slots(grads_back[:, :, slot_width:])
    d_normed_s = matmul(key_grad, key_full.T) + matmul(value_grad, value_full.T)
    source_grad = norm_back(source_rows, source_gain, d_normed_s)
    d_normed_t = jnp.sum(target_back.astype(jnp.float32), axis=0)
    target_grad = out_cotangent.astype(jnp.float32) + norm_back(
        target_rows, target_gain, d_normed_t
    )
    attended_rows = attended_all.reshape(sp_n, tp_n, target_local, local_width)
    out_weight_grad = jnp.einsum(
        "stlw,tsld->wd", attended_rows, cot_all, preferred_element_type=jnp.float32
    )
    return (target_grad, source_grad, out_weight_grad)


def fused_kernel(sp_n, tp_n, *refs):
    loads, stores = refs[:9], refs[9:12]
    target, source, tgain, sgain, qw, kw, vw, ow = refs[12:20]
    tgrad, sgrad, owg = refs[20:23]
    t_rx, c_rx, rows, cotf, w_rx, ns, q_all, d_all, kv_tx, kv_rx = refs[23:33]
    k2, v2, kvt, qc, dc, p_buf, dp_buf, own, st, st_rx, o_part = refs[33:44]
    o_tx, o_rx, att, attb, dq_f, dq_tx, dq_rx, qg, dk, dv = refs[44:54]
    g_tx, g_rx, gcat, tt, tp_rx, ts_tx, ts_rx, un = refs[54:62]
    send_s, t_s, c_s, w_s, far_s, cz_s, q_s, d_s, kv_s, near_s = refs[62:72]
    st_s, o_s, att_s, dq_s, g_s, tp_s, ts_s, load_s, store_s = refs[72:81]
    f32, bf16 = jnp.float32, jnp.bfloat16
    z, me = lax.axis_index("sp"), lax.axis_index("tp")
    core = lax.rem(me, 2)
    t_loc, width = target.shape
    s_loc = source.shape[0]
    slab, local_width = w_rx.shape[2], qw.shape[1]
    heads = local_width // HEAD_DIM
    t_block = tp_n * t_loc
    lanes = heads * t_block
    s_block = tp_n * s_loc
    pairs = w_rx.shape[0]
    scale = HEAD_DIM ** (-0.5)

    def across(i):
        return i + 2 - 4 * lax.rem(i // 2, 2)

    def along(i):
        return i + 4 - 8 * lax.rem(i // 4, 2)

    mate = me + 1 - 2 * core
    zt, zn = z + 2 - 4 * (z // 2), z + 1 - 2 * lax.rem(z, 2)
    zs = [lax.rem(z + k, sp_n) for k in range(1, sp_n)]
    ts = [lax.rem(me + k, tp_n) for k in range(1, tp_n)]

    barrier = pltpu.get_barrier_semaphore()
    for peer in zs:
        pl.semaphore_signal(barrier, inc=1, device_id=(peer, me), device_id_type=MESH)
    for peer in ts:
        pl.semaphore_signal(barrier, inc=1, device_id=(z, peer), device_id_type=MESH)

    for peer in ts:
        pl.semaphore_signal(barrier, inc=1, device_id=(zn, peer), device_id_type=MESH)

    sent = []
    ring = send_s.shape[0]

    def drain(one, when):
        if when is None:
            one.wait_send()
        else:
            pl.when(when)(lambda: one.wait_send())

    def push(src, dst, sem, zz, i, when=None):
        turn = len(sent) % ring
        if len(sent) >= ring:
            drain(*sent[len(sent) - ring])
        one = pltpu.make_async_remote_copy(
            src_ref=src,
            dst_ref=dst,
            send_sem=send_s.at[turn],
            recv_sem=sem,
            device_id=(zz, i),
            device_id_type=MESH,
        )
        sent.append((one, when))
        if when is None:
            one.start()
        else:
            pl.when(when)(lambda: one.start())

    def pull(ref, sem):
        pltpu.make_async_remote_copy(
            src_ref=ref,
            dst_ref=ref,
            send_sem=send_s.at[0],
            recv_sem=sem,
            device_id=(z, mate),
            device_id_type=MESH,
        ).wait_recv()

    kept = (target, source, tgain, sgain, qw, kw, vw, ow, c_rx.at[z, me])
    copies = [pltpu.make_async_copy(a, b, load_s.at[i]) for i, (a, b) in enumerate(zip(loads, kept))]
    for i in (0, 2, 8, 5, 6, 1, 3, 4, 7):
        copies[i].start()

    def store(i, a):
        one = pltpu.make_async_copy(a, stores[i], store_s.at[i])
        one.start()
        return one

    def nt(a, b):
        return lax.dot_general(a, b, (((1,), (1,)), ((), ())), preferred_element_type=f32)

    def nn(a, b):
        return jnp.dot(a, b, preferred_element_type=f32)

    class Gather:
        def __init__(self, slot, sem, far, depth):
            self.slot, self.sem, self.far, self.depth = slot, sem, far, depth

        def start(self):
            for peer in (across(me), along(me), mate):
                push(self.slot(me), self.slot(me), self.sem(me), z, peer)

        def half(self, origin, order):
            return self.slot(origin).at[self.depth[order] : self.depth[order + 1]]

        def mid(self):
            for order, origin in enumerate((across(me), along(me))):
                pull(self.slot(origin), self.sem(origin))
                piece = self.half(origin, order)
                push(piece, piece, self.far(order), z, along(me) if order == 0 else across(me))
            for origin in (across(me), along(me)):
                push(self.slot(origin), self.slot(origin), self.sem(origin), z, mate)

        def fin(self):
            origin = across(along(me))
            for order in range(2):
                pull(self.half(origin, order), self.far(order))
            push(self.slot(origin), self.slot(origin), self.sem(origin), z, mate)

        def rest(self):
            for origin in (mate, across(mate), along(mate), across(along(mate))):
                pull(self.slot(origin), self.sem(origin))

    copies[0].wait()
    copies[2].wait()
    t_rx[me] = normalize(target[...], tgain[...])
    copies[8].wait()
    pl.semaphore_wait(barrier, sp_n - 1 + 2 * (tp_n - 1))

    some, more = (0, t_loc // 2 // 8 * 8, t_loc), (0, slab // 2, slab)
    t_all = Gather(lambda o: t_rx.at[o], lambda o: t_s.at[o], lambda k: far_s.at[k], some)
    c_all = [
        Gather(
            lambda o, p=p: c_rx.at[p, o],
            lambda o, p=p: c_s.at[p * tp_n + o],
            lambda k, n=n: far_s.at[2 * n + 2 + k],
            some,
        )
        for n, p in enumerate([z] + zs)
    ]
    c_own, c_far = c_all[0], c_all[1:]
    w_all = [
        Gather(
            lambda o, c=c: w_rx.at[c, o],
            lambda o, c=c: w_s.at[c * tp_n + o],
            lambda k, c=c: far_s.at[2 * (sp_n + 1 + c) + k],
            more,
        )
        for c in range(pairs)
    ]

    t_all.start()
    for peer in zs:
        push(c_rx.at[z, me], c_rx.at[z, me], cz_s.at[z], peer, me)
    copies[5].wait()
    copies[6].wait()
    half = w_rx.shape[3]
    for c in range(pairs):
        part = (kw, vw)[c // 2]
        w_rx[c, me] = part[:, (c % 2) * half : (c % 2 + 1) * half]
    w_all[0].start()
    copies[1].wait()
    copies[3].wait()
    step = min(s_loc, 32)
    for i in range(0, s_loc, step):
        ns[i : i + step] = normalize(source[i : i + step], sgain[...])
    w_all[1].start()
    t_all.mid()
    w_all[0].mid()
    w_all[2].start()
    t_all.fin()
    t_all.rest()
    for o in range(tp_n):
        rows[o * t_loc : (o + 1) * t_loc] = t_rx[o]
    copies[4].wait()
    q_all[0] = (nn(rows[...], qw[...]).astype(bf16) * scale).astype(bf16)
    push(q_all.at[0], q_all.at[1], q_s.at[0], zt, me)
    w_all[1].mid()
    w_all[3].start()

    packed = s_loc // 2

    def split_kv(c):
        w_all[c].rest()
        total = nn(ns[:, :slab], w_rx[c, 0])
        for o in range(1, tp_n):
            total += nn(ns[:, o * slab : (o + 1) * slab], w_rx[c, o])
        total = total.astype(bf16)
        for j in range(tp_n // 2):
            head = (c % 2) * (tp_n // 2) + j
            part = total[:, j * HEAD_DIM : (j + 1) * HEAD_DIM]
            part = jnp.concatenate([part[:packed], part[packed:]], axis=1)
            kv_tx[c // 2, head] = part

            @pl.when(me == head)
            def _():
                kv_rx[0, c // 2, head] = part

            sem = kv_s.at[(c // 2) * tp_n + me]
            push(kv_tx.at[c // 2, head], kv_rx.at[0, c // 2, me], sem, z, head, me != head)
            if c // 2 == 1:
                push(kv_tx.at[1, head], kv_rx.at[1, 1, me], near_s.at[1 + me], zn, head)

    def unpack(w, kind):
        if w == 0:
            for o in ts:
                pull(kv_rx.at[0, kind, o], kv_s.at[kind * tp_n + o])
            if kind == 0:
                push(kv_rx.at[0, 0], kv_rx.at[1, 0], near_s.at[0], zn, me)
        elif kind == 0:
            pull(kv_rx.at[1, 0], near_s.at[0])
        else:
            for o in range(tp_n):
                pull(kv_rx.at[1, 1, o], near_s.at[1 + o])
        out = (k2, v2)[kind]
        for o in range(tp_n):
            part = kv_rx[w, kind, o]
            out[w, o * s_loc : o * s_loc + packed] = part[:, :HEAD_DIM]
            out[w, o * s_loc + packed : (o + 1) * s_loc] = part[:, HEAD_DIM:]

    groups = lanes // 128

    def fold(op, x, n=4):
        size = x.shape[0] // n
        parts = [
            op(x[i * size : (i + 1) * size].reshape(size // 8, 8, x.shape[1]), axis=0)
            for i in range(n)
        ]
        both = jnp.maximum if op is jnp.max else jnp.add
        return op(functools.reduce(both, parts), axis=0, keepdims=True)

    def line(x):
        return jnp.concatenate([x[g : g + 1] for g in range(groups)], axis=1)

    def take(u, full, sems, out):
        if u == 1:
            pull(full.at[1], sems.at[0])
        for h in range(heads):
            cols = slice(h * HEAD_DIM, (h + 1) * HEAD_DIM)
            out[u, h * t_block : (h + 1) * t_block] = full[u, :, cols]

    def weigh(u, w):
        if w == 0:
            take(u, q_all, q_s, qc)
        score = nt(k2[w], qc[u])
        top = fold(jnp.max, score)
        weight = jnp.exp(score - top)
        own[u, w, 0:1] = top
        own[u, w, 1:2] = fold(jnp.sum, weight)
        p_buf[u, w] = weight

    def turn_kv(w):
        for o in range(tp_n):
            part = slice(o * s_loc, (o + 1) * s_loc)
            both = jnp.concatenate([k2[w, part], v2[w, part]], axis=1)
            kvt[w, :, part] = both.astype(f32).T.astype(bf16)

    def first(u, w):
        if w == 0:
            take(u, d_all, d_s, dc)
        weight = p_buf[u, w]
        d_prob = nt(v2[w], dc[u])
        own[u, w, 2:3] = fold(jnp.sum, weight * d_prob)
        dp_buf[u, w] = d_prob
        o_part[u, w] = nn(kvt[w, HEAD_DIM:], weight.astype(bf16))

    def join(u):
        top = jnp.maximum(own[u, 0, 0:1], own[u, 1, 0:1])
        lifts = [jnp.exp(own[u, w, 0:1] - top) for w in range(2)]
        total = sum(own[u, w, 1:2] * lifts[w] for w in range(2))
        inner = sum(own[u, w, 2:3] * lifts[w] for w in range(2)) / total
        o_tx[u] = (sum(o_part[u, w] * lifts[w] for w in range(2)) / total).astype(bf16)
        for k, value in enumerate((top + jnp.log(total), inner)):
            for g in range(groups):
                row = groups * k + g
                st[u, row : row + 1] = value[:, g * 128 : (g + 1) * 128]

    cut = lanes // 2 // 128 * 128
    spans = [slice(0, cut), slice(cut, lanes)] if cut else [slice(0, lanes)]

    w_all[0].fin()
    split_kv(0)
    w_all[2].mid()
    c_own.start()
    w_all[1].fin()
    split_kv(1)
    w_all[3].mid()
    w_all[2].fin()
    unpack(0, 0)
    c_own.mid()
    weigh(0, 0)
    w_all[3].fin()
    split_kv(2)
    split_kv(3)
    c_own.fin()
    c_own.rest()
    for o in range(tp_n):
        cotf[z, o * t_loc : (o + 1) * t_loc] = c_rx[z, o]
    copies[7].wait()
    d_all[0] = nt(cotf[z], ow[...]).astype(bf16)
    push(d_all.at[0], d_all.at[1], d_s.at[0], zt, me)
    for k, p in enumerate(zs):
        pull(c_rx.at[p, me], cz_s.at[p])
        c_far[k].start()
    weigh(1, 0)
    unpack(1, 0)
    weigh(0, 1)
    weigh(1, 1)
    unpack(0, 1)
    turn_kv(0)
    first(0, 0)
    unpack(1, 1)
    turn_kv(1)
    first(0, 1)
    join(0)
    push(st.at[0], st_rx.at[0], st_s.at[0], zt, me)
    c_far[0].mid()
    first(1, 0)
    first(1, 1)
    join(1)
    push(st.at[1], st_rx.at[1], st_s.at[1], zt, me)
    for n, span in enumerate(spans):
        push(o_tx.at[1, :, span], o_rx.at[:, span], o_s.at[n], zt, me)

    def stats(u):
        logs = [st[u, :groups], st_rx[1 - u, :groups]]
        inners = [st[u, groups:], st_rx[1 - u, groups:]]
        top = jnp.maximum(*logs)
        log_total = top + jnp.log(sum(jnp.exp(x - top) for x in logs))
        lifts = [jnp.exp(x - log_total) for x in logs]
        return log_total, lifts, inners[0] * lifts[0] + inners[1] * lifts[1]

    def attend():
        lifts = [line(x) for x in stats(0)[1]]
        for n, span in enumerate(spans):
            pull(o_rx.at[:, span], o_s.at[n])
            mine = o_tx[0, :, span].astype(f32) * lifts[0][:, span]
            other = o_rx[:, span].astype(f32) * lifts[1][:, span]
            att[z, :, span] = (mine + other).astype(bf16)
            for peer in zs:
                part = att.at[z, :, span]
                push(part, part, att_s.at[n * sp_n + z], peer, me)

    def second(u, w, start):
        log_total, lifts, inner = stats(u)
        prob = p_buf[u, w] * jnp.exp(own[u, w, 0:1] - line(log_total))
        d_score = (prob * (dp_buf[u, w] - line(inner))).astype(bf16)
        prob = prob.astype(bf16)
        d_value, d_key = nn(prob, dc[u]), nn(d_score, qc[u])
        dv[w] = d_value if u == 1 else dv[w] + d_value
        dk[w] = d_key if u == 1 else dk[w] + d_key
        d_query = nn(kvt[w, :HEAD_DIM], d_score)
        dq_f[u] = d_query if start else dq_f[u] + d_query

    def send_g(w, plane):
        for o in range(tp_n):
            part = slice(o * s_loc, (o + 1) * s_loc)
            g_tx[w, o] = jnp.concatenate([dk[w, part], dv[w, part]], axis=1).astype(bf16)
        for o in ts + ([me] if w == 1 else []):
            push(g_tx.at[w, o], g_rx.at[w, me], g_s.at[w * tp_n + me], plane, o)

    c_far[1].mid()
    pull(st_rx.at[0], st_s.at[0])
    second(1, 0, True)
    c_far[2].mid()
    second(1, 1, False)
    dq_tx[...] = dq_f[1].astype(bf16)
    push(dq_tx, dq_rx, dq_s.at[0], zt, me)
    pull(st_rx.at[1], st_s.at[1])
    second(0, 1, True)
    send_g(1, zn)
    second(0, 0, False)
    send_g(0, z)
    g_rx[0, me] = g_tx[0, me]
    pull(dq_rx, dq_s.at[0])
    summed = (dq_f[0] + dq_rx[...].astype(f32)) * scale
    summed = summed.T
    for h in range(heads):
        piece = summed[h * t_block : (h + 1) * t_block].astype(bf16)
        qg[:, h * HEAD_DIM : (h + 1) * HEAD_DIM] = piece
    wide = 512

    def terms(j, carry):
        cols = pl.ds(pl.multiple_of(j * wide, wide), wide)
        value = nt(qg[...], qw[cols])
        for o in range(tp_n):
            tt[o, :, cols] = value[o * t_loc : (o + 1) * t_loc].astype(bf16)
        return carry

    lax.fori_loop(0, width // wide, terms, 0)
    chips = tp_n // 2
    for c in range(chips):
        push(tt.at[2 * c + 1 - core], tp_rx.at[c], tp_s.at[c], z, mate)
    attend()
    tile = 256

    for c in range(chips):
        pull(tp_rx.at[c], tp_s.at[c])
        ts_tx[c] = (tt[2 * c + core].astype(f32) + tp_rx[c].astype(f32)).astype(bf16)
    for r, peer in enumerate((across(along(me)), across(me), along(me))):
        push(ts_tx.at[peer // 2], ts_rx.at[r], ts_s.at[r], z, peer)
    for item in c_far:
        item.fin()
    side = tp_n * HEAD_DIM
    for o in ts:
        pull(g_rx.at[0, o], g_s.at[o])
    for o in range(tp_n):
        pull(g_rx.at[1, o], g_s.at[tp_n + o])
        part = (g_rx[0, o].astype(f32) + g_rx[1, o].astype(f32)).astype(bf16)
        gcat[:, o * HEAD_DIM : (o + 1) * HEAD_DIM] = part[:, :HEAD_DIM]
        gcat[:, side + o * HEAD_DIM : side + (o + 1) * HEAD_DIM] = part[:, HEAD_DIM:]

    def upstream(o, carry):
        cols = pl.ds(pl.multiple_of(o * slab, slab), slab)
        total = nt(gcat[:, : 4 * HEAD_DIM], w_rx[0, o])
        for c in range(1, pairs):
            total += nt(gcat[:, c * 4 * HEAD_DIM : (c + 1) * 4 * HEAD_DIM], w_rx[c, o])
        un[:, cols] = total
        return carry

    lax.fori_loop(0, tp_n, upstream, 0)
    for i in range(0, s_loc, step):
        part = slice(i, i + step)
        sgrad[part] = norm_back(source[part], sgain[...], un[part])
    done = [store(1, sgrad)]
    for k, p in enumerate(zs):
        c_far[k].rest()
        for o in range(tp_n):
            cotf[p, o * t_loc : (o + 1) * t_loc] = c_rx[p, o]
    for p in zs:
        for n, span in enumerate(spans):
            pull(att.at[p, :, span], att_s.at[n * sp_n + p])
    for b in range(sp_n):
        for h in range(heads):
            piece = att[b, :, h * t_block : (h + 1) * t_block]
            attb[b, h * HEAD_DIM : (h + 1) * HEAD_DIM] = piece

    def weight_grad(j, carry):
        cols = pl.ds(pl.multiple_of(j * tile, tile), tile)
        owg[:, cols] = sum(nn(attb[b], cotf[b, :, cols]) for b in range(sp_n))
        return carry

    rest = width // tile // 4
    for n in range(4):
        lax.fori_loop(n * rest, (n + 1) * rest, weight_grad, 0)
        part = slice(n * rest * tile, (n + 1) * rest * tile)
        one = pltpu.make_async_copy(owg.at[:, part], stores[2].at[:, part], store_s.at[2 + n])
        one.start()
        done.append(one)
    mine = ts_tx[me // 2].astype(f32)
    for r in range(3):
        pull(ts_rx.at[r], ts_s.at[r])
    mine = mine + sum(ts_rx[r].astype(f32) for r in range(3))
    tgrad[...] = c_rx[z, me].astype(f32) + norm_back(target[...], tgain[...], mine)
    done.append(store(0, tgrad))

    for one, when in sent[-ring:]:
        drain(one, when)
    for one in done:
        one.wait()


def finish_kernel(*refs):
    ins, outs, held = refs[:3], refs[3:6], refs[6:9]
    in_sems, out_sems = refs[9:11]
    pieces = []
    for i in (2, 1, 0):
        size = ins[i].shape[0]
        step = max(size // 4 // 8 * 8, 8)
        for at in range(0, size, step):
            part = pl.ds(at, min(step, size - at))
            pieces.append((ins[i].at[part], held[i].at[part], outs[i].at[part]))
    for k, (a, b, c) in enumerate(pieces):
        pltpu.make_async_copy(a, b, in_sems.at[k]).start()
    for k, (a, b, c) in enumerate(pieces):
        pltpu.make_async_copy(a, b, in_sems.at[k]).wait()
        pltpu.make_async_copy(b, c, out_sems.at[k]).start()
    for k, (a, b, c) in enumerate(pieces):
        pltpu.make_async_copy(b, c, out_sems.at[k]).wait()


def finish(*arrays):
    return pl.pallas_call(
        finish_kernel,
        out_shape=[jax.ShapeDtypeStruct(a.shape, a.dtype) for a in arrays],
        in_specs=[pl.BlockSpec(memory_space=pltpu.HBM)] * 3,
        out_specs=[pl.BlockSpec(memory_space=pl.ANY)] * 3,
        scratch_shapes=[pltpu.VMEM(a.shape, a.dtype) for a in arrays]
        + [pltpu.SemaphoreType.DMA((12,)), pltpu.SemaphoreType.DMA((12,))],
        compiler_params=pltpu.CompilerParams(vmem_limit_bytes=67043328),
    )(*arrays)


def fused_body(
    target_rows,
    source_rows,
    target_gain,
    source_gain,
    query_weight,
    key_weight,
    value_weight,
    out_weight,
    out_cotangent,
):
    sp_n, tp_n = lax.axis_size("sp"), lax.axis_size("tp")
    t_loc, width = target_rows.shape
    s_loc = source_rows.shape[0]
    local_width = query_weight.shape[1]
    heads = local_width // HEAD_DIM
    t_block, s_block = tp_n * t_loc, tp_n * s_loc
    lanes = heads * t_block
    slab = key_weight.shape[0]
    pairs = KV_HEADS // 2
    two = 2 * HEAD_DIM
    f32, bf16 = jnp.float32, jnp.bfloat16
    vmem, sem = pltpu.VMEM, pltpu.SemaphoreType.DMA
    sends = 48
    scratch = [
        vmem((t_loc, width), bf16),
        vmem((s_loc, width), bf16),
        vmem((1, width), f32),
        vmem((1, width), f32),
        vmem((width, local_width), bf16),
        vmem((slab, key_weight.shape[1]), bf16),
        vmem((slab, key_weight.shape[1]), bf16),
        vmem((local_width, width), bf16),
        vmem((t_loc, width), f32),
        vmem((s_loc, width), f32),
        vmem((local_width, width), f32),
        vmem((tp_n, t_loc, width), bf16),
        vmem((sp_n, tp_n, t_loc, width), bf16),
        vmem((t_block, width), bf16),
        vmem((sp_n, t_block, width), bf16),
        vmem((pairs, tp_n, slab, 2 * two), bf16),
        vmem((s_loc, width), bf16),
        vmem((2, t_block, local_width), bf16),
        vmem((2, t_block, local_width), bf16),
        vmem((2, tp_n, s_loc // 2, two), bf16),
        vmem((2, 2, tp_n, s_loc // 2, two), bf16),
        vmem((2, s_block, HEAD_DIM), bf16),
        vmem((2, s_block, HEAD_DIM), bf16),
        vmem((2, two, s_block), bf16),
        vmem((2, lanes, HEAD_DIM), bf16),
        vmem((2, lanes, HEAD_DIM), bf16),
        vmem((2, 2, s_block, lanes), f32),
        vmem((2, 2, s_block, lanes), f32),
        vmem((2, 2, 3, lanes), f32),
        vmem((2, lanes // 64, 128), f32),
        vmem((2, lanes // 64, 128), f32),
        vmem((2, 2, HEAD_DIM, lanes), f32),
        vmem((2, HEAD_DIM, lanes), bf16),
        vmem((HEAD_DIM, lanes), bf16),
        vmem((sp_n, HEAD_DIM, lanes), bf16),
        vmem((sp_n, local_width, t_block), bf16),
        vmem((2, HEAD_DIM, lanes), f32),
        vmem((HEAD_DIM, lanes), bf16),
        vmem((HEAD_DIM, lanes), bf16),
        vmem((t_block, local_width), bf16),
        vmem((2, s_block, HEAD_DIM), f32),
        vmem((2, s_block, HEAD_DIM), f32),
        vmem((2, tp_n, s_loc, two), bf16),
        vmem((2, tp_n, s_loc, two), bf16),
        vmem((s_loc, tp_n * two), bf16),
        vmem((tp_n, t_loc, width), bf16),
        vmem((tp_n // 2, t_loc, width), bf16),
        vmem((tp_n // 2, t_loc, width), bf16),
        vmem((3, t_loc, width), bf16),
        vmem((s_loc, width), f32),
        sem((sends,)),
        sem((tp_n,)),
        sem((sp_n * tp_n,)),
        sem((pairs * tp_n,)),
        sem((2 * (sp_n + 1 + pairs),)),
        sem((sp_n,)),
        sem((1,)),
        sem((1,)),
        sem((2 * tp_n,)),
        sem((1 + tp_n,)),
        sem((2,)),
        sem((2,)),
        sem((2 * sp_n,)),
        sem((1,)),
        sem((2 * tp_n,)),
        sem((tp_n // 2,)),
        sem((3,)),
        sem((9,)),
        sem((6,)),
    ]
    results = pl.pallas_call(
        functools.partial(fused_kernel, sp_n, tp_n),
        out_shape=[
            jax.ShapeDtypeStruct((t_loc, width), f32),
            jax.ShapeDtypeStruct((s_loc, width), f32),
            jax.ShapeDtypeStruct((local_width, width), f32),
        ],
        in_specs=[pl.BlockSpec(memory_space=pl.ANY)] * 9,
        out_specs=[pl.BlockSpec(memory_space=pl.ANY)] * 3,
        scratch_shapes=scratch,
        compiler_params=pltpu.CompilerParams(
            collective_id=0,
            has_side_effects=True,
            vmem_limit_bytes=67043328,
        ),
    )(
        target_rows,
        source_rows,
        target_gain[None],
        source_gain[None],
        query_weight,
        key_weight,
        value_weight,
        out_weight,
        out_cotangent,
    )
    return tuple(finish(*results))


def choose(*args):
    square = lax.axis_size("tp") == 8 and KV_HEADS == 8 and lax.axis_size("sp") == 4
    lanes = lax.axis_size("tp") * args[0].shape[0] * args[4].shape[1] // HEAD_DIM
    if square and lanes % 128 == 0 and lanes <= 1024:
        return fused_body(*args)
    return body(*args)


def solution(mesh):
    return jax.shard_map(
        choose,
        mesh=mesh,
        in_specs=(
            P(("sp", "tp"), None),
            P(("sp", "tp"), None),
            P(),
            P(),
            P(None, "tp"),
            P("tp", None),
            P("tp", None),
            P("tp", None),
            P(("sp", "tp"), None),
        ),
        out_specs=(P(("sp", "tp"), None), P(("sp", "tp"), None), P("tp", None)),
        check_vma=False,
    )
```

```python
import functools

import jax
import jax.numpy as jnp
from jax import lax
from jax.experimental import pallas as pl
from jax.experimental.pallas import tpu as pltpu
from jax.sharding import PartitionSpec as P

HEAD_DIM = 64
KV_HEADS = 8
EPSILON = 1e-06
MESH = pl.DeviceIdType.MESH


def normalize(matrix, gain_vector):
    widened = matrix.astype(jnp.float32)
    factor = lax.rsqrt(jnp.mean(widened * widened, axis=-1, keepdims=True) + EPSILON)
    return (widened * factor * gain_vector).astype(jnp.bfloat16)


def norm_back(matrix, gain_vector, upstream):
    widened = matrix.astype(jnp.float32)
    factor = lax.rsqrt(jnp.mean(widened * widened, axis=-1, keepdims=True) + EPSILON)
    weighted = upstream * gain_vector
    inner_sum = jnp.mean(weighted * widened, axis=-1, keepdims=True)
    return factor * weighted - widened * factor**3 * inner_sum


def exchange_kernel(kinds, sp_n, tp_n, *refs):
    count = len(kinds)
    ins, outs = refs[:count], refs[count : 2 * count]
    send_sems, recv_sems = refs[2 * count : 3 * count], refs[3 * count :]
    sp_me, tp_me = lax.axis_index("sp"), lax.axis_index("tp")
    sizes, places = {"sp": sp_n, "tp": tp_n}, {"sp": sp_me, "tp": tp_me}

    def address(axis, peer):
        return (peer, tp_me) if axis == "sp" else (sp_me, peer)

    axes = sorted({kind.split("_")[1] for kind in kinds})
    barrier = pltpu.get_barrier_semaphore()
    for axis in axes:
        for k in range(1, sizes[axis]):
            peer = lax.rem(places[axis] + k, sizes[axis])
            pl.semaphore_signal(barrier, inc=1, device_id=address(axis, peer), device_id_type=MESH)
    pl.semaphore_wait(barrier, sum(sizes[axis] - 1 for axis in axes))

    def copy(i, axis, source, slot, k, peer):
        return pltpu.make_async_remote_copy(
            src_ref=source,
            dst_ref=outs[i].at[slot],
            send_sem=send_sems[i].at[k],
            recv_sem=recv_sems[i].at[slot],
            device_id=address(axis, peer),
            device_id_type=MESH,
        )

    sent = []
    used = [0] * count

    def send(i, axis, source, target, recv, peer, keep=True):
        one = pltpu.make_async_remote_copy(
            src_ref=source,
            dst_ref=target,
            send_sem=send_sems[i].at[used[i]],
            recv_sem=recv_sems[i].at[recv],
            device_id=address(axis, peer),
            device_id_type=MESH,
        )
        used[i] += 1
        one.start()
        if keep:
            sent.append(one)
        return one

    def arrived(i, axis, target, recv):
        pltpu.make_async_remote_copy(
            src_ref=target,
            dst_ref=target,
            send_sem=send_sems[i].at[0],
            recv_sem=recv_sems[i].at[recv],
            device_id=address(axis, lax.rem(places[axis] + 1, sizes[axis])),
            device_id_type=MESH,
        ).wait_recv()

    square = tp_n == 8
    partner = tp_me + 1 - 2 * lax.rem(tp_me, 2)

    def across(index):
        return index + 2 - 4 * lax.rem(index // 2, 2)

    def along(index):
        return index + 4 - 8 * lax.rem(index // 4, 2)

    def relatives(index):
        if square:
            return [across(index), along(index)]
        return [lax.rem(index + 2 * k, tp_n) for k in range(1, tp_n // 2)]

    def forward(i, c, origin):
        chunks = ins[i].shape[0]
        piece, recv = outs[i].at[origin, c], origin * chunks + c
        arrived(i, "tp", piece, recv)
        send(i, "tp", piece, piece, recv, partner)
        return piece, recv

    line_sent = []
    depth = max([ins[i].shape[0] for i in range(count) if kinds[i] == "pair_tp"], default=0)
    for c in range(depth):
        for i, kind in enumerate(kinds):
            if kind == "pair_tp" and c < ins[i].shape[0]:
                chunks = ins[i].shape[0]
                for peer in relatives(tp_me) + [partner]:
                    piece = outs[i].at[tp_me, c]
                    send(i, "tp", ins[i].at[c], piece, tp_me * chunks + c, peer)
    for i, kind in enumerate(kinds):
        mode, axis = kind.split("_")
        n, me = sizes[axis], places[axis]
        if mode == "line":
            for step in (1, -1):
                inside = (me < n - 1) if step == 1 else (me > 0)
                for c in range(ins[i].shape[0]):
                    line_sent.append((i, inside, used[i], me, c))
                    recv = me * ins[i].shape[0] + c

                    @pl.when(inside)
                    def _():
                        piece = outs[i].at[me, c]
                        send(i, axis, ins[i].at[c], piece, recv, me + step, keep=False)
        elif mode != "pair":
            for k in range(1, n):
                peer = lax.rem(me + k, n)
                source = ins[i] if mode == "gather" else ins[i].at[peer]
                send(i, axis, source, outs[i].at[me], me, peer)
    for i, kind in enumerate(kinds):
        mode, axis = kind.split("_")
        me = places[axis]
        outs[i][me] = ins[i][me] if mode == "swap" else ins[i][...]

    def line_step(i, far, c):
        n, me = sp_n, sp_me
        chunks = ins[i].shape[0]
        for step in (1, -1):
            origin = me - step * far
            valid = (origin >= 0) if step == 1 else (origin <= n - 1)
            onward = (valid & (me < n - 1)) if step == 1 else (valid & (me > 0))

            @pl.when(valid)
            def _():
                arrived(i, "sp", outs[i].at[origin, c], origin * chunks + c)

            if far < n - 1:
                line_sent.append((i, onward, used[i], origin, c))

                @pl.when(onward)
                def _():
                    piece = outs[i].at[origin, c]
                    recv = origin * chunks + c
                    send(i, "sp", piece, piece, recv, me + step, keep=False)

    def pair_step(i, c):
        me = tp_me
        chunks = ins[i].shape[0]
        for order, origin in enumerate(relatives(me)):
            piece, recv = forward(i, c, origin)
            if square and order == (i + c) % 2:
                send(i, "tp", piece, piece, recv, along(me) if order == 0 else across(me))

    lines = [i for i in range(count) if kinds[i] == "line_sp"]
    pairs = [i for i in range(count) if kinds[i] == "pair_tp"]
    for turn in range(max(depth, sp_n - 1 if lines else 0)):
        for i in pairs:
            if turn < ins[i].shape[0]:
                pair_step(i, turn)
        for i in lines:
            if turn + 1 < sp_n:
                for c in range(ins[i].shape[0]):
                    line_step(i, turn + 1, c)
    if square:
        for c in range(depth):
            for i in pairs:
                if c < ins[i].shape[0]:
                    forward(i, c, across(along(tp_me)))
    for i, kind in enumerate(kinds):
        mode, axis = kind.split("_")
        n, me = sizes[axis], places[axis]
        if mode == "pair":
            chunks = ins[i].shape[0]
            others = relatives(partner) + ([across(along(partner))] if square else [])
            for origin in [partner] + others:
                for c in range(chunks):
                    arrived(i, axis, outs[i].at[origin, c], origin * chunks + c)
        elif mode != "line":
            for k in range(1, n):
                origin = lax.rem(me + n - k, n)
                arrived(i, axis, outs[i].at[origin], origin)
    for one in sent:
        one.wait_send()
    for i, happened, slot, origin, c in line_sent:

        @pl.when(happened)
        def _():
            pltpu.make_async_remote_copy(
                src_ref=outs[i].at[origin, c],
                dst_ref=outs[i].at[origin, c],
                send_sem=send_sems[i].at[slot],
                recv_sem=recv_sems[i].at[0],
                device_id=address("sp", lax.rem(sp_me + 1, sp_n)),
                device_id_type=MESH,
            ).wait_send()


def exchange(collective_id, *parts):
    sp_n, tp_n = lax.axis_size("sp"), lax.axis_size("tp")
    kinds = tuple(kind for kind, array in parts)
    arrays = [array for kind, array in parts]
    shapes, sends, recvs = [], [], []
    for kind, array in parts:
        mode, axis = kind.split("_")
        n = sp_n if axis == "sp" else tp_n
        shape = array.shape if mode == "swap" else (n,) + array.shape
        shapes.append(jax.ShapeDtypeStruct(shape, array.dtype))
        chunks = array.shape[0] if mode in ("pair", "line") else 1
        sends.append(pltpu.SemaphoreType.DMA(((2 * n + 8) * chunks,)))
        recvs.append(pltpu.SemaphoreType.DMA((n * chunks,)))
    return pl.pallas_call(
        functools.partial(exchange_kernel, kinds, sp_n, tp_n),
        out_shape=shapes,
        in_specs=[pl.BlockSpec(memory_space=pltpu.VMEM)] * len(parts),
        out_specs=[pl.BlockSpec(memory_space=pltpu.VMEM)] * len(parts),
        scratch_shapes=sends + recvs,
        compiler_params=pltpu.CompilerParams(
            collective_id=collective_id,
            has_side_effects=True,
            vmem_limit_bytes=56 * 1024 * 1024,
        ),
    )(*arrays)


def matmul(left, right):
    return jnp.dot(left, right, preferred_element_type=jnp.float32)


def einsum(text, left, right):
    return jnp.einsum(text, left, right, preferred_element_type=jnp.float32)


def body(
    target_rows,
    source_rows,
    target_gain,
    source_gain,
    query_weight,
    key_weight,
    value_weight,
    out_weight,
    out_cotangent,
):
    sp_n, tp_n = lax.axis_size("sp"), lax.axis_size("tp")
    width = target_rows.shape[1]
    local_width = query_weight.shape[1]
    local_heads = local_width // HEAD_DIM
    slot_heads = max(1, KV_HEADS // tp_n)
    copies = max(1, tp_n // KV_HEADS)
    per_slot = local_heads // slot_heads
    slot_width = slot_heads * HEAD_DIM
    score_scale = HEAD_DIM ** (-0.5)
    bf16 = jnp.bfloat16

    normed_t = normalize(target_rows, target_gain)
    normed_s = normalize(source_rows, source_gain)
    source_local = normed_s.shape[0]
    target_local = normed_t.shape[0]
    target_block = tp_n * target_local
    source_block = tp_n * source_local

    rows_in, cot_in = exchange(
        0,
        ("pair_tp", normed_t[None]),
        ("pair_tp", out_cotangent[None]),
    )
    queries = matmul(rows_in.reshape(target_block, width), query_weight).astype(bf16)
    d_attended = matmul(cot_in.reshape(target_block, width), out_weight.T).astype(bf16)
    halves = (2, key_weight.shape[0] // 2, key_weight.shape[1])
    split = (2, target_block // 2, local_width)
    key_full, value_full, all_queries, all_grads, cot_column = exchange(
        1,
        ("pair_tp", key_weight.reshape(halves)),
        ("pair_tp", value_weight.reshape(halves)),
        ("line_sp", queries.reshape(split)),
        ("line_sp", d_attended.reshape(split)),
        ("line_sp", out_cotangent[None]),
    )
    key_full = key_full.reshape(width, -1)
    value_full = value_full.reshape(width, -1)
    key_own = matmul(normed_s, key_full).astype(bf16)
    value_own = matmul(normed_s, value_full).astype(bf16)

    def to_slots(matrix):
        split = matrix.reshape(source_local, tp_n // copies, 1, slot_width)
        spread = jnp.broadcast_to(split, (source_local, tp_n // copies, copies, slot_width))
        return spread.reshape(source_local, tp_n, slot_width).transpose(1, 0, 2)

    slots = jnp.concatenate([to_slots(key_own), to_slots(value_own)], axis=2)
    (kv_block,) = exchange(2, ("swap_tp", slots))
    whole_rows = sp_n * target_block
    kv_block = kv_block.reshape(source_block, 2, slot_heads, HEAD_DIM)
    keys, values = kv_block[:, 0], kv_block[:, 1]
    head_shape = (whole_rows, slot_heads, per_slot, HEAD_DIM)
    query_view = all_queries.reshape(head_shape)
    grad_view = all_grads.reshape(head_shape)

    scores = einsum("tgqd,sgd->gqts", query_view, keys) * score_scale
    part_max = jnp.max(scores, axis=-1)
    weights = jnp.exp(scores - part_max[..., None])
    part_total = jnp.sum(weights, axis=-1)
    d_probs = einsum("tgqd,sgd->gqts", grad_view, values)
    part_delta = jnp.sum(weights * d_probs, axis=-1)
    part_sum = einsum("gqts,sgd->tgqd", weights.astype(bf16), values)
    stats = jnp.stack([part_max, part_total, part_delta]).reshape(3 * local_heads, whole_rows)
    (all_stats,) = exchange(3, ("gather_sp", stats))
    all_stats = all_stats.reshape(sp_n, 3, slot_heads, per_slot, whole_rows)
    row_max = jnp.max(all_stats[:, 0], axis=0)
    rescale = jnp.exp(all_stats[:, 0] - row_max)
    total = jnp.sum(all_stats[:, 1] * rescale, axis=0)
    delta = jnp.sum(all_stats[:, 2] * rescale, axis=0) / total
    local_scale = jnp.exp(part_max - row_max) / total

    attended_part = part_sum * local_scale.transpose(2, 0, 1)[..., None]
    attended_part = attended_part.reshape(sp_n, target_block, local_width).astype(bf16)
    probs = weights * local_scale[..., None]
    d_scores = (probs * (d_probs - delta[..., None])).astype(bf16)
    value_sum = einsum("gqts,tgqd->sgd", probs.astype(bf16), grad_view)
    key_sum = einsum("gqts,tgqd->sgd", d_scores, query_view) * score_scale
    d_query = einsum("gqts,sgd->tgqd", d_scores, keys) * score_scale
    d_query = d_query.reshape(sp_n, target_block, local_width).astype(bf16)
    grads = jnp.concatenate(
        [key_sum.reshape(source_block, slot_width), value_sum.reshape(source_block, slot_width)],
        axis=1,
    )
    grads = grads.reshape(tp_n, source_local, 2 * slot_width).astype(bf16)
    query_terms, attended_terms, grads_back, cot_all = exchange(
        4,
        ("swap_sp", d_query),
        ("swap_sp", attended_part),
        ("swap_tp", grads),
        ("pair_tp", cot_column.reshape(sp_n, target_local, width)),
    )
    query_grad = jnp.sum(query_terms.astype(jnp.float32), axis=0).astype(bf16)
    attended = jnp.sum(attended_terms.astype(jnp.float32), axis=0).astype(bf16)

    target_terms = matmul(query_grad, query_weight.T).astype(bf16)
    target_back, attended_all = exchange(
        5,
        ("swap_tp", target_terms.reshape(tp_n, target_local, width)),
        ("line_sp", attended.reshape(split)),
    )

    def from_slots(matrix):
        folded = matrix.reshape(tp_n // copies, copies, source_local, slot_width)
        folded = jnp.sum(folded.astype(jnp.float32), axis=1)
        return folded.transpose(1, 0, 2).reshape(source_local, -1).astype(bf16)

    key_grad = from_slots(grads_back[:, :, :slot_width])
    value_grad = from_slots(grads_back[:, :, slot_width:])
    d_normed_s = matmul(key_grad, key_full.T) + matmul(value_grad, value_full.T)
    source_grad = norm_back(source_rows, source_gain, d_normed_s)
    d_normed_t = jnp.sum(target_back.astype(jnp.float32), axis=0)
    target_grad = out_cotangent.astype(jnp.float32) + norm_back(
        target_rows, target_gain, d_normed_t
    )
    attended_rows = attended_all.reshape(sp_n, tp_n, target_local, local_width)
    out_weight_grad = jnp.einsum(
        "stlw,tsld->wd", attended_rows, cot_all, preferred_element_type=jnp.float32
    )
    return (target_grad, source_grad, out_weight_grad)


def fused_kernel(sp_n, tp_n, *refs):
    loads, stores = refs[:9], refs[9:12]
    target, source, tgain, sgain, qw, kw, vw, ow = refs[12:20]
    tgrad, sgrad, owg = refs[20:23]
    t_rx, c_rx, rows, cotf, w_rx, ns, q_all, d_all, kv_tx, kv_rx = refs[23:33]
    k2, v2, kvt, qc, dc, p_buf, dp_buf, own, st, st_rx, o_part = refs[33:44]
    o_tx, o_rx, att, attb, dq_f, dq_tx, dq_rx, qg, dk, dv = refs[44:54]
    g_tx, g_rx, gcat, tt, tp_rx, ts_tx, ts_rx, un = refs[54:62]
    send_s, t_s, c_s, w_s, far_s, cz_s, q_s, d_s, kv_s, near_s = refs[62:72]
    st_s, o_s, att_s, dq_s, g_s, tp_s, ts_s, load_s, store_s = refs[72:81]
    f32, bf16 = jnp.float32, jnp.bfloat16
    z, me = lax.axis_index("sp"), lax.axis_index("tp")
    core = lax.rem(me, 2)
    t_loc, width = target.shape
    s_loc = source.shape[0]
    slab, local_width = w_rx.shape[2], qw.shape[1]
    heads = local_width // HEAD_DIM
    t_block = tp_n * t_loc
    lanes = heads * t_block
    s_block = tp_n * s_loc
    pairs = w_rx.shape[0]
    scale = HEAD_DIM ** (-0.5)

    def across(i):
        return i + 2 - 4 * lax.rem(i // 2, 2)

    def along(i):
        return i + 4 - 8 * lax.rem(i // 4, 2)

    mate = me + 1 - 2 * core
    zt, zn = z + 2 - 4 * (z // 2), z + 1 - 2 * lax.rem(z, 2)
    zs = [lax.rem(z + k, sp_n) for k in range(1, sp_n)]
    ts = [lax.rem(me + k, tp_n) for k in range(1, tp_n)]

    barrier = pltpu.get_barrier_semaphore()
    for peer in zs:
        pl.semaphore_signal(barrier, inc=1, device_id=(peer, me), device_id_type=MESH)
    for peer in ts:
        pl.semaphore_signal(barrier, inc=1, device_id=(z, peer), device_id_type=MESH)

    for peer in ts:
        pl.semaphore_signal(barrier, inc=1, device_id=(zn, peer), device_id_type=MESH)

    sent = []
    ring = send_s.shape[0]

    def drain(one, when):
        if when is None:
            one.wait_send()
        else:
            pl.when(when)(lambda: one.wait_send())

    def push(src, dst, sem, zz, i, when=None):
        turn = len(sent) % ring
        if len(sent) >= ring:
            drain(*sent[len(sent) - ring])
        one = pltpu.make_async_remote_copy(
            src_ref=src,
            dst_ref=dst,
            send_sem=send_s.at[turn],
            recv_sem=sem,
            device_id=(zz, i),
            device_id_type=MESH,
        )
        sent.append((one, when))
        if when is None:
            one.start()
        else:
            pl.when(when)(lambda: one.start())

    def pull(ref, sem):
        pltpu.make_async_remote_copy(
            src_ref=ref,
            dst_ref=ref,
            send_sem=send_s.at[0],
            recv_sem=sem,
            device_id=(z, mate),
            device_id_type=MESH,
        ).wait_recv()

    kept = (target, source, tgain, sgain, qw, kw, vw, ow, c_rx.at[z, me])
    copies = [pltpu.make_async_copy(a, b, load_s.at[i]) for i, (a, b) in enumerate(zip(loads, kept))]
    for i in (0, 2, 8, 5, 6, 1, 3, 4, 7):
        copies[i].start()

    def store(i, a):
        one = pltpu.make_async_copy(a, stores[i], store_s.at[i])
        one.start()
        return one

    def nt(a, b):
        return lax.dot_general(a, b, (((1,), (1,)), ((), ())), preferred_element_type=f32)

    def nn(a, b):
        return jnp.dot(a, b, preferred_element_type=f32)

    class Gather:
        def __init__(self, slot, sem, far, depth):
            self.slot, self.sem, self.far, self.depth = slot, sem, far, depth

        def start(self):
            for peer in (across(me), along(me), mate):
                push(self.slot(me), self.slot(me), self.sem(me), z, peer)

        def half(self, origin, order):
            return self.slot(origin).at[self.depth[order] : self.depth[order + 1]]

        def mid(self):
            for order, origin in enumerate((across(me), along(me))):
                pull(self.slot(origin), self.sem(origin))
                piece = self.half(origin, order)
                push(piece, piece, self.far(order), z, along(me) if order == 0 else across(me))
            for origin in (across(me), along(me)):
                push(self.slot(origin), self.slot(origin), self.sem(origin), z, mate)

        def fin(self):
            origin = across(along(me))
            for order in range(2):
                pull(self.half(origin, order), self.far(order))
            push(self.slot(origin), self.slot(origin), self.sem(origin), z, mate)

        def rest(self):
            for origin in (mate, across(mate), along(mate), across(along(mate))):
                pull(self.slot(origin), self.sem(origin))

    copies[0].wait()
    copies[2].wait()
    t_rx[me] = normalize(target[...], tgain[...])
    copies[8].wait()
    pl.semaphore_wait(barrier, sp_n - 1 + 2 * (tp_n - 1))

    some, more = (0, t_loc // 2 // 8 * 8, t_loc), (0, slab // 2, slab)
    t_all = Gather(lambda o: t_rx.at[o], lambda o: t_s.at[o], lambda k: far_s.at[k], some)
    c_all = [
        Gather(
            lambda o, p=p: c_rx.at[p, o],
            lambda o, p=p: c_s.at[p * tp_n + o],
            lambda k, n=n: far_s.at[2 * n + 2 + k],
            some,
        )
        for n, p in enumerate([z] + zs)
    ]
    c_own, c_far = c_all[0], c_all[1:]
    w_all = [
        Gather(
            lambda o, c=c: w_rx.at[c, o],
            lambda o, c=c: w_s.at[c * tp_n + o],
            lambda k, c=c: far_s.at[2 * (sp_n + 1 + c) + k],
            more,
        )
        for c in range(pairs)
    ]

    t_all.start()
    for peer in zs:
        push(c_rx.at[z, me], c_rx.at[z, me], cz_s.at[z], peer, me)
    copies[5].wait()
    copies[6].wait()
    half = w_rx.shape[3]
    for c in range(pairs):
        part = (kw, vw)[c // 2]
        w_rx[c, me] = part[:, (c % 2) * half : (c % 2 + 1) * half]
    w_all[0].start()
    copies[1].wait()
    copies[3].wait()
    step = min(s_loc, 32)
    for i in range(0, s_loc, step):
        ns[i : i + step] = normalize(source[i : i + step], sgain[...])
    w_all[1].start()
    t_all.mid()
    w_all[0].mid()
    w_all[2].start()
    t_all.fin()
    t_all.rest()
    for o in range(tp_n):
        rows[o * t_loc : (o + 1) * t_loc] = t_rx[o]
    copies[4].wait()
    q_all[0] = (nn(rows[...], qw[...]).astype(bf16) * scale).astype(bf16)
    push(q_all.at[0], q_all.at[1], q_s.at[0], zt, me)
    w_all[1].mid()
    w_all[3].start()

    packed = s_loc // 2

    def split_kv(c):
        w_all[c].rest()
        total = nn(ns[:, :slab], w_rx[c, 0])
        for o in range(1, tp_n):
            total += nn(ns[:, o * slab : (o + 1) * slab], w_rx[c, o])
        total = total.astype(bf16)
        for j in range(tp_n // 2):
            head = (c % 2) * (tp_n // 2) + j
            part = total[:, j * HEAD_DIM : (j + 1) * HEAD_DIM]
            part = jnp.concatenate([part[:packed], part[packed:]], axis=1)
            kv_tx[c // 2, head] = part

            @pl.when(me == head)
            def _():
                kv_rx[0, c // 2, head] = part

            sem = kv_s.at[(c // 2) * tp_n + me]
            push(kv_tx.at[c // 2, head], kv_rx.at[0, c // 2, me], sem, z, head, me != head)
            if c // 2 == 1:
                push(kv_tx.at[1, head], kv_rx.at[1, 1, me], near_s.at[1 + me], zn, head)

    def unpack(w, kind):
        if w == 0:
            for o in ts:
                pull(kv_rx.at[0, kind, o], kv_s.at[kind * tp_n + o])
            if kind == 0:
                push(kv_rx.at[0, 0], kv_rx.at[1, 0], near_s.at[0], zn, me)
        elif kind == 0:
            pull(kv_rx.at[1, 0], near_s.at[0])
        else:
            for o in range(tp_n):
                pull(kv_rx.at[1, 1, o], near_s.at[1 + o])
        out = (k2, v2)[kind]
        for o in range(tp_n):
            part = kv_rx[w, kind, o]
            out[w, o * s_loc : o * s_loc + packed] = part[:, :HEAD_DIM]
            out[w, o * s_loc + packed : (o + 1) * s_loc] = part[:, HEAD_DIM:]

    groups = lanes // 128

    def fold(op, x, n=4):
        size = x.shape[0] // n
        parts = [
            op(x[i * size : (i + 1) * size].reshape(size // 8, 8, x.shape[1]), axis=0)
            for i in range(n)
        ]
        both = jnp.maximum if op is jnp.max else jnp.add
        return op(functools.reduce(both, parts), axis=0, keepdims=True)

    def line(x):
        return jnp.concatenate([x[g : g + 1] for g in range(groups)], axis=1)

    def take(u, full, sems, out):
        if u == 1:
            pull(full.at[1], sems.at[0])
        for h in range(heads):
            cols = slice(h * HEAD_DIM, (h + 1) * HEAD_DIM)
            out[u, h * t_block : (h + 1) * t_block] = full[u, :, cols]

    def weigh(u, w):
        if w == 0:
            take(u, q_all, q_s, qc)
        score = nt(k2[w], qc[u])
        top = fold(jnp.max, score)
        weight = jnp.exp(score - top)
        own[u, w, 0:1] = top
        own[u, w, 1:2] = fold(jnp.sum, weight)
        p_buf[u, w] = weight

    def turn_kv(w):
        for o in range(tp_n):
            part = slice(o * s_loc, (o + 1) * s_loc)
            both = jnp.concatenate([k2[w, part], v2[w, part]], axis=1)
            kvt[w, :, part] = both.astype(f32).T.astype(bf16)

    def first(u, w):
        if w == 0:
            take(u, d_all, d_s, dc)
        weight = p_buf[u, w]
        d_prob = nt(v2[w], dc[u])
        own[u, w, 2:3] = fold(jnp.sum, weight * d_prob)
        dp_buf[u, w] = d_prob
        o_part[u, w] = nn(kvt[w, HEAD_DIM:], weight.astype(bf16))

    def join(u):
        top = jnp.maximum(own[u, 0, 0:1], own[u, 1, 0:1])
        lifts = [jnp.exp(own[u, w, 0:1] - top) for w in range(2)]
        total = sum(own[u, w, 1:2] * lifts[w] for w in range(2))
        inner = sum(own[u, w, 2:3] * lifts[w] for w in range(2)) / total
        o_tx[u] = (sum(o_part[u, w] * lifts[w] for w in range(2)) / total).astype(bf16)
        for k, value in enumerate((top + jnp.log(total), inner)):
            for g in range(groups):
                row = groups * k + g
                st[u, row : row + 1] = value[:, g * 128 : (g + 1) * 128]

    cut = lanes // 2 // 128 * 128
    spans = [slice(0, cut), slice(cut, lanes)] if cut else [slice(0, lanes)]

    w_all[0].fin()
    split_kv(0)
    w_all[2].mid()
    c_own.start()
    w_all[1].fin()
    split_kv(1)
    w_all[3].mid()
    w_all[2].fin()
    unpack(0, 0)
    c_own.mid()
    weigh(0, 0)
    w_all[3].fin()
    split_kv(2)
    split_kv(3)
    c_own.fin()
    c_own.rest()
    for o in range(tp_n):
        cotf[z, o * t_loc : (o + 1) * t_loc] = c_rx[z, o]
    copies[7].wait()
    d_all[0] = nt(cotf[z], ow[...]).astype(bf16)
    push(d_all.at[0], d_all.at[1], d_s.at[0], zt, me)
    for k, p in enumerate(zs):
        pull(c_rx.at[p, me], cz_s.at[p])
        c_far[k].start()
    weigh(1, 0)
    unpack(1, 0)
    weigh(0, 1)
    weigh(1, 1)
    unpack(0, 1)
    turn_kv(0)
    first(0, 0)
    unpack(1, 1)
    turn_kv(1)
    first(0, 1)
    join(0)
    push(st.at[0], st_rx.at[0], st_s.at[0], zt, me)
    c_far[0].mid()
    first(1, 0)
    first(1, 1)
    join(1)
    push(st.at[1], st_rx.at[1], st_s.at[1], zt, me)
    for n, span in enumerate(spans):
        push(o_tx.at[1, :, span], o_rx.at[:, span], o_s.at[n], zt, me)

    def stats(u):
        logs = [st[u, :groups], st_rx[1 - u, :groups]]
        inners = [st[u, groups:], st_rx[1 - u, groups:]]
        top = jnp.maximum(*logs)
        log_total = top + jnp.log(sum(jnp.exp(x - top) for x in logs))
        lifts = [jnp.exp(x - log_total) for x in logs]
        return log_total, lifts, inners[0] * lifts[0] + inners[1] * lifts[1]

    def attend():
        lifts = [line(x) for x in stats(0)[1]]
        for n, span in enumerate(spans):
            pull(o_rx.at[:, span], o_s.at[n])
            mine = o_tx[0, :, span].astype(f32) * lifts[0][:, span]
            other = o_rx[:, span].astype(f32) * lifts[1][:, span]
            att[z, :, span] = (mine + other).astype(bf16)
            for peer in zs:
                part = att.at[z, :, span]
                push(part, part, att_s.at[n * sp_n + z], peer, me)

    def second(u, w, start):
        log_total, lifts, inner = stats(u)
        prob = p_buf[u, w] * jnp.exp(own[u, w, 0:1] - line(log_total))
        d_score = (prob * (dp_buf[u, w] - line(inner))).astype(bf16)
        prob = prob.astype(bf16)
        d_value, d_key = nn(prob, dc[u]), nn(d_score, qc[u])
        dv[w] = d_value if u == 1 else dv[w] + d_value
        dk[w] = d_key if u == 1 else dk[w] + d_key
        d_query = nn(kvt[w, :HEAD_DIM], d_score)
        dq_f[u] = d_query if start else dq_f[u] + d_query

    def send_g(w, plane):
        for o in range(tp_n):
            part = slice(o * s_loc, (o + 1) * s_loc)
            g_tx[w, o] = jnp.concatenate([dk[w, part], dv[w, part]], axis=1).astype(bf16)
        for o in ts + ([me] if w == 1 else []):
            push(g_tx.at[w, o], g_rx.at[w, me], g_s.at[w * tp_n + me], plane, o)

    c_far[1].mid()
    pull(st_rx.at[0], st_s.at[0])
    second(1, 0, True)
    c_far[2].mid()
    second(1, 1, False)
    dq_tx[...] = dq_f[1].astype(bf16)
    push(dq_tx, dq_rx, dq_s.at[0], zt, me)
    pull(st_rx.at[1], st_s.at[1])
    second(0, 1, True)
    send_g(1, zn)
    second(0, 0, False)
    send_g(0, z)
    g_rx[0, me] = g_tx[0, me]
    pull(dq_rx, dq_s.at[0])
    summed = (dq_f[0] + dq_rx[...].astype(f32)) * scale
    summed = summed.T
    for h in range(heads):
        piece = summed[h * t_block : (h + 1) * t_block].astype(bf16)
        qg[:, h * HEAD_DIM : (h + 1) * HEAD_DIM] = piece
    wide = 512

    def terms(j, carry):
        cols = pl.ds(j * wide, wide)
        value = nt(qg[...], qw[cols])
        for o in range(tp_n):
            tt[o, :, cols] = value[o * t_loc : (o + 1) * t_loc].astype(bf16)
        return carry

    for j in range(width // wide):
        terms(j, 0)
    chips = tp_n // 2
    for c in range(chips):
        push(tt.at[2 * c + 1 - core], tp_rx.at[c], tp_s.at[c], z, mate)
    attend()
    tile = 256

    for c in range(chips):
        pull(tp_rx.at[c], tp_s.at[c])
        ts_tx[c] = (tt[2 * c + core].astype(f32) + tp_rx[c].astype(f32)).astype(bf16)
    for r, peer in enumerate((across(along(me)), across(me), along(me))):
        push(ts_tx.at[peer // 2], ts_rx.at[r], ts_s.at[r], z, peer)
    for item in c_far:
        item.fin()
    side = tp_n * HEAD_DIM
    for o in ts:
        pull(g_rx.at[0, o], g_s.at[o])
    for o in range(tp_n):
        pull(g_rx.at[1, o], g_s.at[tp_n + o])
        part = (g_rx[0, o].astype(f32) + g_rx[1, o].astype(f32)).astype(bf16)
        gcat[:, o * HEAD_DIM : (o + 1) * HEAD_DIM] = part[:, :HEAD_DIM]
        gcat[:, side + o * HEAD_DIM : side + (o + 1) * HEAD_DIM] = part[:, HEAD_DIM:]

    def upstream(o, carry):
        for n in range(2):
            at = 2 * o + n
            cols = pl.ds(pl.multiple_of(at * slab, slab), slab)
            total = nt(gcat[:, : 4 * HEAD_DIM], w_rx[0, at])
            for c in range(1, pairs):
                total += nt(gcat[:, c * 4 * HEAD_DIM : (c + 1) * 4 * HEAD_DIM], w_rx[c, at])
            un[:, cols] = total
        return carry

    lax.fori_loop(0, tp_n // 2, upstream, 0)
    for i in range(0, s_loc, step):
        part = slice(i, i + step)
        sgrad[part] = norm_back(source[part], sgain[...], un[part])
    done = [store(1, sgrad)]
    for k, p in enumerate(zs):
        c_far[k].rest()
        for o in range(tp_n):
            cotf[p, o * t_loc : (o + 1) * t_loc] = c_rx[p, o]
    for p in zs:
        for n, span in enumerate(spans):
            pull(att.at[p, :, span], att_s.at[n * sp_n + p])
    for b in range(sp_n):
        for h in range(heads):
            piece = att[b, :, h * t_block : (h + 1) * t_block]
            attb[b, h * HEAD_DIM : (h + 1) * HEAD_DIM] = piece

    def weight_grad(j, carry):
        cols = pl.ds(j * tile, tile)
        owg[:, cols] = sum(nn(attb[b], cotf[b, :, cols]) for b in range(sp_n))
        return carry

    rest = width // tile // 4
    for n in range(4):
        for j in range(n * rest, (n + 1) * rest):
            weight_grad(j, 0)
        part = slice(n * rest * tile, (n + 1) * rest * tile)
        one = pltpu.make_async_copy(owg.at[:, part], stores[2].at[:, part], store_s.at[2 + n])
        one.start()
        done.append(one)
    mine = ts_tx[me // 2].astype(f32)
    for r in range(3):
        pull(ts_rx.at[r], ts_s.at[r])
    mine = mine + sum(ts_rx[r].astype(f32) for r in range(3))
    tgrad[...] = c_rx[z, me].astype(f32) + norm_back(target[...], tgain[...], mine)
    done.append(store(0, tgrad))

    for one, when in sent[-ring:]:
        drain(one, when)
    for one in done:
        one.wait()


def finish_kernel(*refs):
    ins, outs, held = refs[:3], refs[3:6], refs[6:9]
    in_sems, out_sems = refs[9:11]
    pieces = []
    for i in (2, 1, 0):
        size = ins[i].shape[0]
        step = max(size // 4 // 8 * 8, 8)
        for at in range(0, size, step):
            part = pl.ds(at, min(step, size - at))
            pieces.append((ins[i].at[part], held[i].at[part], outs[i].at[part]))
    for k, (a, b, c) in enumerate(pieces):
        pltpu.make_async_copy(a, b, in_sems.at[k]).start()
    for k, (a, b, c) in enumerate(pieces):
        pltpu.make_async_copy(a, b, in_sems.at[k]).wait()
        pltpu.make_async_copy(b, c, out_sems.at[k]).start()
    for k, (a, b, c) in enumerate(pieces):
        pltpu.make_async_copy(b, c, out_sems.at[k]).wait()


def finish(*arrays):
    return pl.pallas_call(
        finish_kernel,
        out_shape=[jax.ShapeDtypeStruct(a.shape, a.dtype) for a in arrays],
        in_specs=[pl.BlockSpec(memory_space=pltpu.HBM)] * 3,
        out_specs=[pl.BlockSpec(memory_space=pl.ANY)] * 3,
        scratch_shapes=[pltpu.VMEM(a.shape, a.dtype) for a in arrays]
        + [pltpu.SemaphoreType.DMA((12,)), pltpu.SemaphoreType.DMA((12,))],
        compiler_params=pltpu.CompilerParams(vmem_limit_bytes=67043328),
    )(*arrays)


def fused_body(
    target_rows,
    source_rows,
    target_gain,
    source_gain,
    query_weight,
    key_weight,
    value_weight,
    out_weight,
    out_cotangent,
):
    sp_n, tp_n = lax.axis_size("sp"), lax.axis_size("tp")
    t_loc, width = target_rows.shape
    s_loc = source_rows.shape[0]
    local_width = query_weight.shape[1]
    heads = local_width // HEAD_DIM
    t_block, s_block = tp_n * t_loc, tp_n * s_loc
    lanes = heads * t_block
    slab = key_weight.shape[0]
    pairs = KV_HEADS // 2
    two = 2 * HEAD_DIM
    f32, bf16 = jnp.float32, jnp.bfloat16
    vmem, sem = pltpu.VMEM, pltpu.SemaphoreType.DMA
    sends = 48
    scratch = [
        vmem((t_loc, width), bf16),
        vmem((s_loc, width), bf16),
        vmem((1, width), f32),
        vmem((1, width), f32),
        vmem((width, local_width), bf16),
        vmem((slab, key_weight.shape[1]), bf16),
        vmem((slab, key_weight.shape[1]), bf16),
        vmem((local_width, width), bf16),
        vmem((t_loc, width), f32),
        vmem((s_loc, width), f32),
        vmem((local_width, width), f32),
        vmem((tp_n, t_loc, width), bf16),
        vmem((sp_n, tp_n, t_loc, width), bf16),
        vmem((t_block, width), bf16),
        vmem((sp_n, t_block, width), bf16),
        vmem((pairs, tp_n, slab, 2 * two), bf16),
        vmem((s_loc, width), bf16),
        vmem((2, t_block, local_width), bf16),
        vmem((2, t_block, local_width), bf16),
        vmem((2, tp_n, s_loc // 2, two), bf16),
        vmem((2, 2, tp_n, s_loc // 2, two), bf16),
        vmem((2, s_block, HEAD_DIM), bf16),
        vmem((2, s_block, HEAD_DIM), bf16),
        vmem((2, two, s_block), bf16),
        vmem((2, lanes, HEAD_DIM), bf16),
        vmem((2, lanes, HEAD_DIM), bf16),
        vmem((2, 2, s_block, lanes), f32),
        vmem((2, 2, s_block, lanes), f32),
        vmem((2, 2, 3, lanes), f32),
        vmem((2, lanes // 64, 128), f32),
        vmem((2, lanes // 64, 128), f32),
        vmem((2, 2, HEAD_DIM, lanes), f32),
        vmem((2, HEAD_DIM, lanes), bf16),
        vmem((HEAD_DIM, lanes), bf16),
        vmem((sp_n, HEAD_DIM, lanes), bf16),
        vmem((sp_n, local_width, t_block), bf16),
        vmem((2, HEAD_DIM, lanes), f32),
        vmem((HEAD_DIM, lanes), bf16),
        vmem((HEAD_DIM, lanes), bf16),
        vmem((t_block, local_width), bf16),
        vmem((2, s_block, HEAD_DIM), f32),
        vmem((2, s_block, HEAD_DIM), f32),
        vmem((2, tp_n, s_loc, two), bf16),
        vmem((2, tp_n, s_loc, two), bf16),
        vmem((s_loc, tp_n * two), bf16),
        vmem((tp_n, t_loc, width), bf16),
        vmem((tp_n // 2, t_loc, width), bf16),
        vmem((tp_n // 2, t_loc, width), bf16),
        vmem((3, t_loc, width), bf16),
        vmem((s_loc, width), f32),
        sem((sends,)),
        sem((tp_n,)),
        sem((sp_n * tp_n,)),
        sem((pairs * tp_n,)),
        sem((2 * (sp_n + 1 + pairs),)),
        sem((sp_n,)),
        sem((1,)),
        sem((1,)),
        sem((2 * tp_n,)),
        sem((1 + tp_n,)),
        sem((2,)),
        sem((2,)),
        sem((2 * sp_n,)),
        sem((1,)),
        sem((2 * tp_n,)),
        sem((tp_n // 2,)),
        sem((3,)),
        sem((9,)),
        sem((6,)),
    ]
    results = pl.pallas_call(
        functools.partial(fused_kernel, sp_n, tp_n),
        out_shape=[
            jax.ShapeDtypeStruct((t_loc, width), f32),
            jax.ShapeDtypeStruct((s_loc, width), f32),
            jax.ShapeDtypeStruct((local_width, width), f32),
        ],
        in_specs=[pl.BlockSpec(memory_space=pl.ANY)] * 9,
        out_specs=[pl.BlockSpec(memory_space=pl.ANY)] * 3,
        scratch_shapes=scratch,
        compiler_params=pltpu.CompilerParams(
            collective_id=0,
            has_side_effects=True,
            vmem_limit_bytes=67043328,
        ),
    )(
        target_rows,
        source_rows,
        target_gain[None],
        source_gain[None],
        query_weight,
        key_weight,
        value_weight,
        out_weight,
        out_cotangent,
    )
    return tuple(finish(*results))


def choose(*args):
    square = lax.axis_size("tp") == 8 and KV_HEADS == 8 and lax.axis_size("sp") == 4
    lanes = lax.axis_size("tp") * args[0].shape[0] * args[4].shape[1] // HEAD_DIM
    if square and lanes % 128 == 0 and lanes <= 1024:
        return fused_body(*args)
    return body(*args)


def solution(mesh):
    return jax.shard_map(
        choose,
        mesh=mesh,
        in_specs=(
            P(("sp", "tp"), None),
            P(("sp", "tp"), None),
            P(),
            P(),
            P(None, "tp"),
            P("tp", None),
            P("tp", None),
            P("tp", None),
            P(("sp", "tp"), None),
        ),
        out_specs=(P(("sp", "tp"), None), P(("sp", "tp"), None), P("tp", None)),
        check_vma=False,
    )
```
